32 devices in a mesh: gr: 2 (over x), fs: 8 (over z, y), tp: 2 (over core).
Axes of the slice: x: 2, y: 2, z: 4, core: 2. Of those that a mesh axis runs over, the one named last changes fastest.
Arguments:
- tokens: bfloat16 [4096, 2048], P(('gr', 'fs')), may hold values from -6 to 6
- norm_gain: float32 [2048], P(('gr', 'fs')), may hold values from 0.1 to 1.9
- gate_train: float32 [8, 2048, 1024], P(None, ('gr', 'fs'), 'tp'), may hold values from -0.125 to 0.125
- up_train: float32 [8, 2048, 1024], P(None, ('gr', 'fs'), 'tp'), may hold values from -0.125 to 0.125
- down_train: float32 [8, 1024, 2048], P(None, 'tp', ('gr', 'fs')), may hold values from -0.1875 to 0.1875
- expert_ids: int32 [4096, 2], P(('gr', 'fs')), may hold values from 0 to 7, all different within a row; in each aligned block of 256 rows (0 to 255, 256 to 511, ...) at most 128 rows name the same one
- route_score: float32 [4096, 2], P(('gr', 'fs')), may hold values from 0.05 to 1
Outputs:
- gate_ready: bfloat16 [8, 2048, 1024], P('fs', None, 'tp')
- up_ready: bfloat16 [8, 2048, 1024], P('fs', None, 'tp')
- down_ready: bfloat16 [8, 1024, 2048], P('fs', 'tp')
- mixed: bfloat16 [4096, 2048], P(('gr', 'fs'), 'tp')
The draws below stay inside these ranges and needn't reach their ends.
Inputs may be any that keep to these rules, and one draw needn't show every extreme that they name: `expert_ids`: each row names two different experts. Among the 256 rows of one device no expert is named more than 128 times, and in every draw some expert is named exactly 128 times by some device's rows.
All inputs are finite; a program needn't handle non-finite values.
Results may differ from the reference program's by a relative error of at most 0.015.
Values may be sent and summed in bfloat16 or wider, within the bound.
A program may use at most 64 MiB of HBM per device.

```python
import math
import jax
import jax.numpy as jnp
import numpy as np
from jax import lax

D = 2048
FF = 1024
TOK_DEV = 256
EXPERTS = 8
CAP = 128
TOKENS = 4096
N_GR = 2
N_FS = 8
N_TP = 2


def block_levels(stream_key, dims, pieces, least, top_value):
    loudness, own = 1.0, jax.random.fold_in(stream_key, 6)
    for dim, parts in pieces:
        draws = jnp.exp(jax.random.uniform(jax.random.fold_in(own, dim), (parts,), jnp.float32, least / len(pieces), top_value / len(pieces)))
        loudness = loudness * jnp.repeat(draws, dims[dim] // parts).reshape([-1 if axis == dim else 1 for axis in range(len(dims))])
    return loudness


def assign_block(own_key, own, number, rows, count, top, most, slope):
    ranking = jax.random.permutation(own_key, count)
    crowded, usual = portions_of(count, rows * top, most, slope, True), portions_of(count, rows * top, most, slope, False)
    places = jnp.arange(count)

    def named(lengths, rotation):
        used = int((lengths > 0).sum())
        fixed = max(1, used // 4)
        moved = fixed + (places - fixed + rotation * (used - fixed)) % max(1, count - fixed)
        return jnp.zeros((count,), jnp.int32).at[ranking[jnp.where(places < fixed, places, moved)]].set(jnp.asarray(lengths, jnp.int32))

    lengths = jnp.where(number % 4 == 0, named(crowded, number // 4), named(usual, number - number // 4 - 1))
    mixed = jax.random.permutation(jax.random.fold_in(own, 3), count)
    source_of, receiver = mixed[0:count // 2 * 2:2], mixed[1:count // 2 * 2:2]
    slack = jnp.minimum(lengths[source_of] - 1, most - lengths[receiver]) // 2
    slack = jnp.where((source_of == ranking[0]) | (receiver == ranking[0]) | (lengths[receiver] == 0), 0, jnp.maximum(slack, 0))
    moved = jax.random.randint(jax.random.fold_in(own, 4), (count // 2,), 0, 1 << 20) % (slack + 1)
    lengths = lengths.at[source_of].add(-moved).at[receiver].add(moved)
    members = jnp.searchsorted(jnp.cumsum(lengths), jnp.arange(rows * top), side="right").astype(jnp.int32)
    table = members.reshape(top, rows).T
    table = table[jax.random.permutation(jax.random.fold_in(own, 1), rows)]
    rotation = jax.random.randint(jax.random.fold_in(own, 2), (rows, 1), 0, top)
    return jnp.take_along_axis(table, (jnp.arange(top)[None, :] + rotation) % top, axis=1)


def portions_of(amount, total, reach, slope, full):
    portions = [(1 << 20) // math.isqrt(standing ** slope) + 1 for standing in range(1, amount + 1)]
    largest = reach if full else min(reach, max(-(-total // amount), total * portions[0] // sum(portions)))
    least = 1 if total - largest >= amount - 1 else 0
    holding, rest = [largest] + [least] * (amount - 1), total - largest - least * (amount - 1)
    while rest > 0:
        candidates = [i for i in range(1, amount) if holding[i] < largest] or [i for i in range(1, amount) if holding[i] < reach]
        pool, left = sum([portions[i] for i in candidates]), rest
        for i in candidates:
            addition = min(reach - holding[i], max(1, left * portions[i] // pool), rest)
            holding[i] = holding[i] + addition
            rest = rest - addition
    return np.array(holding)


def gaussian(own_key, shape, scale, bound, split=(), kind=jnp.bfloat16):
    result = scale * jax.random.normal(own_key, shape, jnp.float32)
    if split:
        result = result * block_levels(own_key, shape, split, -0.22, 0.18)
    return jnp.clip(result, -bound, bound).astype(kind)


def setup_inputs(seed: int = 0) -> dict:
    key_list = jax.random.split(jax.random.key(seed), 8)
    tokens = gaussian(key_list[0], (TOKENS, D), 1.0, 6.0, ((0, 16),))
    norm_gain = jnp.clip(1.0 + 0.18 * jax.random.normal(key_list[1], (D,), jnp.float32), 0.1, 1.9)
    gate_train = gaussian(key_list[2], (EXPERTS, D, FF), D ** -0.5, 0.125, ((1, 16), (2, 2)), jnp.float32)
    up_train = gaussian(key_list[3], (EXPERTS, D, FF), D ** -0.5, 0.125, ((1, 16), (2, 2)), jnp.float32)
    down_train = gaussian(key_list[4], (EXPERTS, FF, D), FF ** -0.5, 0.1875, ((1, 2), (2, 16)), jnp.float32)
    expert_ids_keys = jax.random.split(jax.random.fold_in(key_list[5], 1), TOKENS // TOK_DEV)
    expert_ids_turns = jax.random.permutation(jax.random.fold_in(key_list[5], 3), TOKENS // TOK_DEV)
    expert_ids = jax.vmap(lambda own, number: assign_block(jax.random.fold_in(key_list[5], 2), own, number, TOK_DEV, EXPERTS, 2, CAP, 2))(expert_ids_keys, expert_ids_turns).reshape((TOKENS, 2))
    route_score = jnp.clip(jnp.exp(math.log(1.0) - 2.9957323 * jax.random.uniform(key_list[6], (TOKENS, 2), jnp.float32) ** block_levels(key_list[6], (TOKENS, 2), ((0, 16),), -0.2, 0.2)), 0.05, 1.0)
    return dict(tokens=tokens, norm_gain=norm_gain, gate_train=gate_train, up_train=up_train, down_train=down_train, expert_ids=expert_ids, route_score=route_score)


epsilon = 1e-06

def reference(tokens, norm_gain, gate_train, up_train, down_train, expert_ids, route_score):
    gate_ready = (norm_gain[None, :, None] * gate_train).astype(jnp.bfloat16)
    up_ready = (norm_gain[None, :, None] * up_train).astype(jnp.bfloat16)
    down_ready = down_train.astype(jnp.bfloat16)
    floated = tokens.astype(jnp.float32)
    normed = (floated * lax.rsqrt(lax.optimization_barrier(jnp.mean(floated * floated, axis=-1, keepdims=True)) + epsilon)).astype(jnp.bfloat16)
    route_share = route_score / lax.optimization_barrier(jnp.sum(route_score, axis=-1, keepdims=True))
    blocks = N_GR * N_FS
    picks = TOK_DEV * 2
    flat_ids = expert_ids.reshape(blocks, picks)
    flat_share = route_share.reshape(blocks, picks)
    token_of = ((jnp.arange(picks, dtype=jnp.int32) // 2)[None, :] + (jnp.arange(blocks, dtype=jnp.int32) * TOK_DEV)[:, None]).astype(jnp.int32)
    block_rows = jnp.broadcast_to(jnp.arange(blocks, dtype=jnp.int32)[:, None], (blocks, picks))
    hidden_block = FF // N_TP

    def per_expert(total, expert):
        matches = (flat_ids == expert).astype(jnp.int32)
        ranked = jnp.cumsum(matches, axis=1) - 1
        column = jnp.where(matches > 0, ranked, CAP).astype(jnp.int32)
        token_table = jnp.zeros((blocks, CAP), jnp.int32).at[block_rows, column].set(token_of, mode='drop')
        share_table = jnp.zeros((blocks, CAP), jnp.float32).at[block_rows, column].set(flat_share, mode='drop')
        token_index = token_table.reshape(-1)
        picked_rows = normed[token_index]
        gate_act = jnp.dot(picked_rows, gate_ready[expert], preferred_element_type=jnp.float32)
        up_act = jnp.dot(picked_rows, up_ready[expert], preferred_element_type=jnp.float32)
        hidden = (jax.nn.silu(gate_act) * up_act).astype(jnp.bfloat16)
        partial_value = jnp.einsum('rnh,nhk->rnk', hidden.reshape(-1, N_TP, hidden_block).astype(jnp.float32), down_ready[expert].reshape(N_TP, hidden_block, D).astype(jnp.float32))
        rounded = lax.optimization_barrier(partial_value.astype(jnp.bfloat16))
        expert_out = lax.optimization_barrier(jnp.sum(rounded.astype(jnp.float32), axis=1)).astype(jnp.bfloat16)
        total = total.at[token_index].add(share_table.reshape(-1)[:, None] * expert_out.astype(jnp.float32))
        return (total, None)
    start = jnp.zeros((TOKENS, D), jnp.float32)
    summed, _ = lax.scan(per_expert, start, jnp.arange(EXPERTS, dtype=jnp.int32))
    return (gate_ready, up_ready, down_ready, summed.astype(jnp.bfloat16))
```

```python
import functools

import jax
import jax.numpy as jnp
from jax import lax
from jax.experimental import pallas as pl
from jax.experimental.pallas import tpu as pltpu
from jax.sharding import PartitionSpec as P

epsilon = 1e-06
MESH = pl.DeviceIdType.MESH


def remote(src, dst, send_sem, recv_sem, where):
    return pltpu.make_async_remote_copy(
        src_ref=src, dst_ref=dst, send_sem=send_sem, recv_sem=recv_sem, device_id=where, device_id_type=MESH
    )


def greet(sizes):
    barrier = pltpu.get_barrier_semaphore()
    count = 0
    for name, size in sizes.items():
        me = lax.axis_index(name)
        for k in range(1, size):
            pl.semaphore_signal(barrier, inc=1, device_id={name: lax.rem(me + k, size)}, device_id_type=MESH)
            count += 1
    pl.semaphore_wait(barrier, count)


def spread_kernel(sizes, local, direct_down, gate, up, down, rows, keys, gate_out, up_out, down_out, rows_out, keys_out,
                  w_send, w_recv, g_send, g_recv, up_send, low_send, y_send, x_recv, t_send, t_recv, k_send, k_recv, own_sem):
    n_gr, n_fs, n_tp = sizes["gr"], sizes["fs"], sizes["tp"]
    g, f, p = lax.axis_index("gr"), lax.axis_index("fs"), lax.axis_index("tp")
    inner = 2 if n_fs % 2 == 0 else 1
    lines = n_fs // inner
    z, y = f // inner, lax.rem(f, inner)
    depth = gate.shape[1]
    half = rows.shape[1] // n_tp
    cols = pl.ds(pl.multiple_of(p * half, half), half)
    sources, outs = (gate, up, down), (gate_out, up_out, down_out)

    def place(w, block):
        start = pl.multiple_of(block * depth, depth)
        if w < 2:
            return outs[w].at[:, pl.ds(start, depth), :]
        return outs[w].at[:, :, pl.ds(start, depth)] if direct_down else outs[w].at[block]

    greet(sizes)

    own = [pltpu.make_async_copy(rows, rows_out.at[f], own_sem.at[0]),
           pltpu.make_async_copy(keys, keys_out.at[f], own_sem.at[1])]
    for w in range(3):
        own.append(pltpu.make_async_copy(sources[w].at[pl.ds(f * local, local)], place(w, g * n_fs + f), own_sem.at[2 + w]))

    def block_of(b):
        return rows_out.at[b, :, cols]

    def row_copy(b, first, kind, where):
        src = rows.at[:, cols] if first else block_of(b)
        return remote(src, block_of(b), {"u": up_send, "d": low_send, "y": y_send}[kind].at[b], x_recv.at[b], where)

    def tp_copy(b, j):
        return remote(block_of(b), block_of(b), t_send.at[j, b], t_recv.at[j, b], {"tp": lax.rem(p + j + 1, n_tp)})

    def go_up(b, first, act):
        @pl.when(z < lines - 1)
        def _():
            act(row_copy(b, first, "u", {"fs": lax.rem(f + inner, n_fs)}))

    def go_down(b, first, act):
        @pl.when(z > 0)
        def _():
            act(row_copy(b, first, "d", {"fs": lax.rem(f + n_fs - inner, n_fs)}))

    def go_side(b, first, act):
        if inner == 2:
            act(row_copy(b, first, "y", {"fs": f + 1 - 2 * y}))

    def start(c):
        c.start()

    def recv(c):
        c.wait_recv()

    def sent(c):
        c.wait_send()

    go_up(f, True, start)
    go_down(f, True, start)
    go_side(f, True, start)
    key_copies = []
    for k in range(1, n_fs):
        to = lax.rem(f + k, n_fs)
        c = remote(keys, keys_out.at[f], k_send.at[k], k_recv.at[k], {"fs": to})
        c.start()
        key_copies.append(c)
    for c in own:
        c.start()

    def gr_copy(w, b, k, j, first):
        src = sources[w].at[pl.ds(f * local, local)] if first else place(w, b)
        return remote(src, place(w, b), g_send.at[w, k, j], g_recv.at[w, k, j], {"gr": lax.rem(g + j + 1, n_gr)})

    for w in range(3):
        for j in range(n_gr - 1):
            gr_copy(w, g * n_fs + f, 0, j, True).start()

    for s in range(1, lines):
        @pl.when(z >= s)
        def _():
            b = f - s * inner
            row_copy(b, False, "u", {"fs": lax.rem(f + inner, n_fs)}).wait_recv()
            go_up(b, False, start)
            go_side(b, False, start)
            for j in range(n_tp - 1):
                tp_copy(b, j).start()

        @pl.when(z < lines - s)
        def _():
            b = f + s * inner
            row_copy(b, False, "d", {"fs": lax.rem(f + inner, n_fs)}).wait_recv()
            go_down(b, False, start)
            go_side(b, False, start)
            for j in range(n_tp - 1):
                tp_copy(b, j).start()

    def w_copy(w, k):
        to = lax.rem(f + k, n_fs)
        return remote(sources[w].at[pl.ds(to * local, local)], place(w, g * n_fs + f), w_send.at[w, k], w_recv.at[w, k], {"fs": to})

    for w in range(3):
        for k in range(1, n_fs):
            w_copy(w, k).start()

    if inner == 2:
        for s in range(lines):
            b = lax.rem(z + s, lines) * inner + 1 - y
            row_copy(b, False, "y", {"fs": f + 1 - 2 * y}).wait_recv()
            for j in range(n_tp - 1):
                tp_copy(b, j).start()

    for w in range(3):
        for k in range(1, n_fs):
            w_copy(w, k).wait_recv()
            b = g * n_fs + lax.rem(f + n_fs - k, n_fs)
            for j in range(n_gr - 1):
                gr_copy(w, b, k, j, False).start()

    for k in range(1, n_fs):
        b = lax.rem(f + k, n_fs)
        for j in range(n_tp - 1):
            c = tp_copy(b, j)
            c.wait_recv()
            c.wait_send()
    for c in key_copies:
        c.wait_recv()
        c.wait_send()
    for c in own:
        c.wait()
    go_up(f, True, sent)
    go_down(f, True, sent)
    go_side(f, True, sent)
    for s in range(1, lines):
        @pl.when(z >= s)
        def _():
            go_up(f - s * inner, False, sent)
            go_side(f - s * inner, False, sent)

        @pl.when(z < lines - s)
        def _():
            go_down(f + s * inner, False, sent)
            go_side(f + s * inner, False, sent)
    for w in range(3):
        for k in range(n_fs):
            if k:
                w_copy(w, k).wait_send()
            for j in range(n_gr - 1):
                c = gr_copy(w, g * n_fs + lax.rem(f + n_fs - k, n_fs), k, j, False)
                c.wait_recv()
                c.wait_send()


def return_kernel(sizes, part, out, held, total, t_send, t_recv, f_send, f_recv):
    n_fs, n_tp = sizes["fs"], sizes["tp"]
    f, p = lax.axis_index("fs"), lax.axis_index("tp")
    half = part.shape[2] // n_tp

    def cols(q):
        return pl.ds(pl.multiple_of(q * half, half), half)

    greet({"fs": n_fs, "tp": n_tp})
    order = list(range(1, n_fs)) + [0]

    def tp_copy(k, j):
        to = lax.rem(p + j + 1, n_tp)
        b = lax.rem(f + k, n_fs)
        return remote(part.at[b, :, cols(to)], held.at[j, b], t_send.at[j, k], t_recv.at[j, k], {"tp": to})

    def f_copy(k):
        b = lax.rem(f + k, n_fs)
        return remote(total.at[b], out.at[f], f_send.at[k], f_recv.at[k], {"fs": b})

    for k in order:
        for j in range(n_tp - 1):
            tp_copy(k, j).start()
    for k in order:
        b = lax.rem(f + k, n_fs)
        value = part[b, :, cols(p)].astype(jnp.float32)
        for j in range(n_tp - 1):
            tp_copy(k, j).wait_recv()
            value = value + held[j, b].astype(jnp.float32)
        value = value.astype(jnp.bfloat16)
        if k == 0:
            out[b] = value
        else:
            total[b] = value
            f_copy(k).start()
    for k in order:
        for j in range(n_tp - 1):
            tp_copy(k, j).wait_send()
        if k:
            f_copy(k).wait_recv()
            f_copy(k).wait_send()


def handover_kernel(sizes, tokens, gain, ids, score, gate_hbm, up_hbm, down_hbm, gate_out, up_out, down_out, mixed,
                    gate_raw, up_raw, down_raw, gate_cut, up_cut, down_cut, rows_in, meta, picked, hidden, part, held,
                    total, back, collect, far_out, far_in, near_w, gate_w,
                    load_sem, w_send, w_recv, g_send, g_recv, x_recv, line_send, y_send, t_send, t_recv, k_send, k_recv,
                    p_send, p_recv, n_send, n_recv, c_send, c_recv, o_send, o_recv):
    n_fs = sizes["fs"]
    g, f, p = lax.axis_index("gr"), lax.axis_index("fs"), lax.axis_index("tp")
    z, y = f // 2, lax.rem(f, 2)
    low, side = lax.rem(z, 2), z // 2
    depth = gate_hbm.shape[1]
    count, width = tokens.shape
    slots = back.shape[0] * 2 // n_fs
    half = width // 2
    span = half // 2
    quad = n_fs // 2
    bf16, f32 = jnp.bfloat16, jnp.float32
    raws, cuts, outs = (gate_raw, up_raw, down_raw), (gate_cut, up_cut, down_cut), (gate_out, up_out, down_out)
    hbms = (gate_hbm, up_hbm, down_hbm)
    near = [(0, 1), (1, 0), (1, 1)]
    far = [(2, 0), (3, 0), (2, 1), (3, 1)]
    index = {t: i for i, t in enumerate(near + far + [(0, 0)])}
    door = 1 + side
    is_door = z == door

    def level(s):
        lo = 1 - low if s % 2 else low
        hi = 1 - side if s // 2 else side
        return hi * 2 + lo

    def peer(t):
        return level(t[0]) * 2 + (1 - y if t[1] else y)

    def cols(q):
        return pl.ds(pl.multiple_of(q * half, half), half)

    def place(w, block):
        at = pl.ds(pl.multiple_of(block * depth, depth), depth)
        return outs[w].at[0, at, :] if w < 2 else outs[w].at[0, :, at]

    def w_copy(w, t):
        to = peer(t)
        return remote(cuts[w].at[to], place(w, g * n_fs + f), w_send.at[w, index[t]], w_recv.at[w, index[t]], {"fs": to})

    def g_copy(w, t):
        b = g * n_fs + peer(t)
        src = cuts[w].at[f] if t == (0, 0) else place(w, b)
        return remote(src, place(w, b), g_send.at[w, index[t]], g_recv.at[w, index[t]], {"gr": 1 - g})

    def send_weights(w):
        for t in near + far:
            w_copy(w, t).start()
        g_copy(w, (0, 0)).start()

    def pass_on(w, t):
        w_copy(w, t).wait_recv()
        g_copy(w, t).start()

    def block_of(b):
        return rows_in.at[b, :, cols(p)]

    def line_copy(b, i, to):
        return remote(block_of(b), block_of(b), line_send.at[i], x_recv.at[b], {"fs": to})

    def y_copy(b):
        return remote(block_of(b), block_of(b), y_send.at[lax.div(b, 2)], x_recv.at[b], {"fs": z * 2 + 1 - y})

    def tp_copy(b):
        return remote(block_of(b), block_of(b), t_send.at[b], t_recv.at[b], {"tp": 1 - p})

    def key_copy(t):
        return remote(meta.at[f], meta.at[f], k_send.at[index[t]], k_recv.at[index[t]], {"fs": peer(t)})

    def arrived(b):
        line_copy(b, 0, z * 2 + 1 - y).wait_recv()

    def cut(w):
        pltpu.make_async_copy(hbms[w], raws[w], load_sem.at[w]).wait()
        if w < 2:
            scale = jnp.broadcast_to(gain[...], (128, depth)).T
            for e in range(n_fs):
                for c in range(0, raws[w].shape[2], 128):
                    cuts[w][e, :, c:c + 128] = (scale * raws[w][e, :, c:c + 128]).astype(bf16)
            outs[w][0, pl.ds(pl.multiple_of((g * n_fs + f) * depth, depth), depth), :] = cuts[w][f]
        else:
            for e in range(n_fs):
                cuts[w][e] = raws[w][e].astype(bf16)
            outs[w][0, :, pl.ds(pl.multiple_of((g * n_fs + f) * depth, depth), depth)] = cuts[w][f]

    def pick_rows(b):
        wanted = (f * slots + lax.broadcasted_iota(jnp.int32, (slots, count), 0)).astype(f32)
        hit = ((meta[b, 0:1, :] == wanted) | (meta[b, 1:2, :] == wanted)).astype(f32).astype(bf16)
        for c in range(0, width, 512):
            picked[pl.ds(pl.multiple_of(b * slots, slots), slots), c:c + 512] = jnp.dot(
                hit, rows_in[b, :, c:c + 512], preferred_element_type=f32).astype(bf16)

    def shares(b):
        wanted = (side * (quad * slots) + lax.broadcasted_iota(jnp.int32, (quad * slots, count), 0)).astype(f32)
        table = jnp.where(meta[b, 0:1, :] == wanted, meta[b, 2:3, :], 0.0) + jnp.where(
            meta[b, 1:2, :] == wanted, meta[b, 3:4, :], 0.0)
        return table.T.astype(bf16)

    for w in range(3):
        pltpu.make_async_copy(hbms[w], raws[w], load_sem.at[w]).start()
    barrier = pltpu.get_barrier_semaphore()
    heard = 0
    for name, size in sizes.items():
        me = lax.axis_index(name)
        for k in range(1, size):
            pl.semaphore_signal(barrier, inc=1, device_id={name: lax.rem(me + k, size)}, device_id_type=MESH)
            heard += 1

    expert = lax.broadcasted_iota(jnp.int32, (16, count), 0)
    names = ((ids[0:1, :] == expert) | (ids[1:2, :] == expert)).astype(f32).astype(bf16)
    earlier = lax.broadcasted_iota(jnp.int32, (count, count), 0) < lax.broadcasted_iota(jnp.int32, (count, count), 1)
    rank = jnp.dot(names, earlier.astype(f32).astype(bf16), preferred_element_type=f32) + (expert * slots).astype(f32)
    both = score[0:1, :] + score[1:2, :]
    table = [jnp.sum(jnp.where(ids[k:k + 1, :] == expert, rank, 0.0), axis=0, keepdims=True) for k in range(2)]
    table += [score[k:k + 1, :] / both for k in range(2)]
    for i in range(4):
        meta[f, i:i + 1, :] = table[i]
    meta[f, 4:8, :] = jnp.zeros((4, count), f32)

    cut(0)
    pl.semaphore_wait(barrier, heard)
    send_weights(0)
    for r in range(0, count, 32):
        x = tokens[r:r + 32, :].astype(f32)
        rows_in[f, r:r + 32, :] = (x * lax.rsqrt(jnp.mean(x * x, axis=-1, keepdims=True) + epsilon)).astype(bf16)
    for t in near + far:
        key_copy(t).start()
    line_copy(f, 0, level(1) * 2 + y).start()
    line_copy(f, 1, (2 - side) * 2 + y).start()
    y_copy(f).start()
    cut(1)
    send_weights(1)
    cut(2)

    for w in range(2):
        for t in near:
            pass_on(w, t)
    b = peer((1, 0))
    arrived(b)
    y_copy(b).start()
    tp_copy(b).start()
    for t in far:
        pass_on(0, t)
    for i, t in enumerate([(2, 0), (3, 0)]):
        b = peer(t)
        arrived(b)

        @pl.when(is_door)
        def _():
            line_copy(b, 2 + i, level(1) * 2 + y).start()

        y_copy(b).start()
        tp_copy(b).start()
    send_weights(2)
    for t in [(0, 1), (1, 1), (2, 1), (3, 1)]:
        b = peer(t)
        arrived(b)
        tp_copy(b).start()
    pick_rows(f)
    near_w[...] = shares(f)
    for t in near + far:
        key_copy(t).wait_recv()
    for i in range(2):
        gate_w[i] = shares(((1 - side) * 2 + i) * 2 + y)
    for t in far:
        pass_on(1, t)
    for t in near + far:
        tp_copy(peer(t)).wait_recv()
        pick_rows(peer(t))
    for w in range(2):
        for t in near + far + [(0, 0)]:
            g_copy(w, t).wait_recv()

    def pair(s):
        return pl.ds(pl.multiple_of(level(s) * (2 * slots), 2 * slots), 2 * slots)

    order = [2, 3, 1, 0]
    for i, s in enumerate(order):
        gate_act = jnp.dot(picked[pair(s), :], gate_out[0], preferred_element_type=f32)
        up_act = jnp.dot(picked[pair(s), :], up_out[0], preferred_element_type=f32)
        hidden[pair(s), :] = (gate_act / (1.0 + jnp.exp(-gate_act)) * up_act).astype(bf16)
        if i < len(near):
            pass_on(2, near[i])

    def seat(b):
        return pl.ds(pl.multiple_of(b * slots, slots), slots)

    mine = lax.rem(f, quad)

    def stage(st, between):
        at = side if st == 0 else 1 - side
        here = pl.ds(pl.multiple_of(at * span, span), span)

        def wide(q):
            return pl.ds(pl.multiple_of(q * half + at * span, span), span)

        def p_copy(s):
            return remote(part.at[pair(s), wide(1 - p)], held.at[pair(s), here], p_send.at[st, s], p_recv.at[st, s], {"tp": 1 - p})

        def n_copy(t):
            return remote(total.at[seat(peer(t)), here], back.at[seat(mine), here], n_send.at[st, index[t]],
                          n_recv.at[st, index[t]], {"fs": peer(t)})

        def c_copy(t):
            to = door * 2 + (1 - y if t[1] else y)
            return remote(total.at[seat(peer(t)), here], collect.at[lax.rem(level(t[0]), 2), seat(mine), here],
                          c_send.at[st, index[t]], c_recv.at[st, lax.rem(level(t[0]), 2), mine], {"fs": to})

        def o_copy(i):
            to = ((1 - side) * 2 + i) * 2 + y
            return remote(far_out.at[i, :, here], far_in.at[:, here], o_send.at[st, i], o_recv.at[st], {"fs": to})

        def compute(s):
            for q in range(2):
                part[pair(s), wide(q)] = jnp.dot(hidden[pair(s), :], down_out[0, :, wide(q)], preferred_element_type=f32).astype(bf16)

        def add(s):
            p_copy(s).wait_recv()
            total[pair(s), here] = (part[pair(s), wide(p)].astype(f32) + held[pair(s), here].astype(f32)).astype(bf16)

        def give(s):
            for dy in range(2):
                t = (s, dy)
                if s > 1:
                    if dy:
                        c_copy(t).start()
                    else:
                        @pl.when(is_door)
                        def _():
                            collect[lax.rem(level(s), 2), seat(mine), here] = total[seat(peer(t)), here]

                        @pl.when(z != door)
                        def _():
                            c_copy(t).start()
                elif t == (0, 0):
                    back[seat(mine), here] = total[seat(f), here]
                else:
                    n_copy(t).start()

        for i in range(len(order) + 3):
            if i < len(order):
                compute(order[i])
            if 0 <= i - 1 < len(order):
                p_copy(order[i - 1]).start()
            if 0 <= i - 2 < len(order):
                add(order[i - 2])
            if 0 <= i - 3 < len(order):
                give(order[i - 3])
            between(i)

        @pl.when(is_door)
        def _():
            for i in range(2):
                for k in range(1, quad):
                    j = lax.rem(mine + k, quad)
                    block = collect.at[i, seat(j), here]
                    remote(block, block, c_send.at[st, 0], c_recv.at[st, i, j], {"tp": 1 - p}).wait_recv()
                far_out[i, :, here] = jnp.dot(gate_w[i], collect[i, :, here], preferred_element_type=f32).astype(bf16)
            for i in range(2):
                o_copy(i).start()

        def finish():
            for t in near:
                n_copy(t).wait_recv()

        def finish_far():
            there = pl.ds(pl.multiple_of((1 - at) * span, span), span)
            block = far_in.at[:, there]
            remote(block, block, o_send.at[st, 0], o_recv.at[st], {"tp": 1 - p}).wait_recv()

        def drain():
            for s in order:
                p_copy(s).wait_send()
            for t in near:
                n_copy(t).wait_send()
            for t in far:
                if t[1]:
                    c_copy(t).wait_send()
                else:
                    @pl.when(z != door)
                    def _():
                        c_copy(t).wait_send()

            @pl.when(is_door)
            def _():
                for i in range(2):
                    o_copy(i).wait_send()

        return here, finish, finish_far, drain

    for t in near + [(0, 0)]:
        g_copy(2, t).wait_recv()
    here, near_first, far_first, drain_first = stage(0, lambda i: None)
    for t in far:
        pass_on(2, t)
    for t in far:
        g_copy(2, t).wait_recv()
    there, near_last, far_last, drain_last = stage(1, lambda i: None)
    near_first()
    acc = jnp.dot(near_w[...], back[:, here], preferred_element_type=f32)
    near_last()
    more = jnp.dot(near_w[...], back[:, there], preferred_element_type=f32)
    far_first()
    mixed[:, there] = (more + far_in[:, there].astype(f32)).astype(bf16)
    far_last()
    mixed[:, here] = (acc + far_in[:, here].astype(f32)).astype(bf16)

    drain_first()
    drain_last()
    for t in near + far:
        key_copy(t).wait_send()
        tp_copy(peer(t)).wait_send()
    for w in range(3):
        for t in near + far:
            w_copy(w, t).wait_send()
        for t in near + far + [(0, 0)]:
            g_copy(w, t).wait_send()
    line_copy(f, 0, level(1) * 2 + y).wait_send()
    line_copy(f, 1, (2 - side) * 2 + y).wait_send()
    for t in [(0, 0), (1, 0), (2, 0), (3, 0)]:
        y_copy(peer(t)).wait_send()

    @pl.when(is_door)
    def _():
        for i, t in enumerate([(2, 0), (3, 0)]):
            line_copy(peer(t), 2 + i, level(1) * 2 + y).wait_send()


def run_handover(sizes, slots, tokens, norm_gain, gate_train, up_train, down_train, expert_ids, route_score):
    n_gr, n_fs, n_tp = sizes["gr"], sizes["fs"], sizes["tp"]
    _, depth, hid = gate_train.shape
    count, width = tokens.shape
    half, quad = width // n_tp, n_fs // 2
    bf16, f32, dma = jnp.bfloat16, jnp.float32, pltpu.SemaphoreType.DMA
    vmem, hbm = pl.BlockSpec(memory_space=pltpu.VMEM), pl.BlockSpec(memory_space=pl.ANY)
    return pl.pallas_call(
        functools.partial(handover_kernel, sizes),
        out_shape=(
            pltpu.VMEM((1, width, hid), bf16),
            pltpu.VMEM((1, width, hid), bf16),
            pltpu.VMEM((1, hid, width), bf16),
            pltpu.VMEM((count, half), bf16),
        ),
        in_specs=[vmem] * 4 + [hbm] * 3,
        out_specs=[vmem] * 4,
        scratch_shapes=[
            pltpu.VMEM((n_fs, depth, hid), f32), pltpu.VMEM((n_fs, depth, hid), f32), pltpu.VMEM((n_fs, hid, depth), f32),
            pltpu.VMEM((n_fs, depth, hid), bf16), pltpu.VMEM((n_fs, depth, hid), bf16), pltpu.VMEM((n_fs, hid, depth), bf16),
            pltpu.VMEM((n_fs, count, width), bf16), pltpu.VMEM((n_fs, 8, count), f32),
            pltpu.VMEM((n_fs * slots, width), bf16), pltpu.VMEM((n_fs * slots, hid), bf16),
            pltpu.VMEM((n_fs * slots, width), bf16), pltpu.VMEM((n_fs * slots, half), bf16),
            pltpu.VMEM((n_fs * slots, half), bf16), pltpu.VMEM((quad * slots, half), bf16),
            pltpu.VMEM((2, quad * slots, half), bf16), pltpu.VMEM((2, count, half), bf16), pltpu.VMEM((count, half), bf16),
            pltpu.VMEM((count, quad * slots), bf16), pltpu.VMEM((2, count, quad * slots), bf16),
            dma((3,)), dma((3, n_fs)), dma((3, n_fs)), dma((3, n_fs)), dma((3, n_fs)), dma((n_fs,)), dma((4,)), dma((n_fs,)),
            dma((n_fs,)), dma((n_fs,)), dma((n_fs,)), dma((n_fs,)),
            dma((2, 4)), dma((2, 4)), dma((2, n_fs)), dma((2, n_fs)), dma((2, n_fs)), dma((2, 2, quad)),
            dma((2, 2)), dma((2,)),
        ],
        compiler_params=pltpu.CompilerParams(collective_id=2, has_side_effects=True, vmem_limit_bytes=54 * 2**20),
        name="handover",
    )(tokens, norm_gain.reshape(1, depth), expert_ids.T, route_score.T, gate_train, up_train, down_train)


def on_device(sizes, tokens, norm_gain, gate_train, up_train, down_train, expert_ids, route_score):
    n_gr, n_fs, n_tp = sizes["gr"], sizes["fs"], sizes["tp"]
    bf16 = jnp.bfloat16
    experts, depth, hid = gate_train.shape
    local = experts // n_fs
    count, width = tokens.shape
    capacity = 4 * count // experts
    direct_down = depth % 128 == 0
    if direct_down and local == 1 and capacity % 128 == 0 and (n_gr, n_fs, n_tp) == (2, 8, 2):
        return run_handover(sizes, capacity, tokens, norm_gain, gate_train, up_train, down_train, expert_ids, route_score)

    gate_cast = (norm_gain[None, :, None] * gate_train).astype(bf16)
    up_cast = (norm_gain[None, :, None] * up_train).astype(bf16)
    down_cast = down_train.astype(bf16)
    floated = tokens.astype(jnp.float32)
    normed = (floated * lax.rsqrt(jnp.mean(floated * floated, axis=-1, keepdims=True) + epsilon)).astype(bf16)

    named = expert_ids[:, :, None] == jnp.arange(experts, dtype=jnp.int32)
    names = jnp.any(named, axis=1)
    earlier = jnp.arange(count)[:, None] > jnp.arange(count)[None, :]
    rank = jnp.dot(earlier.astype(bf16), names.astype(bf16), preferred_element_type=jnp.float32).astype(jnp.int32)
    slot = expert_ids * capacity + jnp.sum(jnp.where(named, rank[:, None, :], 0), axis=2)
    keys = jnp.concatenate([slot.T, jnp.full((6, count), -1, jnp.int32)], axis=0)

    share = route_score / jnp.sum(route_score, axis=-1, keepdims=True)
    down_shape = (local, hid, n_gr * n_fs * depth) if direct_down else (n_gr * n_fs, local, hid, depth)
    dma = pltpu.SemaphoreType.DMA
    gate_ready, up_ready, down_ready, gathered, all_keys = pl.pallas_call(
        functools.partial(spread_kernel, sizes, local, direct_down),
        out_shape=(
            jax.ShapeDtypeStruct((local, n_gr * n_fs * depth, hid), bf16),
            jax.ShapeDtypeStruct((local, n_gr * n_fs * depth, hid), bf16),
            jax.ShapeDtypeStruct(down_shape, bf16),
            jax.ShapeDtypeStruct((n_fs, count, width), bf16),
            jax.ShapeDtypeStruct((n_fs, 8, count), jnp.int32),
        ),
        in_specs=[pl.BlockSpec(memory_space=pltpu.VMEM)] * 5,
        out_specs=[pl.BlockSpec(memory_space=pl.ANY)] * 5,
        scratch_shapes=[
            dma((3, n_fs)), dma((3, n_fs)), dma((3, n_fs, n_gr)), dma((3, n_fs, n_gr)),
            dma((n_fs,)), dma((n_fs,)), dma((n_fs,)), dma((n_fs,)),
            dma((n_tp, n_fs)), dma((n_tp, n_fs)), dma((n_fs,)), dma((n_fs,)), dma((5,)),
        ],
        compiler_params=pltpu.CompilerParams(collective_id=0, has_side_effects=True),
        name="spread",
    )(gate_cast, up_cast, down_cast, normed, keys)
    if not direct_down:
        down_ready = down_ready.transpose(1, 2, 0, 3).reshape(local, hid, -1)

    wanted = (lax.axis_index("fs") * local * capacity + jnp.arange(local * capacity, dtype=jnp.int32))[None, :, None]
    pick = ((all_keys[:, 0][:, None, :] == wanted) | (all_keys[:, 1][:, None, :] == wanted)).astype(bf16)
    rows = jnp.einsum("sct,std->scd", pick, gathered, preferred_element_type=jnp.float32).astype(bf16)
    rows = rows.reshape(n_fs, local, capacity, width)
    gate_act = jnp.einsum("seck,ekh->sech", rows, gate_ready, preferred_element_type=jnp.float32)
    up_act = jnp.einsum("seck,ekh->sech", rows, up_ready, preferred_element_type=jnp.float32)
    hidden = (jax.nn.silu(gate_act) * up_act).astype(bf16)
    part = jnp.einsum("sech,ehk->seck", hidden, down_ready, preferred_element_type=jnp.float32).astype(bf16)
    part = part.reshape(n_fs, local * capacity, width)
    half = width // n_tp
    returned = pl.pallas_call(
        functools.partial(return_kernel, sizes),
        out_shape=jax.ShapeDtypeStruct((n_fs, local * capacity, half), bf16),
        in_specs=[pl.BlockSpec(memory_space=pltpu.VMEM)],
        out_specs=pl.BlockSpec(memory_space=pltpu.VMEM),
        scratch_shapes=[
            pltpu.VMEM((max(n_tp - 1, 1), n_fs, local * capacity, half), bf16),
            pltpu.VMEM((n_fs, local * capacity, half), bf16),
            dma((n_tp, n_fs)), dma((n_tp, n_fs)), dma((n_fs,)), dma((n_fs,)),
        ],
        compiler_params=pltpu.CompilerParams(collective_id=1, has_side_effects=True),
        name="giveback",
    )(part)
    at = jnp.arange(experts * capacity, dtype=jnp.int32)[None, :]
    weight = jnp.where(slot[:, :1] == at, share[:, :1], 0.0) + jnp.where(slot[:, 1:] == at, share[:, 1:], 0.0)
    mixed = jnp.dot(weight.astype(bf16), returned.reshape(experts * capacity, half), preferred_element_type=jnp.float32)
    return gate_ready, up_ready, down_ready, mixed.astype(bf16)


def solution(mesh):
    return jax.shard_map(
        functools.partial(on_device, dict(mesh.shape)),
        mesh=mesh,
        in_specs=(
            P(("gr", "fs"), None),
            P(("gr", "fs")),
            P(None, ("gr", "fs"), "tp"),
            P(None, ("gr", "fs"), "tp"),
            P(None, "tp", ("gr", "fs")),
            P(("gr", "fs"), None),
            P(("gr", "fs"), None),
        ),
        out_specs=(
            P("fs", None, "tp"),
            P("fs", None, "tp"),
            P("fs", "tp", None),
            P(("gr", "fs"), "tp"),
        ),
        check_vma=False,
    )
```

```python
import functools

import jax
import jax.numpy as jnp
from jax import lax
from jax.experimental import pallas as pl
from jax.experimental.pallas import tpu as pltpu
from jax.sharding import PartitionSpec as P

epsilon = 1e-06
MESH = pl.DeviceIdType.MESH


def remote(src, dst, send_sem, recv_sem, where):
    return pltpu.make_async_remote_copy(
        src_ref=src, dst_ref=dst, send_sem=send_sem, recv_sem=recv_sem, device_id=where, device_id_type=MESH
    )


def greet(sizes):
    barrier = pltpu.get_barrier_semaphore()
    count = 0
    for name, size in sizes.items():
        me = lax.axis_index(name)
        for k in range(1, size):
            pl.semaphore_signal(barrier, inc=1, device_id={name: lax.rem(me + k, size)}, device_id_type=MESH)
            count += 1
    pl.semaphore_wait(barrier, count)


def spread_kernel(sizes, local, direct_down, gate, up, down, rows, keys, gate_out, up_out, down_out, rows_out, keys_out,
                  w_send, w_recv, g_send, g_recv, up_send, low_send, y_send, x_recv, t_send, t_recv, k_send, k_recv, own_sem):
    n_gr, n_fs, n_tp = sizes["gr"], sizes["fs"], sizes["tp"]
    g, f, p = lax.axis_index("gr"), lax.axis_index("fs"), lax.axis_index("tp")
    inner = 2 if n_fs % 2 == 0 else 1
    lines = n_fs // inner
    z, y = f // inner, lax.rem(f, inner)
    depth = gate.shape[1]
    half = rows.shape[1] // n_tp
    cols = pl.ds(pl.multiple_of(p * half, half), half)
    sources, outs = (gate, up, down), (gate_out, up_out, down_out)

    def place(w, block):
        start = pl.multiple_of(block * depth, depth)
        if w < 2:
            return outs[w].at[:, pl.ds(start, depth), :]
        return outs[w].at[:, :, pl.ds(start, depth)] if direct_down else outs[w].at[block]

    greet(sizes)

    own = [pltpu.make_async_copy(rows, rows_out.at[f], own_sem.at[0]),
           pltpu.make_async_copy(keys, keys_out.at[f], own_sem.at[1])]
    for w in range(3):
        own.append(pltpu.make_async_copy(sources[w].at[pl.ds(f * local, local)], place(w, g * n_fs + f), own_sem.at[2 + w]))

    def block_of(b):
        return rows_out.at[b, :, cols]

    def row_copy(b, first, kind, where):
        src = rows.at[:, cols] if first else block_of(b)
        return remote(src, block_of(b), {"u": up_send, "d": low_send, "y": y_send}[kind].at[b], x_recv.at[b], where)

    def tp_copy(b, j):
        return remote(block_of(b), block_of(b), t_send.at[j, b], t_recv.at[j, b], {"tp": lax.rem(p + j + 1, n_tp)})

    def go_up(b, first, act):
        @pl.when(z < lines - 1)
        def _():
            act(row_copy(b, first, "u", {"fs": lax.rem(f + inner, n_fs)}))

    def go_down(b, first, act):
        @pl.when(z > 0)
        def _():
            act(row_copy(b, first, "d", {"fs": lax.rem(f + n_fs - inner, n_fs)}))

    def go_side(b, first, act):
        if inner == 2:
            act(row_copy(b, first, "y", {"fs": f + 1 - 2 * y}))

    def start(c):
        c.start()

    def recv(c):
        c.wait_recv()

    def sent(c):
        c.wait_send()

    go_up(f, True, start)
    go_down(f, True, start)
    go_side(f, True, start)
    key_copies = []
    for k in range(1, n_fs):
        to = lax.rem(f + k, n_fs)
        c = remote(keys, keys_out.at[f], k_send.at[k], k_recv.at[k], {"fs": to})
        c.start()
        key_copies.append(c)
    for c in own:
        c.start()

    def gr_copy(w, b, k, j, first):
        src = sources[w].at[pl.ds(f * local, local)] if first else place(w, b)
        return remote(src, place(w, b), g_send.at[w, k, j], g_recv.at[w, k, j], {"gr": lax.rem(g + j + 1, n_gr)})

    for w in range(3):
        for j in range(n_gr - 1):
            gr_copy(w, g * n_fs + f, 0, j, True).start()

    for s in range(1, lines):
        @pl.when(z >= s)
        def _():
            b = f - s * inner
            row_copy(b, False, "u", {"fs": lax.rem(f + inner, n_fs)}).wait_recv()
            go_up(b, False, start)
            go_side(b, False, start)
            for j in range(n_tp - 1):
                tp_copy(b, j).start()

        @pl.when(z < lines - s)
        def _():
            b = f + s * inner
            row_copy(b, False, "d", {"fs": lax.rem(f + inner, n_fs)}).wait_recv()
            go_down(b, False, start)
            go_side(b, False, start)
            for j in range(n_tp - 1):
                tp_copy(b, j).start()

    def w_copy(w, k):
        to = lax.rem(f + k, n_fs)
        return remote(sources[w].at[pl.ds(to * local, local)], place(w, g * n_fs + f), w_send.at[w, k], w_recv.at[w, k], {"fs": to})

    for w in range(3):
        for k in range(1, n_fs):
            w_copy(w, k).start()

    if inner == 2:
        for s in range(lines):
            b = lax.rem(z + s, lines) * inner + 1 - y
            row_copy(b, False, "y", {"fs": f + 1 - 2 * y}).wait_recv()
            for j in range(n_tp - 1):
                tp_copy(b, j).start()

    for w in range(3):
        for k in range(1, n_fs):
            w_copy(w, k).wait_recv()
            b = g * n_fs + lax.rem(f + n_fs - k, n_fs)
            for j in range(n_gr - 1):
                gr_copy(w, b, k, j, False).start()

    for k in range(1, n_fs):
        b = lax.rem(f + k, n_fs)
        for j in range(n_tp - 1):
            c = tp_copy(b, j)
            c.wait_recv()
            c.wait_send()
    for c in key_copies:
        c.wait_recv()
        c.wait_send()
    for c in own:
        c.wait()
    go_up(f, True, sent)
    go_down(f, True, sent)
    go_side(f, True, sent)
    for s in range(1, lines):
        @pl.when(z >= s)
        def _():
            go_up(f - s * inner, False, sent)
            go_side(f - s * inner, False, sent)

        @pl.when(z < lines - s)
        def _():
            go_down(f + s * inner, False, sent)
            go_side(f + s * inner, False, sent)
    for w in range(3):
        for k in range(n_fs):
            if k:
                w_copy(w, k).wait_send()
            for j in range(n_gr - 1):
                c = gr_copy(w, g * n_fs + lax.rem(f + n_fs - k, n_fs), k, j, False)
                c.wait_recv()
                c.wait_send()


def return_kernel(sizes, part, out, held, total, t_send, t_recv, f_send, f_recv):
    n_fs, n_tp = sizes["fs"], sizes["tp"]
    f, p = lax.axis_index("fs"), lax.axis_index("tp")
    half = part.shape[2] // n_tp

    def cols(q):
        return pl.ds(pl.multiple_of(q * half, half), half)

    greet({"fs": n_fs, "tp": n_tp})
    order = list(range(1, n_fs)) + [0]

    def tp_copy(k, j):
        to = lax.rem(p + j + 1, n_tp)
        b = lax.rem(f + k, n_fs)
        return remote(part.at[b, :, cols(to)], held.at[j, b], t_send.at[j, k], t_recv.at[j, k], {"tp": to})

    def f_copy(k):
        b = lax.rem(f + k, n_fs)
        return remote(total.at[b], out.at[f], f_send.at[k], f_recv.at[k], {"fs": b})

    for k in order:
        for j in range(n_tp - 1):
            tp_copy(k, j).start()
    for k in order:
        b = lax.rem(f + k, n_fs)
        value = part[b, :, cols(p)].astype(jnp.float32)
        for j in range(n_tp - 1):
            tp_copy(k, j).wait_recv()
            value = value + held[j, b].astype(jnp.float32)
        value = value.astype(jnp.bfloat16)
        if k == 0:
            out[b] = value
        else:
            total[b] = value
            f_copy(k).start()
    for k in order:
        for j in range(n_tp - 1):
            tp_copy(k, j).wait_send()
        if k:
            f_copy(k).wait_recv()
            f_copy(k).wait_send()


def handover_kernel(sizes, tokens, gain, ids, score, gate_hbm, up_hbm, down_hbm, gate_out, up_out, down_out, mixed,
                    gate_raw, up_raw, down_raw, gate_cut, up_cut, down_cut, rows_own, line_in, meta, y_pick, picked, hidden,
                    part, held, total, back, collect, far_out, far_in, near_w, gate_w,
                    load_sem, w_send, w_recv, g_send, g_recv, x_send, x_recv, y_send, y_recv, t_send, t_recv, k_send, k_recv,
                    p_send, p_recv, n_send, n_recv, c_send, c_recv, o_send, o_recv):
    n_fs = sizes["fs"]
    g, f, p = lax.axis_index("gr"), lax.axis_index("fs"), lax.axis_index("tp")
    z, y = f // 2, lax.rem(f, 2)
    low, side = lax.rem(z, 2), z // 2
    door = 1 + side
    is_door = z == door
    role = 1 - (low + side - 2 * low * side)
    depth = gate_hbm.shape[1]
    count, width = tokens.shape
    slots = back.shape[0] * 2 // n_fs
    half = width // 2
    span = half // 2
    quad = n_fs // 2
    bf16, f32 = jnp.bfloat16, jnp.float32
    raws, cuts, outs = (gate_raw, up_raw, down_raw), (gate_cut, up_cut, down_cut), (gate_out, up_out, down_out)
    hbms = (gate_hbm, up_hbm, down_hbm)
    near = [(0, 1), (1, 0), (1, 1)]
    far = [(2, 0), (2, 1), (3, 0), (3, 1)]
    index = {t: i for i, t in enumerate(near + far + [(0, 0)])}
    mine = lax.rem(f, quad)

    def level(s):
        return (z, z + 1 - 2 * low, 2 - side, 3 - 3 * side)[s]

    def peer(t):
        return level(t[0]) * 2 + (1 - y if t[1] else y)

    def there(t):
        return index[t] if t[0] < 2 else len(near) + 2 * role + t[1]

    def cols(q):
        return pl.ds(pl.multiple_of(q * half, half), half)

    def seat(b):
        return pl.ds(pl.multiple_of(b * slots, slots), slots)

    def pair(s):
        return pl.ds(pl.multiple_of(level(s) * (2 * slots), 2 * slots), 2 * slots)

    def place(w, block):
        at = pl.ds(pl.multiple_of(block * depth, depth), depth)
        return outs[w].at[0, at, :] if w < 2 else outs[w].at[0, :, at]

    def w_copy(w, t):
        to = peer(t)
        return remote(cuts[w].at[to], place(w, g * n_fs + f), w_send.at[w, index[t]], w_recv.at[w, there(t)], {"fs": to})

    def w_wait(w, t):
        block = place(w, g * n_fs + peer(t))
        remote(block, block, w_send.at[w, index[t]], w_recv.at[w, index[t]], {"fs": peer(t)}).wait_recv()

    def g_copy(w, t):
        b = g * n_fs + peer(t)
        src = cuts[w].at[f] if t == (0, 0) else place(w, b)
        return remote(src, place(w, b), g_send.at[w, index[t]], g_recv.at[w, index[t]], {"gr": 1 - g})

    def pass_on(w, t):
        w_wait(w, t)
        g_copy(w, t).start()

    def row_copy(s):
        if s == 1:
            return remote(rows_own.at[:, cols(p)], line_in.at[0], x_send.at[0], x_recv.at[0], {"fs": peer((1, 0))})
        return remote(rows_own.at[:, cols(p)], line_in.at[1 + role], x_send.at[1], x_recv.at[1 + role], {"fs": peer((2, 0))})

    def end_copy(s):
        return remote(line_in.at[s - 1], line_in.at[s - 1], x_send.at[s], x_recv.at[s - 1], {"fs": peer((1, 0))})

    def y_copy(s):
        return remote(y_pick.at[s], picked.at[seat(peer((s, 0))), cols(p)], y_send.at[s], y_recv.at[s], {"fs": peer((0, 1))})

    def y_wait(s):
        block = picked.at[seat(peer((s, 1))), cols(p)]
        remote(block, block, y_send.at[s], y_recv.at[s], {"fs": peer((0, 1))}).wait_recv()

    def tp_copy(t):
        block = picked.at[seat(peer(t)), cols(p)]
        return remote(block, block, t_send.at[index[t]], t_recv.at[index[t]], {"tp": 1 - p})

    def key_copy(s):
        to = s if s < 2 else 2 + role
        return remote(meta.at[f], meta.at[f], k_send.at[s], k_recv.at[to], {"fs": peer((s, 0))})

    def key_wait(s):
        block = meta.at[peer((s, 0))]
        remote(block, block, k_send.at[s], k_recv.at[s], {"fs": peer((s, 0))}).wait_recv()

    def cut(w):
        pltpu.make_async_copy(hbms[w], raws[w], load_sem.at[w]).wait()
        if w < 2:
            scale = jnp.broadcast_to(gain[...], (128, depth)).T
            for e in range(n_fs):
                for c in range(0, raws[w].shape[2], 128):
                    cuts[w][e, :, c:c + 128] = (scale * raws[w][e, :, c:c + 128]).astype(bf16)
            outs[w][0, pl.ds(pl.multiple_of((g * n_fs + f) * depth, depth), depth), :] = cuts[w][f]
        else:
            for e in range(n_fs):
                cuts[w][e] = raws[w][e].astype(bf16)
            outs[w][0, :, pl.ds(pl.multiple_of((g * n_fs + f) * depth, depth), depth)] = cuts[w][f]

    def pick(b, expert, rows):
        wanted = (expert * slots + lax.broadcasted_iota(jnp.int32, (slots, count), 0)).astype(f32)
        hit = ((meta[b, 0:1, :] == wanted) | (meta[b, 1:2, :] == wanted)).astype(f32).astype(bf16)
        return jnp.dot(hit, rows, preferred_element_type=f32).astype(bf16)

    def shares(b):
        wanted = (side * (quad * slots) + lax.broadcasted_iota(jnp.int32, (quad * slots, count), 0)).astype(f32)
        table = jnp.where(meta[b, 0:1, :] == wanted, meta[b, 2:3, :], 0.0) + jnp.where(
            meta[b, 1:2, :] == wanted, meta[b, 3:4, :], 0.0)
        return table.T.astype(bf16)

    def take_line(s, relay):
        arriving = remote(line_in.at[s - 1], line_in.at[s - 1], x_send.at[0], x_recv.at[s - 1], {"fs": peer((1, 0))})
        arriving.wait_recv()
        if relay:
            end_copy(s).start()
        b = peer((s, 0))
        key_wait(s)
        y_pick[s] = pick(b, peer((0, 1)), line_in[s - 1])
        picked[seat(b), cols(p)] = pick(b, f, line_in[s - 1])
        y_copy(s).start()
        tp_copy((s, 0)).start()

    for w in range(3):
        pltpu.make_async_copy(hbms[w], raws[w], load_sem.at[w]).start()
    barrier = pltpu.get_barrier_semaphore()
    heard = 0
    for name, size in sizes.items():
        me = lax.axis_index(name)
        for k in range(1, size):
            pl.semaphore_signal(barrier, inc=1, device_id={name: lax.rem(me + k, size)}, device_id_type=MESH)
            heard += 1

    expert = lax.broadcasted_iota(jnp.int32, (16, count), 0)
    names = ((ids[0:1, :] == expert) | (ids[1:2, :] == expert)).astype(f32).astype(bf16)
    earlier = lax.broadcasted_iota(jnp.int32, (count, count), 0) < lax.broadcasted_iota(jnp.int32, (count, count), 1)
    rank = jnp.dot(names, earlier.astype(f32).astype(bf16), preferred_element_type=f32) + (expert * slots).astype(f32)
    both = score[0:1, :] + score[1:2, :]
    table = [jnp.sum(jnp.where(ids[k:k + 1, :] == expert, rank, 0.0), axis=0, keepdims=True) for k in range(2)]
    table += [score[k:k + 1, :] / both for k in range(2)]
    for i in range(4):
        meta[f, i:i + 1, :] = table[i]
    meta[f, 4:8, :] = jnp.zeros((4, count), f32)
    for r in range(0, count, 32):
        x = tokens[r:r + 32, :].astype(f32)
        rows_own[r:r + 32, :] = (x * lax.rsqrt(jnp.mean(x * x, axis=-1, keepdims=True) + epsilon)).astype(bf16)
    y_pick[0] = pick(f, peer((0, 1)), rows_own[:, cols(p)])
    pl.semaphore_wait(barrier, heard)
    for s in range(1, 4):
        key_copy(s).start()
    row_copy(1).start()
    row_copy(2).start()
    y_copy(0).start()
    cut(0)
    for t in near:
        w_copy(0, t).start()
    g_copy(0, (0, 0)).start()
    cut(1)
    for w, ts in [(1, near), (0, far), (1, far)]:
        for t in ts:
            w_copy(w, t).start()
    g_copy(1, (0, 0)).start()
    cut(2)
    w_copy(2, (0, 1)).start()
    g_copy(2, (0, 0)).start()

    @pl.when(z != door)
    def _():
        w_copy(2, (1, 0)).start()
        w_copy(2, (1, 1)).start()

    for c in range(0, width, 512):
        picked[seat(f), c:c + 512] = pick(f, f, rows_own[:, c:c + 512])
    near_w[...] = shares(f)
    y_wait(0)
    tp_copy((0, 1)).start()
    pass_on(0, (0, 1))
    pass_on(1, (0, 1))
    take_line(1, False)

    @pl.when(is_door)
    def _():
        take_line(2, True)

    pass_on(0, (1, 0))
    pass_on(0, (1, 1))

    @pl.when(is_door)
    def _():
        take_line(3, True)

    pass_on(1, (1, 0))
    pass_on(1, (1, 1))

    @pl.when(is_door)
    def _():
        for i in range(2):
            gate_w[i] = shares(peer((2 + i, 0)))

    pass_on(0, (3, 0))
    pass_on(0, (3, 1))
    pass_on(0, (2, 0))
    pass_on(0, (2, 1))
    y_wait(1)
    tp_copy((1, 1)).start()

    @pl.when(z != door)
    def _():
        take_line(2, False)


    @pl.when(is_door)
    def _():
        for s in (2, 3):
            y_wait(s)
            tp_copy((s, 1)).start()

    pass_on(2, (0, 1))
    pass_on(1, (3, 0))
    pass_on(1, (3, 1))

    @pl.when(z != door)
    def _():
        take_line(3, False)
        y_wait(2)
        tp_copy((2, 1)).start()

    pass_on(1, (2, 0))
    pass_on(1, (2, 1))

    @pl.when(is_door)
    def _():
        w_copy(2, (1, 0)).start()
        w_copy(2, (1, 1)).start()

    for t in far:
        w_copy(2, t).start()

    @pl.when(z != door)
    def _():
        y_wait(3)
        tp_copy((3, 1)).start()

    for t in near[1:]:
        pass_on(2, t)
    for t in near + far:
        tp_copy(t).wait_recv()
    for w in range(2):
        for t in near + far + [(0, 0)]:
            g_copy(w, t).wait_recv()
    order = [2, 3, 1, 0]

    def act(s):
        gate_act = jnp.dot(picked[pair(s), :], gate_out[0], preferred_element_type=f32)
        up_act = jnp.dot(picked[pair(s), :], up_out[0], preferred_element_type=f32)
        hidden[pair(s), :] = (gate_act / (1.0 + jnp.exp(-gate_act)) * up_act).astype(bf16)

    def here(st, base=0):
        size = span if st == 0 else 2 * depth
        return pl.ds(pl.multiple_of(base + (side * span if st == 0 else level(1 + st) * (2 * depth)), size), size)

    def p_copy(st, s):
        return remote(part.at[pair(s), here(st, (1 - p) * half)], held.at[pair(s), here(st)], p_send.at[st, s], p_recv.at[st, s],
                      {"tp": 1 - p})

    def n_copy(st, t):
        return remote(total.at[seat(peer(t)), here(st)], back.at[seat(mine), here(st)], n_send.at[st, index[t]],
                      n_recv.at[st, index[t]], {"fs": peer(t)})

    def c_copy(st, t):
        return remote(total.at[seat(peer(t)), here(st)], collect.at[t[0] - 2, seat(mine), here(st)], c_send.at[st, index[t]],
                      c_recv.at[st, t[0] - 2, mine], {"fs": door * 2 + (1 - y if t[1] else y)})

    def o_copy(st, i):
        return remote(far_out.at[i, :, here(st)], far_in.at[:, here(st)], o_send.at[st, i], o_recv.at[st], {"fs": peer((2 + i, 0))})

    def stage(st):
        def compute(s):
            for q in range(2):
                part[pair(s), here(st, q * half)] = jnp.dot(
                    hidden[pair(s), :], down_out[0, :, here(st, q * half)], preferred_element_type=f32).astype(bf16)

        def add(s):
            p_copy(st, s).wait_recv()
            total[pair(s), here(st)] = (part[pair(s), here(st, p * half)].astype(f32) + held[pair(s), here(st)].astype(f32)).astype(bf16)

        def give(s):
            for dy in range(2):
                t = (s, dy)
                if t == (0, 0):
                    back[seat(mine), here(st)] = total[seat(f), here(st)]
                elif s == 0:
                    n_copy(st, t).start()
                elif s == 1:
                    pass
                elif dy:
                    c_copy(st, t).start()
                else:
                    @pl.when(is_door)
                    def _():
                        collect[s - 2, seat(mine), here(st)] = total[seat(peer(t)), here(st)]

                    @pl.when(z != door)
                    def _():
                        c_copy(st, t).start()

        for i in range(len(order) + 3):
            if i < len(order):
                if st == 0:
                    act(order[i])
                compute(order[i])
            if 0 <= i - 1 < len(order):
                p_copy(st, order[i - 1]).start()
            if 0 <= i - 2 < len(order):
                add(order[i - 2])
            if 0 <= i - 3 < len(order):
                give(order[i - 3])

    def merge(st):
        @pl.when(is_door)
        def _():
            for i in range(2):
                for k in range(1, quad):
                    j = lax.rem(mine + k, quad)
                    block = collect.at[i, seat(j), here(st)]
                    remote(block, block, c_send.at[st, 0], c_recv.at[st, i, j], {"tp": 1 - p}).wait_recv()
                far_out[i, :, here(st)] = jnp.dot(gate_w[i], collect[i, :, here(st)], preferred_element_type=f32).astype(bf16)
                o_copy(st, i).start()

    def far_wait(st):
        size = span if st == 0 else 2 * depth
        start = (1 - side) * span if st == 0 else (door if st == 1 else 3 * side) * size
        block = far_in.at[:, pl.ds(pl.multiple_of(start, size), size)]
        remote(block, block, o_send.at[st, 0], o_recv.at[st], {"tp": 1 - p}).wait_recv()

    def ready(t):
        g_copy(2, t).wait_recv()

    for t in near + [(0, 0)]:
        ready(t)
    stage(0)
    pass_on(2, (2, 0))
    pass_on(2, (2, 1))
    ready((2, 0))
    ready((2, 1))
    stage(1)
    pass_on(2, (3, 0))
    pass_on(2, (3, 1))
    merge(0)
    ready((3, 0))
    ready((3, 1))
    stage(2)
    for st in range(3):
        n_copy(st, (1, 0)).start()
        n_copy(st, (1, 1)).start()
    merge(1)
    merge(2)
    for t in near:
        n_copy(0, t).wait_recv()
    acc = jnp.dot(near_w[...], back[:, here(0)], preferred_element_type=f32)
    far_wait(0)
    for st in (1, 2):
        for t in near:
            n_copy(st, t).wait_recv()
        more = jnp.dot(near_w[...], back[:, here(st)], preferred_element_type=f32)
        mixed[:, here(st)] = (more + far_in[:, here(st)].astype(f32)).astype(bf16)
    far_wait(1)
    far_wait(2)
    mixed[:, here(0)] = (acc + far_in[:, here(0)].astype(f32)).astype(bf16)
    for st in range(3):
        for s in order:
            p_copy(st, s).wait_send()
        for t in near:
            n_copy(st, t).wait_send()
        for t in far:
            if t[1]:
                c_copy(st, t).wait_send()
    for t in near + far:
        tp_copy(t).wait_send()
    for w in range(3):
        for t in near + far:
            w_copy(w, t).wait_send()
        for t in near + far + [(0, 0)]:
            g_copy(w, t).wait_send()
    for s in range(1, 4):
        key_copy(s).wait_send()
    for s in range(4):
        y_copy(s).wait_send()
    row_copy(1).wait_send()
    row_copy(2).wait_send()

    @pl.when(is_door)
    def _():
        end_copy(2).wait_send()
        end_copy(3).wait_send()
        for st in range(3):
            for i in range(2):
                o_copy(st, i).wait_send()

    @pl.when(z != door)
    def _():
        for st in range(3):
            c_copy(st, (2, 0)).wait_send()
            c_copy(st, (3, 0)).wait_send()


def run_handover(sizes, slots, tokens, norm_gain, gate_train, up_train, down_train, expert_ids, route_score):
    n_gr, n_fs, n_tp = sizes["gr"], sizes["fs"], sizes["tp"]
    _, depth, hid = gate_train.shape
    count, width = tokens.shape
    half, quad = width // n_tp, n_fs // 2
    bf16, f32, dma = jnp.bfloat16, jnp.float32, pltpu.SemaphoreType.DMA
    vmem, hbm = pl.BlockSpec(memory_space=pltpu.VMEM), pl.BlockSpec(memory_space=pl.ANY)
    return pl.pallas_call(
        functools.partial(handover_kernel, sizes),
        out_shape=(
            pltpu.VMEM((1, width, hid), bf16),
            pltpu.VMEM((1, width, hid), bf16),
            pltpu.VMEM((1, hid, width), bf16),
            pltpu.VMEM((count, half), bf16),
        ),
        in_specs=[vmem] * 4 + [hbm] * 3,
        out_specs=[vmem] * 4,
        scratch_shapes=[
            pltpu.VMEM((n_fs, depth, hid), f32), pltpu.VMEM((n_fs, depth, hid), f32), pltpu.VMEM((n_fs, hid, depth), f32),
            pltpu.VMEM((n_fs, depth, hid), bf16), pltpu.VMEM((n_fs, depth, hid), bf16), pltpu.VMEM((n_fs, hid, depth), bf16),
            pltpu.VMEM((count, width), bf16), pltpu.VMEM((3, count, half), bf16), pltpu.VMEM((n_fs, 8, count), f32),
            pltpu.VMEM((4, slots, half), bf16),
            pltpu.VMEM((n_fs * slots, width), bf16), pltpu.VMEM((n_fs * slots, hid), bf16),
            pltpu.VMEM((n_fs * slots, width), bf16), pltpu.VMEM((n_fs * slots, half), bf16),
            pltpu.VMEM((n_fs * slots, half), bf16), pltpu.VMEM((quad * slots, half), bf16),
            pltpu.VMEM((2, quad * slots, half), bf16), pltpu.VMEM((2, count, half), bf16), pltpu.VMEM((count, half), bf16),
            pltpu.VMEM((count, quad * slots), bf16), pltpu.VMEM((2, count, quad * slots), bf16),
            dma((3,)), dma((3, n_fs)), dma((3, n_fs)), dma((3, n_fs)), dma((3, n_fs)), dma((4,)), dma((3,)), dma((4,)), dma((4,)),
            dma((n_fs,)), dma((n_fs,)), dma((4,)), dma((4,)),
            dma((3, 4)), dma((3, 4)), dma((3, n_fs)), dma((3, n_fs)), dma((3, n_fs)), dma((3, 2, quad)),
            dma((3, 2)), dma((3,)),
        ],
        compiler_params=pltpu.CompilerParams(collective_id=2, has_side_effects=True, vmem_limit_bytes=54 * 2**20),
        name="handover",
    )(tokens, norm_gain.reshape(1, depth), expert_ids.T, route_score.T, gate_train, up_train, down_train)


def on_device(sizes, tokens, norm_gain, gate_train, up_train, down_train, expert_ids, route_score):
    n_gr, n_fs, n_tp = sizes["gr"], sizes["fs"], sizes["tp"]
    bf16 = jnp.bfloat16
    experts, depth, hid = gate_train.shape
    local = experts // n_fs
    count, width = tokens.shape
    capacity = 4 * count // experts
    direct_down = depth % 128 == 0
    if direct_down and local == 1 and capacity % 128 == 0 and (n_gr, n_fs, n_tp) == (2, 8, 2):
        return run_handover(sizes, capacity, tokens, norm_gain, gate_train, up_train, down_train, expert_ids, route_score)

    gate_cast = (norm_gain[None, :, None] * gate_train).astype(bf16)
    up_cast = (norm_gain[None, :, None] * up_train).astype(bf16)
    down_cast = down_train.astype(bf16)
    floated = tokens.astype(jnp.float32)
    normed = (floated * lax.rsqrt(jnp.mean(floated * floated, axis=-1, keepdims=True) + epsilon)).astype(bf16)

    named = expert_ids[:, :, None] == jnp.arange(experts, dtype=jnp.int32)
    names = jnp.any(named, axis=1)
    earlier = jnp.arange(count)[:, None] > jnp.arange(count)[None, :]
    rank = jnp.dot(earlier.astype(bf16), names.astype(bf16), preferred_element_type=jnp.float32).astype(jnp.int32)
    slot = expert_ids * capacity + jnp.sum(jnp.where(named, rank[:, None, :], 0), axis=2)
    keys = jnp.concatenate([slot.T, jnp.full((6, count), -1, jnp.int32)], axis=0)

    share = route_score / jnp.sum(route_score, axis=-1, keepdims=True)
    down_shape = (local, hid, n_gr * n_fs * depth) if direct_down else (n_gr * n_fs, local, hid, depth)
    dma = pltpu.SemaphoreType.DMA
    gate_ready, up_ready, down_ready, gathered, all_keys = pl.pallas_call(
        functools.partial(spread_kernel, sizes, local, direct_down),
        out_shape=(
            jax.ShapeDtypeStruct((local, n_gr * n_fs * depth, hid), bf16),
            jax.ShapeDtypeStruct((local, n_gr * n_fs * depth, hid), bf16),
            jax.ShapeDtypeStruct(down_shape, bf16),
            jax.ShapeDtypeStruct((n_fs, count, width), bf16),
            jax.ShapeDtypeStruct((n_fs, 8, count), jnp.int32),
        ),
        in_specs=[pl.BlockSpec(memory_space=pltpu.VMEM)] * 5,
        out_specs=[pl.BlockSpec(memory_space=pl.ANY)] * 5,
        scratch_shapes=[
            dma((3, n_fs)), dma((3, n_fs)), dma((3, n_fs, n_gr)), dma((3, n_fs, n_gr)),
            dma((n_fs,)), dma((n_fs,)), dma((n_fs,)), dma((n_fs,)),
            dma((n_tp, n_fs)), dma((n_tp, n_fs)), dma((n_fs,)), dma((n_fs,)), dma((5,)),
        ],
        compiler_params=pltpu.CompilerParams(collective_id=0, has_side_effects=True),
        name="spread",
    )(gate_cast, up_cast, down_cast, normed, keys)
    if not direct_down:
        down_ready = down_ready.transpose(1, 2, 0, 3).reshape(local, hid, -1)

    wanted = (lax.axis_index("fs") * local * capacity + jnp.arange(local * capacity, dtype=jnp.int32))[None, :, None]
    pick = ((all_keys[:, 0][:, None, :] == wanted) | (all_keys[:, 1][:, None, :] == wanted)).astype(bf16)
    rows = jnp.einsum("sct,std->scd", pick, gathered, preferred_element_type=jnp.float32).astype(bf16)
    rows = rows.reshape(n_fs, local, capacity, width)
    gate_act = jnp.einsum("seck,ekh->sech", rows, gate_ready, preferred_element_type=jnp.float32)
    up_act = jnp.einsum("seck,ekh->sech", rows, up_ready, preferred_element_type=jnp.float32)
    hidden = (jax.nn.silu(gate_act) * up_act).astype(bf16)
    part = jnp.einsum("sech,ehk->seck", hidden, down_ready, preferred_element_type=jnp.float32).astype(bf16)
    part = part.reshape(n_fs, local * capacity, width)
    half = width // n_tp
    returned = pl.pallas_call(
        functools.partial(return_kernel, sizes),
        out_shape=jax.ShapeDtypeStruct((n_fs, local * capacity, half), bf16),
        in_specs=[pl.BlockSpec(memory_space=pltpu.VMEM)],
        out_specs=pl.BlockSpec(memory_space=pltpu.VMEM),
        scratch_shapes=[
            pltpu.VMEM((max(n_tp - 1, 1), n_fs, local * capacity, half), bf16),
            pltpu.VMEM((n_fs, local * capacity, half), bf16),
            dma((n_tp, n_fs)), dma((n_tp, n_fs)), dma((n_fs,)), dma((n_fs,)),
        ],
        compiler_params=pltpu.CompilerParams(collective_id=1, has_side_effects=True),
        name="giveback",
    )(part)
    at = jnp.arange(experts * capacity, dtype=jnp.int32)[None, :]
    weight = jnp.where(slot[:, :1] == at, share[:, :1], 0.0) + jnp.where(slot[:, 1:] == at, share[:, 1:], 0.0)
    mixed = jnp.dot(weight.astype(bf16), returned.reshape(experts * capacity, half), preferred_element_type=jnp.float32)
    return gate_ready, up_ready, down_ready, mixed.astype(bf16)


def solution(mesh):
    return jax.shard_map(
        functools.partial(on_device, dict(mesh.shape)),
        mesh=mesh,
        in_specs=(
            P(("gr", "fs"), None),
            P(("gr", "fs")),
            P(None, ("gr", "fs"), "tp"),
            P(None, ("gr", "fs"), "tp"),
            P(None, "tp", ("gr", "fs")),
            P(("gr", "fs"), None),
            P(("gr", "fs"), None),
        ),
        out_specs=(
            P("fs", None, "tp"),
            P("fs", None, "tp"),
            P("fs", "tp", None),
            P(("gr", "fs"), "tp"),
        ),
        check_vma=False,
    )
```

```python
import functools

import jax
import jax.numpy as jnp
from jax import lax
from jax.experimental import pallas as pl
from jax.experimental.pallas import tpu as pltpu
from jax.sharding import PartitionSpec as P

epsilon = 1e-06
MESH = pl.DeviceIdType.MESH


def remote(src, dst, send_sem, recv_sem, where):
    return pltpu.make_async_remote_copy(
        src_ref=src, dst_ref=dst, send_sem=send_sem, recv_sem=recv_sem, device_id=where, device_id_type=MESH
    )


def greet(sizes):
    barrier = pltpu.get_barrier_semaphore()
    count = 0
    for name, size in sizes.items():
        me = lax.axis_index(name)
        for k in range(1, size):
            pl.semaphore_signal(barrier, inc=1, device_id={name: lax.rem(me + k, size)}, device_id_type=MESH)
            count += 1
    pl.semaphore_wait(barrier, count)


def spread_kernel(sizes, local, direct_down, gate, up, down, rows, keys, gate_out, up_out, down_out, rows_out, keys_out,
                  w_send, w_recv, g_send, g_recv, up_send, low_send, y_send, x_recv, t_send, t_recv, k_send, k_recv, own_sem):
    n_gr, n_fs, n_tp = sizes["gr"], sizes["fs"], sizes["tp"]
    g, f, p = lax.axis_index("gr"), lax.axis_index("fs"), lax.axis_index("tp")
    inner = 2 if n_fs % 2 == 0 else 1
    lines = n_fs // inner
    z, y = f // inner, lax.rem(f, inner)
    depth = gate.shape[1]
    half = rows.shape[1] // n_tp
    cols = pl.ds(pl.multiple_of(p * half, half), half)
    sources, outs = (gate, up, down), (gate_out, up_out, down_out)

    def place(w, block):
        start = pl.multiple_of(block * depth, depth)
        if w < 2:
            return outs[w].at[:, pl.ds(start, depth), :]
        return outs[w].at[:, :, pl.ds(start, depth)] if direct_down else outs[w].at[block]

    greet(sizes)

    own = [pltpu.make_async_copy(rows, rows_out.at[f], own_sem.at[0]),
           pltpu.make_async_copy(keys, keys_out.at[f], own_sem.at[1])]
    for w in range(3):
        own.append(pltpu.make_async_copy(sources[w].at[pl.ds(f * local, local)], place(w, g * n_fs + f), own_sem.at[2 + w]))

    def block_of(b):
        return rows_out.at[b, :, cols]

    def row_copy(b, first, kind, where):
        src = rows.at[:, cols] if first else block_of(b)
        return remote(src, block_of(b), {"u": up_send, "d": low_send, "y": y_send}[kind].at[b], x_recv.at[b], where)

    def tp_copy(b, j):
        return remote(block_of(b), block_of(b), t_send.at[j, b], t_recv.at[j, b], {"tp": lax.rem(p + j + 1, n_tp)})

    def go_up(b, first, act):
        @pl.when(z < lines - 1)
        def _():
            act(row_copy(b, first, "u", {"fs": lax.rem(f + inner, n_fs)}))

    def go_down(b, first, act):
        @pl.when(z > 0)
        def _():
            act(row_copy(b, first, "d", {"fs": lax.rem(f + n_fs - inner, n_fs)}))

    def go_side(b, first, act):
        if inner == 2:
            act(row_copy(b, first, "y", {"fs": f + 1 - 2 * y}))

    def start(c):
        c.start()

    def recv(c):
        c.wait_recv()

    def sent(c):
        c.wait_send()

    go_up(f, True, start)
    go_down(f, True, start)
    go_side(f, True, start)
    key_copies = []
    for k in range(1, n_fs):
        to = lax.rem(f + k, n_fs)
        c = remote(keys, keys_out.at[f], k_send.at[k], k_recv.at[k], {"fs": to})
        c.start()
        key_copies.append(c)
    for c in own:
        c.start()

    def gr_copy(w, b, k, j, first):
        src = sources[w].at[pl.ds(f * local, local)] if first else place(w, b)
        return remote(src, place(w, b), g_send.at[w, k, j], g_recv.at[w, k, j], {"gr": lax.rem(g + j + 1, n_gr)})

    for w in range(3):
        for j in range(n_gr - 1):
            gr_copy(w, g * n_fs + f, 0, j, True).start()

    for s in range(1, lines):
        @pl.when(z >= s)
        def _():
            b = f - s * inner
            row_copy(b, False, "u", {"fs": lax.rem(f + inner, n_fs)}).wait_recv()
            go_up(b, False, start)
            go_side(b, False, start)
            for j in range(n_tp - 1):
                tp_copy(b, j).start()

        @pl.when(z < lines - s)
        def _():
            b = f + s * inner
            row_copy(b, False, "d", {"fs": lax.rem(f + inner, n_fs)}).wait_recv()
            go_down(b, False, start)
            go_side(b, False, start)
            for j in range(n_tp - 1):
                tp_copy(b, j).start()

    def w_copy(w, k):
        to = lax.rem(f + k, n_fs)
        return remote(sources[w].at[pl.ds(to * local, local)], place(w, g * n_fs + f), w_send.at[w, k], w_recv.at[w, k], {"fs": to})

    for w in range(3):
        for k in range(1, n_fs):
            w_copy(w, k).start()

    if inner == 2:
        for s in range(lines):
            b = lax.rem(z + s, lines) * inner + 1 - y
            row_copy(b, False, "y", {"fs": f + 1 - 2 * y}).wait_recv()
            for j in range(n_tp - 1):
                tp_copy(b, j).start()

    for w in range(3):
        for k in range(1, n_fs):
            w_copy(w, k).wait_recv()
            b = g * n_fs + lax.rem(f + n_fs - k, n_fs)
            for j in range(n_gr - 1):
                gr_copy(w, b, k, j, False).start()

    for k in range(1, n_fs):
        b = lax.rem(f + k, n_fs)
        for j in range(n_tp - 1):
            c = tp_copy(b, j)
            c.wait_recv()
            c.wait_send()
    for c in key_copies:
        c.wait_recv()
        c.wait_send()
    for c in own:
        c.wait()
    go_up(f, True, sent)
    go_down(f, True, sent)
    go_side(f, True, sent)
    for s in range(1, lines):
        @pl.when(z >= s)
        def _():
            go_up(f - s * inner, False, sent)
            go_side(f - s * inner, False, sent)

        @pl.when(z < lines - s)
        def _():
            go_down(f + s * inner, False, sent)
            go_side(f + s * inner, False, sent)
    for w in range(3):
        for k in range(n_fs):
            if k:
                w_copy(w, k).wait_send()
            for j in range(n_gr - 1):
                c = gr_copy(w, g * n_fs + lax.rem(f + n_fs - k, n_fs), k, j, False)
                c.wait_recv()
                c.wait_send()


def return_kernel(sizes, part, out, held, total, t_send, t_recv, f_send, f_recv):
    n_fs, n_tp = sizes["fs"], sizes["tp"]
    f, p = lax.axis_index("fs"), lax.axis_index("tp")
    half = part.shape[2] // n_tp

    def cols(q):
        return pl.ds(pl.multiple_of(q * half, half), half)

    greet({"fs": n_fs, "tp": n_tp})
    order = list(range(1, n_fs)) + [0]

    def tp_copy(k, j):
        to = lax.rem(p + j + 1, n_tp)
        b = lax.rem(f + k, n_fs)
        return remote(part.at[b, :, cols(to)], held.at[j, b], t_send.at[j, k], t_recv.at[j, k], {"tp": to})

    def f_copy(k):
        b = lax.rem(f + k, n_fs)
        return remote(total.at[b], out.at[f], f_send.at[k], f_recv.at[k], {"fs": b})

    for k in order:
        for j in range(n_tp - 1):
            tp_copy(k, j).start()
    for k in order:
        b = lax.rem(f + k, n_fs)
        value = part[b, :, cols(p)].astype(jnp.float32)
        for j in range(n_tp - 1):
            tp_copy(k, j).wait_recv()
            value = value + held[j, b].astype(jnp.float32)
        value = value.astype(jnp.bfloat16)
        if k == 0:
            out[b] = value
        else:
            total[b] = value
            f_copy(k).start()
    for k in order:
        for j in range(n_tp - 1):
            tp_copy(k, j).wait_send()
        if k:
            f_copy(k).wait_recv()
            f_copy(k).wait_send()


def handover_kernel(sizes, tokens_hbm, gain_hbm, ids_hbm, score_hbm, gate_hbm, up_hbm, down_hbm, gate_out, up_out, down_out, mixed,
                    tokens, gain, ids, score, gate_raw, up_raw, down_raw, gate_cut, up_cut, down_cut, rows_own, line_in, meta, y_pick,
                    picked, hidden, part, held, total, back, collect, far_out, far_in, near_w, gate_w,
                    load_sem, w_send, w_recv, g_send, g_recv, d_recv, x_send, x_recv, y_recv, k_recv, p_recv, n_recv, c_recv, o_recv):
    n_fs = sizes["fs"]
    g, f, p = lax.axis_index("gr"), lax.axis_index("fs"), lax.axis_index("tp")
    z, y = f // 2, lax.rem(f, 2)
    low, side = lax.rem(z, 2), z // 2
    door = 1 + side
    is_door = z == door
    role = 1 - (low + side - 2 * low * side)
    depth = gate_hbm.shape[1]
    count, width = tokens.shape
    slots = back.shape[0] * 2 // n_fs
    half = width // 2
    span = half // 2
    strip = 2 * depth
    quad = n_fs // 2
    bf16, f32 = jnp.bfloat16, jnp.float32
    raws, cuts, outs = (gate_raw, up_raw, down_raw), (gate_cut, up_cut, down_cut), (gate_out, up_out, down_out)
    hbms = (gate_hbm, up_hbm, down_hbm)
    near = [(0, 1), (1, 0), (1, 1)]
    far = [(2, 0), (2, 1), (3, 0), (3, 1)]
    index = {t: i for i, t in enumerate(near + far)}
    mine = lax.rem(f, quad)
    rows_send, relay_send, y_send, t_send, k_send, p_send, n_send, c_send, e_send, o_send, t_recv = [x_send.at[i] for i in range(11)]

    def at_door(act, otherwise=None):
        @pl.when(is_door)
        def _():
            act()

        if otherwise is not None:
            at_end(otherwise)

    def at_end(act):
        @pl.when(z != door)
        def _():
            act()

    def level(s):
        return (z, z + 1 - 2 * low, 2 - side, 3 - 3 * side)[s]

    def peer(t):
        return level(t[0]) * 2 + (1 - y if t[1] else y)

    def there(t):
        return index[t] if t[0] < 2 else len(near) + 2 * role + t[1]

    def cols(q):
        return pl.ds(pl.multiple_of(q * half, half), half)

    def seat(b):
        return pl.ds(pl.multiple_of(b * slots, slots), slots)

    def pair(s):
        return pl.ds(pl.multiple_of(level(s) * (2 * slots), 2 * slots), 2 * slots)

    def place(w, block):
        at = pl.ds(pl.multiple_of(block * depth, depth), depth)
        return outs[w].at[0, at, :] if w < 2 else outs[w].at[0, :, at]

    def local(block, send, recv):
        return remote(block, block, send, recv, {"tp": 1 - p})

    def w_copy(w, t):
        to = peer(t)
        return remote(cuts[w].at[to], place(w, g * n_fs + f), w_send.at[w], w_recv.at[w, there(t)], {"fs": to})

    def g_copy(w, t):
        b = g * n_fs + peer(t)
        src = cuts[w].at[f] if t == (0, 0) else place(w, b)
        return remote(src, place(w, b), g_send.at[w], g_recv.at[w] if w < 2 else d_recv.at[t[0]], {"gr": 1 - g})

    def pass_on(w, *ts):
        for t in ts:
            local(place(w, g * n_fs + peer(t)), w_send.at[w], w_recv.at[w, index[t]]).wait_recv()
            g_copy(w, t).start()

    def ready(s):
        local(down_out.at[0, :, pl.ds(0, strip)], g_send.at[2], d_recv.at[s]).wait_recv()

    def row_copy(s):
        if s == 1:
            return remote(rows_own.at[:, cols(p)], line_in.at[0], rows_send, x_recv.at[0], {"fs": peer((1, 0))})
        return remote(rows_own.at[:, cols(p)], line_in.at[1 + role], rows_send, x_recv.at[1 + role], {"fs": peer((2, 0))})

    def relay_copy(s):
        return remote(line_in.at[s - 1], line_in.at[s - 1], relay_send, x_recv.at[s - 1], {"fs": peer((1, 0))})

    def y_copy(s):
        return remote(y_pick.at[s], picked.at[seat(peer((s, 0))), cols(p)], y_send, y_recv.at[s], {"fs": peer((0, 1))})

    def tp_copy(t):
        block = picked.at[seat(peer(t)), cols(p)]
        return remote(block, block, t_send, t_recv, {"tp": 1 - p})

    def take_y(s):
        local(picked.at[seat(peer((s, 1))), cols(p)], y_send, y_recv.at[s]).wait_recv()
        tp_copy((s, 1)).start()

    def key_copy(s):
        return remote(meta.at[f], meta.at[f], k_send, k_recv.at[s if s < 2 else 2 + role], {"fs": peer((s, 0))})

    def cut(w):
        pltpu.make_async_copy(hbms[w], raws[w], load_sem.at[w]).wait()
        if w < 2:
            scale = jnp.broadcast_to(gain[...], (128, depth)).T
            for e in range(n_fs):
                for c in range(0, raws[w].shape[2], 128):
                    cuts[w][e, :, c:c + 128] = (scale * raws[w][e, :, c:c + 128]).astype(bf16)
            outs[w][0, pl.ds(pl.multiple_of((g * n_fs + f) * depth, depth), depth), :] = cuts[w][f]
        else:
            for e in range(n_fs):
                cuts[w][e] = raws[w][e].astype(bf16)
            outs[w][0, :, pl.ds(pl.multiple_of((g * n_fs + f) * depth, depth), depth)] = cuts[w][f]

    def pick(b, expert, rows):
        wanted = (expert * slots + lax.broadcasted_iota(jnp.int32, (slots, count), 0)).astype(f32)
        hit = ((meta[b, 0:1, :] == wanted) | (meta[b, 1:2, :] == wanted)).astype(f32).astype(bf16)
        return jnp.dot(hit, rows, preferred_element_type=f32).astype(bf16)

    def shares(b):
        wanted = (side * (quad * slots) + lax.broadcasted_iota(jnp.int32, (quad * slots, count), 0)).astype(f32)
        table = jnp.where(meta[b, 0:1, :] == wanted, meta[b, 2:3, :], 0.0) + jnp.where(
            meta[b, 1:2, :] == wanted, meta[b, 3:4, :], 0.0)
        return table.T.astype(bf16)

    def take_line(s, relay):
        local(line_in.at[s - 1], rows_send, x_recv.at[s - 1]).wait_recv()
        if relay:
            relay_copy(s).start()
        b = peer((s, 0))
        local(meta.at[b], k_send, k_recv.at[s]).wait_recv()
        y_pick[s] = pick(b, peer((0, 1)), line_in[s - 1])
        picked[seat(b), cols(p)] = pick(b, f, line_in[s - 1])
        y_copy(s).start()
        tp_copy((s, 0)).start()

    barrier = pltpu.get_barrier_semaphore()
    heard = 0
    for name, size in sizes.items():
        me = lax.axis_index(name)
        for k in range(1, size):
            pl.semaphore_signal(barrier, inc=1, device_id={name: lax.rem(me + k, size)}, device_id_type=MESH)
            heard += 1
    loads = [pltpu.make_async_copy(src, dst, load_sem.at[3 + i]) for i, (src, dst) in enumerate(
        [(ids_hbm, ids), (score_hbm, score), (tokens_hbm, tokens), (gain_hbm, gain)])]
    for c in loads:
        c.start()
    for w in range(3):
        pltpu.make_async_copy(hbms[w], raws[w], load_sem.at[w]).start()
    loads[0].wait()
    loads[1].wait()
    expert = lax.broadcasted_iota(jnp.int32, (16, count), 0)
    names = ((ids[0:1, :] == expert) | (ids[1:2, :] == expert)).astype(f32).astype(bf16)
    earlier = lax.broadcasted_iota(jnp.int32, (count, count), 0) < lax.broadcasted_iota(jnp.int32, (count, count), 1)
    rank = jnp.dot(names, earlier.astype(f32).astype(bf16), preferred_element_type=f32) + (expert * slots).astype(f32)
    both = score[0:1, :] + score[1:2, :]
    table = [jnp.sum(jnp.where(ids[k:k + 1, :] == expert, rank, 0.0), axis=0, keepdims=True) for k in range(2)]
    table += [score[k:k + 1, :] / both for k in range(2)]
    for i in range(4):
        meta[f, i:i + 1, :] = table[i]
    meta[f, 4:8, :] = jnp.zeros((4, count), f32)
    loads[2].wait()
    loads[3].wait()
    for r in range(0, count, 32):
        x = tokens[r:r + 32, :].astype(f32)
        rows_own[r:r + 32, :] = (x * lax.rsqrt(jnp.mean(x * x, axis=-1, keepdims=True) + epsilon)).astype(bf16)
    y_pick[0] = pick(f, peer((0, 1)), rows_own[:, cols(p)])
    pl.semaphore_wait(barrier, heard)
    for s in range(1, 4):
        key_copy(s).start()
    row_copy(1).start()
    row_copy(2).start()
    y_copy(0).start()
    cut(0)
    for t in near:
        w_copy(0, t).start()
    g_copy(0, (0, 0)).start()
    cut(1)
    for w, ts in [(1, near), (0, far), (1, far)]:
        for t in ts:
            w_copy(w, t).start()
    g_copy(1, (0, 0)).start()
    cut(2)
    w_copy(2, (0, 1)).start()
    g_copy(2, (0, 0)).start()

    def early_down():
        w_copy(2, (1, 0)).start()
        w_copy(2, (1, 1)).start()

    at_end(early_down)
    for c in range(0, width, 512):
        picked[seat(f), c:c + 512] = pick(f, f, rows_own[:, c:c + 512])
    near_w[...] = shares(f)
    take_y(0)
    pass_on(0, (0, 1))
    pass_on(1, (0, 1))
    take_line(1, False)
    at_door(lambda: take_line(2, True))
    pass_on(0, (1, 0), (1, 1))
    at_door(lambda: take_line(3, True))
    pass_on(1, (1, 0), (1, 1))

    def gate_shares():
        for i in range(2):
            gate_w[i] = shares(peer((2 + i, 0)))

    at_door(gate_shares)
    pass_on(0, (3, 0), (3, 1))
    pass_on(0, (2, 0))
    at_end(lambda: take_line(2, False))
    at_door(lambda: pass_on(0, (2, 1)))
    take_y(1)

    def take_both():
        take_y(2)
        take_y(3)

    at_door(take_both)
    pass_on(2, (0, 1))
    pass_on(1, (3, 0), (3, 1))
    at_end(lambda: pass_on(0, (2, 1)))
    at_end(lambda: take_line(3, False))
    at_end(lambda: take_y(2))
    pass_on(1, (2, 0), (2, 1))
    at_door(early_down)
    for t in far:
        w_copy(2, t).start()
    at_end(lambda: take_y(3))
    at_door(lambda: pass_on(2, (1, 0), (1, 1)))
    local(picked.at[pl.ds(0, (n_fs - 1) * slots), pl.ds(0, half)], t_send, t_recv).wait_recv()
    for w in range(2):
        local(outs[w].at[0, pl.ds(0, n_fs * depth), :], g_send.at[w], g_recv.at[w]).wait_recv()
    order = [2, 3, 1, 0]

    def act(s):
        gate_act = jnp.dot(picked[pair(s), :], gate_out[0], preferred_element_type=f32)
        up_act = jnp.dot(picked[pair(s), :], up_out[0], preferred_element_type=f32)
        hidden[pair(s), :] = (gate_act / (1.0 + jnp.exp(-gate_act)) * up_act).astype(bf16)

    def here(st, base=0):
        layer = (3 * side, door, 2 - side, 3 - 3 * side)[st]
        return pl.ds(pl.multiple_of(base + layer * strip, strip), strip)

    def p_copy(st, s):
        return remote(part.at[pair(s), here(st, (1 - p) * half)], held.at[pair(s), here(st)], p_send, p_recv.at[st, s], {"tp": 1 - p})

    def n_copy(st, t):
        return remote(total.at[seat(peer(t)), here(st)], back.at[seat(mine), here(st)], n_send, n_recv.at[max(st - 1, 0)],
                      {"fs": peer(t)})

    def c_copy(st, t):
        return remote(total.at[seat(peer(t)), here(st)], collect.at[t[0] - 2, seat(mine), here(st)], c_send if t[1] else e_send,
                      c_recv.at[st, t[0] - 2], {"fs": door * 2 + (1 - y if t[1] else y)})

    def o_copy(st, i):
        return remote(far_out.at[i, :, here(st)], far_in.at[:, here(st)], o_send, o_recv.at[st], {"fs": peer((2 + i, 0))})

    def compute(st):
        for i, s in enumerate(order):
            if st == 0:
                act(s)
            for q in range(2):
                part[pair(s), here(st, q * half)] = jnp.dot(
                    hidden[pair(s), :], down_out[0, :, here(st, q * half)], preferred_element_type=f32).astype(bf16)
            if i:
                p_copy(st, order[i - 1]).start()
        p_copy(st, order[-1]).start()

    def give(st):
        def send(s):
            for dy in range(2):
                t = (s, dy)
                if t == (0, 0):
                    back[seat(mine), here(st)] = total[seat(f), here(st)]
                elif s == 0:
                    n_copy(st, t).start()
                elif dy and s > 1:
                    c_copy(st, t).start()
                elif s > 1:
                    def keep():
                        collect[s - 2, seat(mine), here(st)] = total[seat(peer(t)), here(st)]

                    at_door(keep, lambda: c_copy(st, t).start())

        for i, s in enumerate(order):
            p_copy(st, s).wait_recv()
            total[pair(s), here(st)] = (part[pair(s), here(st, p * half)].astype(f32) + held[pair(s), here(st)].astype(f32)).astype(bf16)
            if i:
                send(order[i - 1])
        send(order[-1])

    def give_near(st):
        n_copy(st, (1, 0)).start()
        n_copy(st, (1, 1)).start()

    def merge(st):
        def act():
            for i in range(2):
                local(collect.at[i, pl.ds(0, (quad - 1) * slots), here(st)], c_send, c_recv.at[st, i]).wait_recv()
                far_out[i, :, here(st)] = jnp.dot(gate_w[i], collect[i, :, here(st)], preferred_element_type=f32).astype(bf16)
                o_copy(st, i).start()

        at_door(act)

    def far_wait(st):
        layer = (3 - 3 * side, 2 - side, door, 3 * side)[st]
        local(far_in.at[:, pl.ds(pl.multiple_of(layer * strip, strip), strip)], o_send, o_recv.at[st]).wait_recv()

    at_door(lambda: ready(1), lambda: ready(0))
    compute(0)
    give(0)

    def late_down():
        pass_on(2, (1, 0), (1, 1))
        ready(1)

    at_door(lambda: ready(0), late_down)
    compute(1)
    pass_on(2, (2, 0), (2, 1))
    give(1)
    give_near(0)
    give_near(1)
    merge(0)
    pass_on(2, (3, 0), (3, 1))
    ready(2)
    compute(2)
    merge(1)
    give(2)
    ready(3)
    compute(3)
    give(3)
    give_near(2)
    give_near(3)
    merge(2)
    merge(3)
    local(back.at[pl.ds(0, 3 * slots // 2), :], n_send, n_recv.at[0]).wait_recv()
    sided = pl.ds(pl.multiple_of(side * span, span), span)
    acc = jnp.dot(near_w[...], back[:, sided], preferred_element_type=f32)
    far_wait(0)
    far_wait(1)
    for st in (2, 3):
        local(back.at[pl.ds(0, 3 * slots // 4), :], n_send, n_recv.at[st - 1]).wait_recv()
        more = jnp.dot(near_w[...], back[:, here(st)], preferred_element_type=f32)
        mixed[:, here(st)] = (more + far_in[:, here(st)].astype(f32)).astype(bf16)
    far_wait(2)
    far_wait(3)
    mixed[:, sided] = (acc + far_in[:, sided].astype(f32)).astype(bf16)

    def sent(block, send):
        local(block, send, o_recv.at[0]).wait_send()

    for w in range(3):
        sent(cuts[w].at[pl.ds(0, n_fs - 1)], w_send.at[w])
        sent(cuts[w], g_send.at[w])
    sent(rows_own, rows_send)
    sent(y_pick, y_send)
    sent(picked.at[pl.ds(0, (n_fs - 1) * slots), pl.ds(0, half)], t_send)
    sent(meta.at[pl.ds(0, 3)], k_send)
    sent(held, p_send)
    sent(held.at[pl.ds(0, 3 * slots), :], n_send)
    sent(held.at[pl.ds(0, 2 * slots), :], c_send)
    at_door(lambda: sent(line_in.at[pl.ds(0, 2)], relay_send), lambda: sent(held.at[pl.ds(0, 2 * slots), :], e_send))
    at_door(lambda: sent(far_out, o_send))


def store_kernel(*refs):
    sems = refs[-1]
    pairs = list(zip(refs[:4], refs[4:8]))
    copies = [pltpu.make_async_copy(src, dst, sems.at[i]) for i, (src, dst) in enumerate(pairs)]
    for c in copies:
        c.start()
    for c in copies:
        c.wait()


def run_handover(sizes, slots, tokens, norm_gain, gate_train, up_train, down_train, expert_ids, route_score):
    n_gr, n_fs, n_tp = sizes["gr"], sizes["fs"], sizes["tp"]
    _, depth, hid = gate_train.shape
    count, width = tokens.shape
    half, quad = width // n_tp, n_fs // 2
    bf16, f32, dma = jnp.bfloat16, jnp.float32, pltpu.SemaphoreType.DMA
    vmem, hbm = pl.BlockSpec(memory_space=pltpu.VMEM), pl.BlockSpec(memory_space=pltpu.HBM)
    shapes = [(1, width, hid), (1, width, hid), (1, hid, width), (count, half)]
    made = pl.pallas_call(
        functools.partial(handover_kernel, sizes),
        out_shape=[pltpu.VMEM(shape, bf16) for shape in shapes],
        in_specs=[hbm] * 7,
        out_specs=[vmem] * 4,
        scratch_shapes=[
            pltpu.VMEM((count, width), bf16), pltpu.VMEM((1, depth), f32), pltpu.VMEM((2, count), jnp.int32), pltpu.VMEM((2, count), f32),
            pltpu.VMEM((n_fs, depth, hid), f32), pltpu.VMEM((n_fs, depth, hid), f32), pltpu.VMEM((n_fs, hid, depth), f32),
            pltpu.VMEM((n_fs, depth, hid), bf16), pltpu.VMEM((n_fs, depth, hid), bf16), pltpu.VMEM((n_fs, hid, depth), bf16),
            pltpu.VMEM((count, width), bf16), pltpu.VMEM((3, count, half), bf16), pltpu.VMEM((n_fs, 8, count), f32),
            pltpu.VMEM((4, slots, half), bf16),
            pltpu.VMEM((n_fs * slots, width), bf16), pltpu.VMEM((n_fs * slots, hid), bf16),
            pltpu.VMEM((n_fs * slots, width), bf16), pltpu.VMEM((n_fs * slots, half), bf16),
            pltpu.VMEM((n_fs * slots, half), bf16), pltpu.VMEM((quad * slots, half), bf16),
            pltpu.VMEM((2, quad * slots, half), bf16), pltpu.VMEM((2, count, half), bf16), pltpu.VMEM((count, half), bf16),
            pltpu.VMEM((count, quad * slots), bf16), pltpu.VMEM((2, count, quad * slots), bf16),
            dma((7,)), dma((3,)), dma((3, n_fs - 1)), dma((3,)), dma((2,)), dma((4,)), dma((11,)), dma((3,)), dma((4,)), dma((4,)),
            dma((4, 4)), dma((3,)), dma((4, 2)), dma((4,)),
        ],
        compiler_params=pltpu.CompilerParams(collective_id=2, has_side_effects=True, vmem_limit_bytes=56 * 2**20),
        name="handover",
    )(tokens, norm_gain.reshape(1, depth), expert_ids.T, route_score.T, gate_train, up_train, down_train)
    return pl.pallas_call(
        store_kernel,
        out_shape=[jax.ShapeDtypeStruct(shape, bf16) for shape in shapes],
        in_specs=[vmem] * 4,
        out_specs=[pl.BlockSpec(memory_space=pl.ANY)] * 4,
        scratch_shapes=[dma((4,))],
        compiler_params=pltpu.CompilerParams(vmem_limit_bytes=16 * 2**20),
        name="store",
    )(*made)


def on_device(sizes, tokens, norm_gain, gate_train, up_train, down_train, expert_ids, route_score):
    n_gr, n_fs, n_tp = sizes["gr"], sizes["fs"], sizes["tp"]
    bf16 = jnp.bfloat16
    experts, depth, hid = gate_train.shape
    local = experts // n_fs
    count, width = tokens.shape
    capacity = 4 * count // experts
    direct_down = depth % 128 == 0
    if direct_down and local == 1 and capacity % 128 == 0 and (n_gr, n_fs, n_tp) == (2, 8, 2):
        return run_handover(sizes, capacity, tokens, norm_gain, gate_train, up_train, down_train, expert_ids, route_score)

    gate_cast = (norm_gain[None, :, None] * gate_train).astype(bf16)
    up_cast = (norm_gain[None, :, None] * up_train).astype(bf16)
    down_cast = down_train.astype(bf16)
    floated = tokens.astype(jnp.float32)
    normed = (floated * lax.rsqrt(jnp.mean(floated * floated, axis=-1, keepdims=True) + epsilon)).astype(bf16)

    named = expert_ids[:, :, None] == jnp.arange(experts, dtype=jnp.int32)
    names = jnp.any(named, axis=1)
    earlier = jnp.arange(count)[:, None] > jnp.arange(count)[None, :]
    rank = jnp.dot(earlier.astype(bf16), names.astype(bf16), preferred_element_type=jnp.float32).astype(jnp.int32)
    slot = expert_ids * capacity + jnp.sum(jnp.where(named, rank[:, None, :], 0), axis=2)
    keys = jnp.concatenate([slot.T, jnp.full((6, count), -1, jnp.int32)], axis=0)

    share = route_score / jnp.sum(route_score, axis=-1, keepdims=True)
    down_shape = (local, hid, n_gr * n_fs * depth) if direct_down else (n_gr * n_fs, local, hid, depth)
    dma = pltpu.SemaphoreType.DMA
    gate_ready, up_ready, down_ready, gathered, all_keys = pl.pallas_call(
        functools.partial(spread_kernel, sizes, local, direct_down),
        out_shape=(
            jax.ShapeDtypeStruct((local, n_gr * n_fs * depth, hid), bf16),
            jax.ShapeDtypeStruct((local, n_gr * n_fs * depth, hid), bf16),
            jax.ShapeDtypeStruct(down_shape, bf16),
            jax.ShapeDtypeStruct((n_fs, count, width), bf16),
            jax.ShapeDtypeStruct((n_fs, 8, count), jnp.int32),
        ),
        in_specs=[pl.BlockSpec(memory_space=pltpu.VMEM)] * 5,
        out_specs=[pl.BlockSpec(memory_space=pl.ANY)] * 5,
        scratch_shapes=[
            dma((3, n_fs)), dma((3, n_fs)), dma((3, n_fs, n_gr)), dma((3, n_fs, n_gr)),
            dma((n_fs,)), dma((n_fs,)), dma((n_fs,)), dma((n_fs,)),
            dma((n_tp, n_fs)), dma((n_tp, n_fs)), dma((n_fs,)), dma((n_fs,)), dma((5,)),
        ],
        compiler_params=pltpu.CompilerParams(collective_id=0, has_side_effects=True),
        name="spread",
    )(gate_cast, up_cast, down_cast, normed, keys)
    if not direct_down:
        down_ready = down_ready.transpose(1, 2, 0, 3).reshape(local, hid, -1)

    wanted = (lax.axis_index("fs") * local * capacity + jnp.arange(local * capacity, dtype=jnp.int32))[None, :, None]
    pick = ((all_keys[:, 0][:, None, :] == wanted) | (all_keys[:, 1][:, None, :] == wanted)).astype(bf16)
    rows = jnp.einsum("sct,std->scd", pick, gathered, preferred_element_type=jnp.float32).astype(bf16)
    rows = rows.reshape(n_fs, local, capacity, width)
    gate_act = jnp.einsum("seck,ekh->sech", rows, gate_ready, preferred_element_type=jnp.float32)
    up_act = jnp.einsum("seck,ekh->sech", rows, up_ready, preferred_element_type=jnp.float32)
    hidden = (jax.nn.silu(gate_act) * up_act).astype(bf16)
    part = jnp.einsum("sech,ehk->seck", hidden, down_ready, preferred_element_type=jnp.float32).astype(bf16)
    part = part.reshape(n_fs, local * capacity, width)
    half = width // n_tp
    returned = pl.pallas_call(
        functools.partial(return_kernel, sizes),
        out_shape=jax.ShapeDtypeStruct((n_fs, local * capacity, half), bf16),
        in_specs=[pl.BlockSpec(memory_space=pltpu.VMEM)],
        out_specs=pl.BlockSpec(memory_space=pltpu.VMEM),
        scratch_shapes=[
            pltpu.VMEM((max(n_tp - 1, 1), n_fs, local * capacity, half), bf16),
            pltpu.VMEM((n_fs, local * capacity, half), bf16),
            dma((n_tp, n_fs)), dma((n_tp, n_fs)), dma((n_fs,)), dma((n_fs,)),
        ],
        compiler_params=pltpu.CompilerParams(collective_id=1, has_side_effects=True),
        name="giveback",
    )(part)
    at = jnp.arange(experts * capacity, dtype=jnp.int32)[None, :]
    weight = jnp.where(slot[:, :1] == at, share[:, :1], 0.0) + jnp.where(slot[:, 1:] == at, share[:, 1:], 0.0)
    mixed = jnp.dot(weight.astype(bf16), returned.reshape(experts * capacity, half), preferred_element_type=jnp.float32)
    return gate_ready, up_ready, down_ready, mixed.astype(bf16)


def solution(mesh):
    return jax.shard_map(
        functools.partial(on_device, dict(mesh.shape)),
        mesh=mesh,
        in_specs=(
            P(("gr", "fs"), None),
            P(("gr", "fs")),
            P(None, ("gr", "fs"), "tp"),
            P(None, ("gr", "fs"), "tp"),
            P(None, "tp", ("gr", "fs")),
            P(("gr", "fs"), None),
            P(("gr", "fs"), None),
        ),
        out_specs=(
            P("fs", None, "tp"),
            P("fs", None, "tp"),
            P("fs", "tp", None),
            P(("gr", "fs"), "tp"),
        ),
        check_vma=False,
    )
```

```python
import functools

import jax
import jax.numpy as jnp
from jax import lax
from jax.experimental import pallas as pl
from jax.experimental.pallas import tpu as pltpu
from jax.sharding import PartitionSpec as P

epsilon = 1e-06
MESH = pl.DeviceIdType.MESH


def remote(src, dst, send_sem, recv_sem, where):
    return pltpu.make_async_remote_copy(
        src_ref=src, dst_ref=dst, send_sem=send_sem, recv_sem=recv_sem, device_id=where, device_id_type=MESH
    )


def greet(sizes):
    barrier = pltpu.get_barrier_semaphore()
    count = 0
    for name, size in sizes.items():
        me = lax.axis_index(name)
        for k in range(1, size):
            pl.semaphore_signal(barrier, inc=1, device_id={name: lax.rem(me + k, size)}, device_id_type=MESH)
            count += 1
    pl.semaphore_wait(barrier, count)


def spread_kernel(sizes, local, direct_down, gate, up, down, rows, keys, gate_out, up_out, down_out, rows_out, keys_out,
                  w_send, w_recv, g_send, g_recv, up_send, low_send, y_send, x_recv, t_send, t_recv, k_send, k_recv, own_sem):
    n_gr, n_fs, n_tp = sizes["gr"], sizes["fs"], sizes["tp"]
    g, f, p = lax.axis_index("gr"), lax.axis_index("fs"), lax.axis_index("tp")
    inner = 2 if n_fs % 2 == 0 else 1
    lines = n_fs // inner
    z, y = f // inner, lax.rem(f, inner)
    depth = gate.shape[1]
    half = rows.shape[1] // n_tp
    cols = pl.ds(pl.multiple_of(p * half, half), half)
    sources, outs = (gate, up, down), (gate_out, up_out, down_out)

    def place(w, block):
        start = pl.multiple_of(block * depth, depth)
        if w < 2:
            return outs[w].at[:, pl.ds(start, depth), :]
        return outs[w].at[:, :, pl.ds(start, depth)] if direct_down else outs[w].at[block]

    greet(sizes)

    own = [pltpu.make_async_copy(rows, rows_out.at[f], own_sem.at[0]),
           pltpu.make_async_copy(keys, keys_out.at[f], own_sem.at[1])]
    for w in range(3):
        own.append(pltpu.make_async_copy(sources[w].at[pl.ds(f * local, local)], place(w, g * n_fs + f), own_sem.at[2 + w]))

    def block_of(b):
        return rows_out.at[b, :, cols]

    def row_copy(b, first, kind, where):
        src = rows.at[:, cols] if first else block_of(b)
        return remote(src, block_of(b), {"u": up_send, "d": low_send, "y": y_send}[kind].at[b], x_recv.at[b], where)

    def tp_copy(b, j):
        return remote(block_of(b), block_of(b), t_send.at[j, b], t_recv.at[j, b], {"tp": lax.rem(p + j + 1, n_tp)})

    def go_up(b, first, act):
        @pl.when(z < lines - 1)
        def _():
            act(row_copy(b, first, "u", {"fs": lax.rem(f + inner, n_fs)}))

    def go_down(b, first, act):
        @pl.when(z > 0)
        def _():
            act(row_copy(b, first, "d", {"fs": lax.rem(f + n_fs - inner, n_fs)}))

    def go_side(b, first, act):
        if inner == 2:
            act(row_copy(b, first, "y", {"fs": f + 1 - 2 * y}))

    def start(c):
        c.start()

    def recv(c):
        c.wait_recv()

    def sent(c):
        c.wait_send()

    go_up(f, True, start)
    go_down(f, True, start)
    go_side(f, True, start)
    key_copies = []
    for k in range(1, n_fs):
        to = lax.rem(f + k, n_fs)
        c = remote(keys, keys_out.at[f], k_send.at[k], k_recv.at[k], {"fs": to})
        c.start()
        key_copies.append(c)
    for c in own:
        c.start()

    def gr_copy(w, b, k, j, first):
        src = sources[w].at[pl.ds(f * local, local)] if first else place(w, b)
        return remote(src, place(w, b), g_send.at[w, k, j], g_recv.at[w, k, j], {"gr": lax.rem(g + j + 1, n_gr)})

    for w in range(3):
        for j in range(n_gr - 1):
            gr_copy(w, g * n_fs + f, 0, j, True).start()

    for s in range(1, lines):
        @pl.when(z >= s)
        def _():
            b = f - s * inner
            row_copy(b, False, "u", {"fs": lax.rem(f + inner, n_fs)}).wait_recv()
            go_up(b, False, start)
            go_side(b, False, start)
            for j in range(n_tp - 1):
                tp_copy(b, j).start()

        @pl.when(z < lines - s)
        def _():
            b = f + s * inner
            row_copy(b, False, "d", {"fs": lax.rem(f + inner, n_fs)}).wait_recv()
            go_down(b, False, start)
            go_side(b, False, start)
            for j in range(n_tp - 1):
                tp_copy(b, j).start()

    def w_copy(w, k):
        to = lax.rem(f + k, n_fs)
        return remote(sources[w].at[pl.ds(to * local, local)], place(w, g * n_fs + f), w_send.at[w, k], w_recv.at[w, k], {"fs": to})

    for w in range(3):
        for k in range(1, n_fs):
            w_copy(w, k).start()

    if inner == 2:
        for s in range(lines):
            b = lax.rem(z + s, lines) * inner + 1 - y
            row_copy(b, False, "y", {"fs": f + 1 - 2 * y}).wait_recv()
            for j in range(n_tp - 1):
                tp_copy(b, j).start()

    for w in range(3):
        for k in range(1, n_fs):
            w_copy(w, k).wait_recv()
            b = g * n_fs + lax.rem(f + n_fs - k, n_fs)
            for j in range(n_gr - 1):
                gr_copy(w, b, k, j, False).start()

    for k in range(1, n_fs):
        b = lax.rem(f + k, n_fs)
        for j in range(n_tp - 1):
            c = tp_copy(b, j)
            c.wait_recv()
            c.wait_send()
    for c in key_copies:
        c.wait_recv()
        c.wait_send()
    for c in own:
        c.wait()
    go_up(f, True, sent)
    go_down(f, True, sent)
    go_side(f, True, sent)
    for s in range(1, lines):
        @pl.when(z >= s)
        def _():
            go_up(f - s * inner, False, sent)
            go_side(f - s * inner, False, sent)

        @pl.when(z < lines - s)
        def _():
            go_down(f + s * inner, False, sent)
            go_side(f + s * inner, False, sent)
    for w in range(3):
        for k in range(n_fs):
            if k:
                w_copy(w, k).wait_send()
            for j in range(n_gr - 1):
                c = gr_copy(w, g * n_fs + lax.rem(f + n_fs - k, n_fs), k, j, False)
                c.wait_recv()
                c.wait_send()


def return_kernel(sizes, part, out, held, total, t_send, t_recv, f_send, f_recv):
    n_fs, n_tp = sizes["fs"], sizes["tp"]
    f, p = lax.axis_index("fs"), lax.axis_index("tp")
    half = part.shape[2] // n_tp

    def cols(q):
        return pl.ds(pl.multiple_of(q * half, half), half)

    greet({"fs": n_fs, "tp": n_tp})
    order = list(range(1, n_fs)) + [0]

    def tp_copy(k, j):
        to = lax.rem(p + j + 1, n_tp)
        b = lax.rem(f + k, n_fs)
        return remote(part.at[b, :, cols(to)], held.at[j, b], t_send.at[j, k], t_recv.at[j, k], {"tp": to})

    def f_copy(k):
        b = lax.rem(f + k, n_fs)
        return remote(total.at[b], out.at[f], f_send.at[k], f_recv.at[k], {"fs": b})

    for k in order:
        for j in range(n_tp - 1):
            tp_copy(k, j).start()
    for k in order:
        b = lax.rem(f + k, n_fs)
        value = part[b, :, cols(p)].astype(jnp.float32)
        for j in range(n_tp - 1):
            tp_copy(k, j).wait_recv()
            value = value + held[j, b].astype(jnp.float32)
        value = value.astype(jnp.bfloat16)
        if k == 0:
            out[b] = value
        else:
            total[b] = value
            f_copy(k).start()
    for k in order:
        for j in range(n_tp - 1):
            tp_copy(k, j).wait_send()
        if k:
            f_copy(k).wait_recv()
            f_copy(k).wait_send()


def handover_kernel(sizes, tokens_hbm, gain_hbm, ids_hbm, score_hbm, gate_hbm, up_hbm, down_hbm, gate_out, up_out, down_out, mixed,
                    tokens, gain, ids, score, gate_raw, up_raw, down_raw, gate_cut, up_cut, down_cut, rows_own, line_in, meta, y_pick,
                    picked, gate_act, hidden, part, held, total, back, collect, far_out, far_in, near_w, gate_w,
                    load_sem, w_send, w_recv, g_send, g_recv, d_recv, x_send, x_recv, y_recv, k_recv, t_recv, p_recv, n_recv, c_recv, o_recv):
    n_fs = sizes["fs"]
    g, f, p = lax.axis_index("gr"), lax.axis_index("fs"), lax.axis_index("tp")
    z, y = f // 2, lax.rem(f, 2)
    low, side = lax.rem(z, 2), z // 2
    door = 1 + side
    is_door = z == door
    role = 1 - (low + side - 2 * low * side)
    depth = gate_hbm.shape[1]
    count, width = tokens.shape
    slots = back.shape[0] * 2 // n_fs
    half = width // 2
    span = half // 2
    strip = 2 * depth
    quad = n_fs // 2
    bf16, f32 = jnp.bfloat16, jnp.float32
    raws, cuts, outs = (gate_raw, up_raw, down_raw), (gate_cut, up_cut, down_cut), (gate_out, up_out, down_out)
    hbms = (gate_hbm, up_hbm, down_hbm)
    near = [(0, 1), (1, 0), (1, 1)]
    far = [(2, 0), (2, 1), (3, 0), (3, 1)]
    index = {t: i for i, t in enumerate(near + far)}
    mine = lax.rem(f, quad)
    rows_send, relay_send, y_send, t_send, k_send, p_send, n_send, c_send, e_send, o_send = [x_send.at[i] for i in range(10)]

    def at_door(act, otherwise=None):
        @pl.when(is_door)
        def _():
            act()

        if otherwise is not None:
            at_end(otherwise)

    def at_end(act):
        @pl.when(z != door)
        def _():
            act()

    def level(s):
        return (z, z + 1 - 2 * low, 2 - side, 3 - 3 * side)[s]

    def peer(t):
        return level(t[0]) * 2 + (1 - y if t[1] else y)

    def there(t):
        return index[t] if t[0] < 2 else len(near) + 2 * role + t[1]

    def cols(q):
        return pl.ds(pl.multiple_of(q * half, half), half)

    def seat(b):
        return pl.ds(pl.multiple_of(b * slots, slots), slots)

    def pair(s):
        return pl.ds(pl.multiple_of(level(s) * (2 * slots), 2 * slots), 2 * slots)

    def place(w, block):
        at = pl.ds(pl.multiple_of(block * depth, depth), depth)
        return outs[w].at[0, at, :] if w < 2 else outs[w].at[0, :, at]

    def local(block, send, recv):
        return remote(block, block, send, recv, {"tp": 1 - p})

    def w_copy(w, t):
        to = peer(t)
        return remote(cuts[w].at[to], place(w, g * n_fs + f), w_send.at[w], w_recv.at[w, there(t)], {"fs": to})

    def g_copy(w, t):
        b = g * n_fs + peer(t)
        src = cuts[w].at[f] if t == (0, 0) else place(w, b)
        return remote(src, place(w, b), g_send.at[w], g_recv.at[w] if w < 2 else d_recv.at[t[0]], {"gr": 1 - g})

    def pass_on(w, *ts):
        for t in ts:
            local(place(w, g * n_fs + peer(t)), w_send.at[w], w_recv.at[w, index[t]]).wait_recv()
            g_copy(w, t).start()

    def ready(s):
        local(down_out.at[0, :, pl.ds(0, strip)], g_send.at[2], d_recv.at[s]).wait_recv()

    def row_copy(s):
        if s == 1:
            return remote(rows_own.at[:, cols(p)], line_in.at[0], rows_send, x_recv.at[0], {"fs": peer((1, 0))})
        return remote(rows_own.at[:, cols(p)], line_in.at[1 + role], rows_send, x_recv.at[1 + role], {"fs": peer((2, 0))})

    def relay_copy(s):
        return remote(line_in.at[s - 1], line_in.at[s - 1], relay_send, x_recv.at[s - 1], {"fs": peer((1, 0))})

    def y_copy(s):
        return remote(y_pick.at[s], picked.at[seat(peer((s, 0))), cols(p)], y_send, y_recv.at[s], {"fs": peer((0, 1))})

    def tp_copy(t):
        block = picked.at[seat(peer(t)), cols(p)]
        return remote(block, block, t_send, t_recv.at[t[0]], {"tp": 1 - p})

    def take_y(s):
        local(picked.at[seat(peer((s, 1))), cols(p)], y_send, y_recv.at[s]).wait_recv()
        tp_copy((s, 1)).start()

    def key_copy(s):
        return remote(meta.at[f], meta.at[f], k_send, k_recv.at[s if s < 2 else 2 + role], {"fs": peer((s, 0))})

    def cut(w):
        pltpu.make_async_copy(hbms[w], raws[w], load_sem.at[w]).wait()
        if w < 2:
            scale = jnp.broadcast_to(gain[...], (128, depth)).T
            for e in range(n_fs):
                for c in range(0, raws[w].shape[2], 128):
                    cuts[w][e, :, c:c + 128] = (scale * raws[w][e, :, c:c + 128]).astype(bf16)
            outs[w][0, pl.ds(pl.multiple_of((g * n_fs + f) * depth, depth), depth), :] = cuts[w][f]
        else:
            for e in range(n_fs):
                cuts[w][e] = raws[w][e].astype(bf16)
            outs[w][0, :, pl.ds(pl.multiple_of((g * n_fs + f) * depth, depth), depth)] = cuts[w][f]

    def pick(b, expert, rows):
        wanted = (expert * slots + lax.broadcasted_iota(jnp.int32, (slots, count), 0)).astype(f32)
        hit = ((meta[b, 0:1, :] == wanted) | (meta[b, 1:2, :] == wanted)).astype(f32).astype(bf16)
        return jnp.dot(hit, rows, preferred_element_type=f32).astype(bf16)

    def shares(b):
        wanted = (side * (quad * slots) + lax.broadcasted_iota(jnp.int32, (quad * slots, count), 0)).astype(f32)
        table = jnp.where(meta[b, 0:1, :] == wanted, meta[b, 2:3, :], 0.0) + jnp.where(
            meta[b, 1:2, :] == wanted, meta[b, 3:4, :], 0.0)
        return table.T.astype(bf16)

    def take_line(s, relay):
        local(line_in.at[s - 1], rows_send, x_recv.at[s - 1]).wait_recv()
        if relay:
            relay_copy(s).start()
        b = peer((s, 0))
        local(meta.at[b], k_send, k_recv.at[s]).wait_recv()
        y_pick[s] = pick(b, peer((0, 1)), line_in[s - 1])
        picked[seat(b), cols(p)] = pick(b, f, line_in[s - 1])
        y_copy(s).start()
        tp_copy((s, 0)).start()

    def whole(w):
        local(outs[w].at[0, pl.ds(0, n_fs * depth), :], g_send.at[w], g_recv.at[w]).wait_recv()

    def gate_of(s):
        blocks = 1 if s == 0 else 2
        local(picked.at[pl.ds(0, blocks * slots), pl.ds(0, half)], t_send, t_recv.at[s]).wait_recv()
        gate_act[pair(s), :] = jnp.dot(picked[pair(s), :], gate_out[0], preferred_element_type=f32)

    barrier = pltpu.get_barrier_semaphore()
    heard = 0
    for name, size in sizes.items():
        me = lax.axis_index(name)
        for k in range(1, size):
            pl.semaphore_signal(barrier, inc=1, device_id={name: lax.rem(me + k, size)}, device_id_type=MESH)
            heard += 1
    loads = [pltpu.make_async_copy(src, dst, load_sem.at[3 + i]) for i, (src, dst) in enumerate(
        [(ids_hbm, ids), (score_hbm, score), (tokens_hbm, tokens), (gain_hbm, gain)])]
    for c in loads:
        c.start()
    for w in range(3):
        pltpu.make_async_copy(hbms[w], raws[w], load_sem.at[w]).start()
    loads[0].wait()
    loads[1].wait()
    expert = lax.broadcasted_iota(jnp.int32, (16, count), 0)
    names = ((ids[0:1, :] == expert) | (ids[1:2, :] == expert)).astype(f32).astype(bf16)
    earlier = lax.broadcasted_iota(jnp.int32, (count, count), 0) < lax.broadcasted_iota(jnp.int32, (count, count), 1)
    rank = jnp.dot(names, earlier.astype(f32).astype(bf16), preferred_element_type=f32) + (expert * slots).astype(f32)
    both = score[0:1, :] + score[1:2, :]
    table = [jnp.sum(jnp.where(ids[k:k + 1, :] == expert, rank, 0.0), axis=0, keepdims=True) for k in range(2)]
    table += [score[k:k + 1, :] / both for k in range(2)]
    for i in range(4):
        meta[f, i:i + 1, :] = table[i]
    meta[f, 4:8, :] = jnp.zeros((4, count), f32)
    loads[2].wait()
    for r in range(0, count, 32):
        x = tokens[r:r + 32, :].astype(f32)
        rows_own[r:r + 32, :] = (x * lax.rsqrt(jnp.mean(x * x, axis=-1, keepdims=True) + epsilon)).astype(bf16)
    pl.semaphore_wait(barrier, heard)
    for s in range(1, 4):
        key_copy(s).start()
    row_copy(1).start()
    row_copy(2).start()
    y_pick[0] = pick(f, peer((0, 1)), rows_own[:, cols(p)])
    loads[3].wait()
    y_copy(0).start()
    cut(0)
    for t in near:
        w_copy(0, t).start()
    g_copy(0, (0, 0)).start()
    cut(1)
    for w, ts in [(1, near), (0, far), (1, far)]:
        for t in ts:
            w_copy(w, t).start()
    g_copy(1, (0, 0)).start()
    cut(2)
    w_copy(2, (0, 1)).start()
    g_copy(2, (0, 0)).start()

    def early_down():
        w_copy(2, (1, 0)).start()
        w_copy(2, (1, 1)).start()

    at_end(early_down)
    for c in range(0, width, 512):
        picked[seat(f), c:c + 512] = pick(f, f, rows_own[:, c:c + 512])
    near_w[...] = shares(f)
    take_y(0)
    pass_on(0, (0, 1))
    pass_on(1, (0, 1))
    take_line(1, False)
    at_door(lambda: take_line(2, True))
    pass_on(0, (1, 0), (1, 1))
    at_door(lambda: take_line(3, True))
    pass_on(1, (1, 0), (1, 1))

    def gate_shares():
        for i in range(2):
            gate_w[i] = shares(peer((2 + i, 0)))

    at_door(gate_shares)
    pass_on(0, (3, 0), (3, 1))
    pass_on(0, (2, 0))
    at_end(lambda: take_line(2, False))
    at_door(lambda: pass_on(0, (2, 1)))
    take_y(1)

    def take_both():
        take_y(2)
        take_y(3)

    at_door(take_both)
    pass_on(2, (0, 1))
    pass_on(1, (3, 0), (3, 1))
    at_end(lambda: pass_on(0, (2, 1)))
    at_end(lambda: take_line(3, False))
    at_end(lambda: take_y(2))

    def far_down():
        for t in far:
            w_copy(2, t).start()

    whole(0)
    for s in (1, 0, 2):
        gate_of(s)
    at_door(lambda: gate_of(3))
    pass_on(1, (2, 0), (2, 1))
    at_door(early_down)
    far_down()
    at_end(lambda: take_y(3))
    at_door(lambda: pass_on(2, (1, 0), (1, 1)))
    whole(1)
    order = [2, 3, 1, 0]

    def act(s):
        gated = gate_act[pair(s), :]
        up_act = jnp.dot(picked[pair(s), :], up_out[0], preferred_element_type=f32)
        hidden[pair(s), :] = (gated / (1.0 + jnp.exp(-gated)) * up_act).astype(bf16)

    def here(st, base=0):
        layer = (3 * side, door, 3 - 3 * side, 2 - side)[st]
        return pl.ds(pl.multiple_of(base + layer * strip, strip), strip)

    def p_copy(st, s):
        return remote(part.at[pair(s), here(st, (1 - p) * half)], held.at[pair(s), here(st)], p_send, p_recv.at[st, s], {"tp": 1 - p})

    def n_copy(st, t):
        return remote(total.at[seat(peer(t)), here(st)], back.at[seat(mine), here(st)], n_send, n_recv.at[max(st - 1, 0)],
                      {"fs": peer(t)})

    def c_copy(st, t):
        return remote(total.at[seat(peer(t)), here(st)], collect.at[t[0] - 2, seat(mine), here(st)], c_send if t[1] else e_send,
                      c_recv.at[st, t[0] - 2], {"fs": door * 2 + (1 - y if t[1] else y)})

    def o_copy(st, i):
        return remote(far_out.at[i, :, here(st)], far_in.at[:, here(st)], o_send, o_recv.at[st], {"fs": peer((2 + i, 0))})

    def spread(st, s):
        for q in range(2):
            part[pair(s), here(st, q * half)] = jnp.dot(
                hidden[pair(s), :], down_out[0, :, here(st, q * half)], preferred_element_type=f32).astype(bf16)

    def add(st, s):
        p_copy(st, s).wait_recv()
        total[pair(s), here(st)] = (part[pair(s), here(st, p * half)].astype(f32) + held[pair(s), here(st)].astype(f32)).astype(bf16)

    def send(st, s):
        for dy in range(2):
            t = (s, dy)
            if t == (0, 0):
                back[seat(mine), here(st)] = total[seat(f), here(st)]
            elif s == 0:
                n_copy(st, t).start()
            elif dy and s > 1:
                c_copy(st, t).start()
            elif s > 1:
                def keep():
                    collect[s - 2, seat(mine), here(st)] = total[seat(peer(t)), here(st)]

                at_door(keep, lambda: c_copy(st, t).start())

    def first():
        for i in range(len(order) + 1):
            if i < len(order):
                if order[i] == 3:
                    at_end(lambda: gate_of(3))
                act(order[i])
            if i:
                add(0, order[i - 1])
            if i < len(order):
                spread(0, order[i])
            if i:
                send(0, order[i - 1])
            if i < len(order):
                p_copy(0, order[i]).start()
            if i == 0:
                at_end(lambda: pass_on(2, (1, 0), (1, 1)))
        give_near(0)

    def compute(st):
        for i, s in enumerate(order):
            spread(st, s)
            if i:
                p_copy(st, order[i - 1]).start()
        p_copy(st, order[-1]).start()

    def give(st):
        for i, s in enumerate(order):
            add(st, s)
            if i:
                send(st, order[i - 1])
        send(st, order[-1])

    def give_near(st):
        n_copy(st, (1, 0)).start()
        n_copy(st, (1, 1)).start()

    def merge(st):
        def act():
            for i in range(2):
                local(collect.at[i, pl.ds(0, (quad - 1) * slots), here(st)], c_send, c_recv.at[st, i]).wait_recv()
                far_out[i, :, here(st)] = jnp.dot(gate_w[i], collect[i, :, here(st)], preferred_element_type=f32).astype(bf16)
                o_copy(st, i).start()

        at_door(act)

    def far_wait(st):
        layer = (3 - 3 * side, 2 - side, 3 * side, door)[st]
        local(far_in.at[:, pl.ds(pl.multiple_of(layer * strip, strip), strip)], o_send, o_recv.at[st]).wait_recv()

    at_door(lambda: ready(1), lambda: ready(0))
    first()

    at_door(lambda: ready(0), lambda: ready(1))
    compute(1)
    give(1)
    pass_on(2, (3, 0), (3, 1))
    merge(0)
    pass_on(2, (2, 0), (2, 1))
    ready(3)
    compute(2)
    give(2)
    merge(1)
    ready(2)
    compute(3)
    give(3)
    for st in (1, 2, 3):
        give_near(st)
    merge(2)
    merge(3)
    local(back.at[pl.ds(0, 3 * slots // 2), :], n_send, n_recv.at[0]).wait_recv()
    sided = pl.ds(pl.multiple_of(side * span, span), span)
    acc = jnp.dot(near_w[...], back[:, sided], preferred_element_type=f32)
    far_wait(0)
    far_wait(1)
    for st in (2, 3):
        local(back.at[pl.ds(0, 3 * slots // 4), :], n_send, n_recv.at[st - 1]).wait_recv()
        more = jnp.dot(near_w[...], back[:, here(st)], preferred_element_type=f32)
        mixed[:, here(st)] = (more + far_in[:, here(st)].astype(f32)).astype(bf16)
    far_wait(2)
    far_wait(3)
    mixed[:, sided] = (acc + far_in[:, sided].astype(f32)).astype(bf16)

    def sent(block, send):
        local(block, send, o_recv.at[0]).wait_send()

    for w in range(3):
        sent(cuts[w].at[pl.ds(0, n_fs - 1)], w_send.at[w])
        sent(cuts[w], g_send.at[w])
    sent(rows_own, rows_send)
    sent(y_pick, y_send)
    sent(picked.at[pl.ds(0, (n_fs - 1) * slots), pl.ds(0, half)], t_send)
    sent(meta.at[pl.ds(0, 3)], k_send)
    sent(held, p_send)
    sent(held.at[pl.ds(0, 3 * slots), :], n_send)
    sent(held.at[pl.ds(0, 2 * slots), :], c_send)
    at_door(lambda: sent(line_in.at[pl.ds(0, 2)], relay_send), lambda: sent(held.at[pl.ds(0, 2 * slots), :], e_send))
    at_door(lambda: sent(far_out, o_send))


def store_kernel(*refs):
    sems = refs[-1]
    pairs = list(zip(refs[:4], refs[4:8]))
    copies = [pltpu.make_async_copy(src, dst, sems.at[i]) for i, (src, dst) in enumerate(pairs)]
    for c in copies:
        c.start()
    for c in copies:
        c.wait()


def run_handover(sizes, slots, tokens, norm_gain, gate_train, up_train, down_train, expert_ids, route_score):
    n_gr, n_fs, n_tp = sizes["gr"], sizes["fs"], sizes["tp"]
    _, depth, hid = gate_train.shape
    count, width = tokens.shape
    half, quad = width // n_tp, n_fs // 2
    bf16, f32, dma = jnp.bfloat16, jnp.float32, pltpu.SemaphoreType.DMA
    vmem, hbm = pl.BlockSpec(memory_space=pltpu.VMEM), pl.BlockSpec(memory_space=pltpu.HBM)
    shapes = [(1, width, hid), (1, width, hid), (1, hid, width), (count, half)]
    made = pl.pallas_call(
        functools.partial(handover_kernel, sizes),
        out_shape=[pltpu.VMEM(shape, bf16) for shape in shapes],
        in_specs=[hbm] * 7,
        out_specs=[vmem] * 4,
        scratch_shapes=[
            pltpu.VMEM((count, width), bf16), pltpu.VMEM((1, depth), f32), pltpu.VMEM((2, count), jnp.int32), pltpu.VMEM((2, count), f32),
            pltpu.VMEM((n_fs, depth, hid), f32), pltpu.VMEM((n_fs, depth, hid), f32), pltpu.VMEM((n_fs, hid, depth), f32),
            pltpu.VMEM((n_fs, depth, hid), bf16), pltpu.VMEM((n_fs, depth, hid), bf16), pltpu.VMEM((n_fs, hid, depth), bf16),
            pltpu.VMEM((count, width), bf16), pltpu.VMEM((3, count, half), bf16), pltpu.VMEM((n_fs, 8, count), f32),
            pltpu.VMEM((4, slots, half), bf16),
            pltpu.VMEM((n_fs * slots, width), bf16), pltpu.VMEM((n_fs * slots, hid), f32), pltpu.VMEM((n_fs * slots, hid), bf16),
            pltpu.VMEM((n_fs * slots, width), bf16), pltpu.VMEM((n_fs * slots, half), bf16),
            pltpu.VMEM((n_fs * slots, half), bf16), pltpu.VMEM((quad * slots, half), bf16),
            pltpu.VMEM((2, quad * slots, half), bf16), pltpu.VMEM((2, count, half), bf16), pltpu.VMEM((count, half), bf16),
            pltpu.VMEM((count, quad * slots), bf16), pltpu.VMEM((2, count, quad * slots), bf16),
            dma((7,)), dma((3,)), dma((3, n_fs - 1)), dma((3,)), dma((2,)), dma((4,)), dma((10,)), dma((3,)), dma((4,)), dma((4,)), dma((4,)),
            dma((4, 4)), dma((3,)), dma((4, 2)), dma((4,)),
        ],
        compiler_params=pltpu.CompilerParams(collective_id=2, has_side_effects=True, vmem_limit_bytes=56 * 2**20),
        name="handover",
    )(tokens, norm_gain.reshape(1, depth), expert_ids.T, route_score.T, gate_train, up_train, down_train)
    return pl.pallas_call(
        store_kernel,
        out_shape=[jax.ShapeDtypeStruct(shape, bf16) for shape in shapes],
        in_specs=[vmem] * 4,
        out_specs=[pl.BlockSpec(memory_space=pl.ANY)] * 4,
        scratch_shapes=[dma((4,))],
        compiler_params=pltpu.CompilerParams(vmem_limit_bytes=16 * 2**20),
        name="store",
    )(*made)


def on_device(sizes, tokens, norm_gain, gate_train, up_train, down_train, expert_ids, route_score):
    n_gr, n_fs, n_tp = sizes["gr"], sizes["fs"], sizes["tp"]
    bf16 = jnp.bfloat16
    experts, depth, hid = gate_train.shape
    local = experts // n_fs
    count, width = tokens.shape
    capacity = 4 * count // experts
    direct_down = depth % 128 == 0
    if direct_down and local == 1 and capacity % 128 == 0 and (n_gr, n_fs, n_tp) == (2, 8, 2):
        return run_handover(sizes, capacity, tokens, norm_gain, gate_train, up_train, down_train, expert_ids, route_score)

    gate_cast = (norm_gain[None, :, None] * gate_train).astype(bf16)
    up_cast = (norm_gain[None, :, None] * up_train).astype(bf16)
    down_cast = down_train.astype(bf16)
    floated = tokens.astype(jnp.float32)
    normed = (floated * lax.rsqrt(jnp.mean(floated * floated, axis=-1, keepdims=True) + epsilon)).astype(bf16)

    named = expert_ids[:, :, None] == jnp.arange(experts, dtype=jnp.int32)
    names = jnp.any(named, axis=1)
    earlier = jnp.arange(count)[:, None] > jnp.arange(count)[None, :]
    rank = jnp.dot(earlier.astype(bf16), names.astype(bf16), preferred_element_type=jnp.float32).astype(jnp.int32)
    slot = expert_ids * capacity + jnp.sum(jnp.where(named, rank[:, None, :], 0), axis=2)
    keys = jnp.concatenate([slot.T, jnp.full((6, count), -1, jnp.int32)], axis=0)

    share = route_score / jnp.sum(route_score, axis=-1, keepdims=True)
    down_shape = (local, hid, n_gr * n_fs * depth) if direct_down else (n_gr * n_fs, local, hid, depth)
    dma = pltpu.SemaphoreType.DMA
    gate_ready, up_ready, down_ready, gathered, all_keys = pl.pallas_call(
        functools.partial(spread_kernel, sizes, local, direct_down),
        out_shape=(
            jax.ShapeDtypeStruct((local, n_gr * n_fs * depth, hid), bf16),
            jax.ShapeDtypeStruct((local, n_gr * n_fs * depth, hid), bf16),
            jax.ShapeDtypeStruct(down_shape, bf16),
            jax.ShapeDtypeStruct((n_fs, count, width), bf16),
            jax.ShapeDtypeStruct((n_fs, 8, count), jnp.int32),
        ),
        in_specs=[pl.BlockSpec(memory_space=pltpu.VMEM)] * 5,
        out_specs=[pl.BlockSpec(memory_space=pl.ANY)] * 5,
        scratch_shapes=[
            dma((3, n_fs)), dma((3, n_fs)), dma((3, n_fs, n_gr)), dma((3, n_fs, n_gr)),
            dma((n_fs,)), dma((n_fs,)), dma((n_fs,)), dma((n_fs,)),
            dma((n_tp, n_fs)), dma((n_tp, n_fs)), dma((n_fs,)), dma((n_fs,)), dma((5,)),
        ],
        compiler_params=pltpu.CompilerParams(collective_id=0, has_side_effects=True),
        name="spread",
    )(gate_cast, up_cast, down_cast, normed, keys)
    if not direct_down:
        down_ready = down_ready.transpose(1, 2, 0, 3).reshape(local, hid, -1)

    wanted = (lax.axis_index("fs") * local * capacity + jnp.arange(local * capacity, dtype=jnp.int32))[None, :, None]
    pick = ((all_keys[:, 0][:, None, :] == wanted) | (all_keys[:, 1][:, None, :] == wanted)).astype(bf16)
    rows = jnp.einsum("sct,std->scd", pick, gathered, preferred_element_type=jnp.float32).astype(bf16)
    rows = rows.reshape(n_fs, local, capacity, width)
    gate_act = jnp.einsum("seck,ekh->sech", rows, gate_ready, preferred_element_type=jnp.float32)
    up_act = jnp.einsum("seck,ekh->sech", rows, up_ready, preferred_element_type=jnp.float32)
    hidden = (jax.nn.silu(gate_act) * up_act).astype(bf16)
    part = jnp.einsum("sech,ehk->seck", hidden, down_ready, preferred_element_type=jnp.float32).astype(bf16)
    part = part.reshape(n_fs, local * capacity, width)
    half = width // n_tp
    returned = pl.pallas_call(
        functools.partial(return_kernel, sizes),
        out_shape=jax.ShapeDtypeStruct((n_fs, local * capacity, half), bf16),
        in_specs=[pl.BlockSpec(memory_space=pltpu.VMEM)],
        out_specs=pl.BlockSpec(memory_space=pltpu.VMEM),
        scratch_shapes=[
            pltpu.VMEM((max(n_tp - 1, 1), n_fs, local * capacity, half), bf16),
            pltpu.VMEM((n_fs, local * capacity, half), bf16),
            dma((n_tp, n_fs)), dma((n_tp, n_fs)), dma((n_fs,)), dma((n_fs,)),
        ],
        compiler_params=pltpu.CompilerParams(collective_id=1, has_side_effects=True),
        name="giveback",
    )(part)
    at = jnp.arange(experts * capacity, dtype=jnp.int32)[None, :]
    weight = jnp.where(slot[:, :1] == at, share[:, :1], 0.0) + jnp.where(slot[:, 1:] == at, share[:, 1:], 0.0)
    mixed = jnp.dot(weight.astype(bf16), returned.reshape(experts * capacity, half), preferred_element_type=jnp.float32)
    return gate_ready, up_ready, down_ready, mixed.astype(bf16)


def solution(mesh):
    return jax.shard_map(
        functools.partial(on_device, dict(mesh.shape)),
        mesh=mesh,
        in_specs=(
            P(("gr", "fs"), None),
            P(("gr", "fs")),
            P(None, ("gr", "fs"), "tp"),
            P(None, ("gr", "fs"), "tp"),
            P(None, "tp", ("gr", "fs")),
            P(("gr", "fs"), None),
            P(("gr", "fs"), None),
        ),
        out_specs=(
            P("fs", None, "tp"),
            P("fs", None, "tp"),
            P("fs", "tp", None),
            P(("gr", "fs"), "tp"),
        ),
        check_vma=False,
    )
```

```python
import functools

import jax
import jax.numpy as jnp
from jax import lax
from jax.experimental import pallas as pl
from jax.experimental.pallas import tpu as pltpu
from jax.sharding import PartitionSpec as P

epsilon = 1e-06
MESH = pl.DeviceIdType.MESH


def remote(src, dst, send_sem, recv_sem, where):
    return pltpu.make_async_remote_copy(
        src_ref=src, dst_ref=dst, send_sem=send_sem, recv_sem=recv_sem, device_id=where, device_id_type=MESH
    )


def greet(sizes):
    barrier = pltpu.get_barrier_semaphore()
    count = 0
    for name, size in sizes.items():
        me = lax.axis_index(name)
        for k in range(1, size):
            pl.semaphore_signal(barrier, inc=1, device_id={name: lax.rem(me + k, size)}, device_id_type=MESH)
            count += 1
    pl.semaphore_wait(barrier, count)


def spread_kernel(sizes, local, direct_down, gate, up, down, rows, keys, gate_out, up_out, down_out, rows_out, keys_out,
                  w_send, w_recv, g_send, g_recv, up_send, low_send, y_send, x_recv, t_send, t_recv, k_send, k_recv, own_sem):
    n_gr, n_fs, n_tp = sizes["gr"], sizes["fs"], sizes["tp"]
    g, f, p = lax.axis_index("gr"), lax.axis_index("fs"), lax.axis_index("tp")
    inner = 2 if n_fs % 2 == 0 else 1
    lines = n_fs // inner
    z, y = f // inner, lax.rem(f, inner)
    depth = gate.shape[1]
    half = rows.shape[1] // n_tp
    cols = pl.ds(pl.multiple_of(p * half, half), half)
    sources, outs = (gate, up, down), (gate_out, up_out, down_out)

    def place(w, block):
        start = pl.multiple_of(block * depth, depth)
        if w < 2:
            return outs[w].at[:, pl.ds(start, depth), :]
        return outs[w].at[:, :, pl.ds(start, depth)] if direct_down else outs[w].at[block]

    greet(sizes)

    own = [pltpu.make_async_copy(rows, rows_out.at[f], own_sem.at[0]),
           pltpu.make_async_copy(keys, keys_out.at[f], own_sem.at[1])]
    for w in range(3):
        own.append(pltpu.make_async_copy(sources[w].at[pl.ds(f * local, local)], place(w, g * n_fs + f), own_sem.at[2 + w]))

    def block_of(b):
        return rows_out.at[b, :, cols]

    def row_copy(b, first, kind, where):
        src = rows.at[:, cols] if first else block_of(b)
        return remote(src, block_of(b), {"u": up_send, "d": low_send, "y": y_send}[kind].at[b], x_recv.at[b], where)

    def tp_copy(b, j):
        return remote(block_of(b), block_of(b), t_send.at[j, b], t_recv.at[j, b], {"tp": lax.rem(p + j + 1, n_tp)})

    def go_up(b, first, act):
        @pl.when(z < lines - 1)
        def _():
            act(row_copy(b, first, "u", {"fs": lax.rem(f + inner, n_fs)}))

    def go_down(b, first, act):
        @pl.when(z > 0)
        def _():
            act(row_copy(b, first, "d", {"fs": lax.rem(f + n_fs - inner, n_fs)}))

    def go_side(b, first, act):
        if inner == 2:
            act(row_copy(b, first, "y", {"fs": f + 1 - 2 * y}))

    def start(c):
        c.start()

    def recv(c):
        c.wait_recv()

    def sent(c):
        c.wait_send()

    go_up(f, True, start)
    go_down(f, True, start)
    go_side(f, True, start)
    key_copies = []
    for k in range(1, n_fs):
        to = lax.rem(f + k, n_fs)
        c = remote(keys, keys_out.at[f], k_send.at[k], k_recv.at[k], {"fs": to})
        c.start()
        key_copies.append(c)
    for c in own:
        c.start()

    def gr_copy(w, b, k, j, first):
        src = sources[w].at[pl.ds(f * local, local)] if first else place(w, b)
        return remote(src, place(w, b), g_send.at[w, k, j], g_recv.at[w, k, j], {"gr": lax.rem(g + j + 1, n_gr)})

    for w in range(3):
        for j in range(n_gr - 1):
            gr_copy(w, g * n_fs + f, 0, j, True).start()

    for s in range(1, lines):
        @pl.when(z >= s)
        def _():
            b = f - s * inner
            row_copy(b, False, "u", {"fs": lax.rem(f + inner, n_fs)}).wait_recv()
            go_up(b, False, start)
            go_side(b, False, start)
            for j in range(n_tp - 1):
                tp_copy(b, j).start()

        @pl.when(z < lines - s)
        def _():
            b = f + s * inner
            row_copy(b, False, "d", {"fs": lax.rem(f + inner, n_fs)}).wait_recv()
            go_down(b, False, start)
            go_side(b, False, start)
            for j in range(n_tp - 1):
                tp_copy(b, j).start()

    def w_copy(w, k):
        to = lax.rem(f + k, n_fs)
        return remote(sources[w].at[pl.ds(to * local, local)], place(w, g * n_fs + f), w_send.at[w, k], w_recv.at[w, k], {"fs": to})

    for w in range(3):
        for k in range(1, n_fs):
            w_copy(w, k).start()

    if inner == 2:
        for s in range(lines):
            b = lax.rem(z + s, lines) * inner + 1 - y
            row_copy(b, False, "y", {"fs": f + 1 - 2 * y}).wait_recv()
            for j in range(n_tp - 1):
                tp_copy(b, j).start()

    for w in range(3):
        for k in range(1, n_fs):
            w_copy(w, k).wait_recv()
            b = g * n_fs + lax.rem(f + n_fs - k, n_fs)
            for j in range(n_gr - 1):
                gr_copy(w, b, k, j, False).start()

    for k in range(1, n_fs):
        b = lax.rem(f + k, n_fs)
        for j in range(n_tp - 1):
            c = tp_copy(b, j)
            c.wait_recv()
            c.wait_send()
    for c in key_copies:
        c.wait_recv()
        c.wait_send()
    for c in own:
        c.wait()
    go_up(f, True, sent)
    go_down(f, True, sent)
    go_side(f, True, sent)
    for s in range(1, lines):
        @pl.when(z >= s)
        def _():
            go_up(f - s * inner, False, sent)
            go_side(f - s * inner, False, sent)

        @pl.when(z < lines - s)
        def _():
            go_down(f + s * inner, False, sent)
            go_side(f + s * inner, False, sent)
    for w in range(3):
        for k in range(n_fs):
            if k:
                w_copy(w, k).wait_send()
            for j in range(n_gr - 1):
                c = gr_copy(w, g * n_fs + lax.rem(f + n_fs - k, n_fs), k, j, False)
                c.wait_recv()
                c.wait_send()


def return_kernel(sizes, part, out, held, total, t_send, t_recv, f_send, f_recv):
    n_fs, n_tp = sizes["fs"], sizes["tp"]
    f, p = lax.axis_index("fs"), lax.axis_index("tp")
    half = part.shape[2] // n_tp

    def cols(q):
        return pl.ds(pl.multiple_of(q * half, half), half)

    greet({"fs": n_fs, "tp": n_tp})
    order = list(range(1, n_fs)) + [0]

    def tp_copy(k, j):
        to = lax.rem(p + j + 1, n_tp)
        b = lax.rem(f + k, n_fs)
        return remote(part.at[b, :, cols(to)], held.at[j, b], t_send.at[j, k], t_recv.at[j, k], {"tp": to})

    def f_copy(k):
        b = lax.rem(f + k, n_fs)
        return remote(total.at[b], out.at[f], f_send.at[k], f_recv.at[k], {"fs": b})

    for k in order:
        for j in range(n_tp - 1):
            tp_copy(k, j).start()
    for k in order:
        b = lax.rem(f + k, n_fs)
        value = part[b, :, cols(p)].astype(jnp.float32)
        for j in range(n_tp - 1):
            tp_copy(k, j).wait_recv()
            value = value + held[j, b].astype(jnp.float32)
        value = value.astype(jnp.bfloat16)
        if k == 0:
            out[b] = value
        else:
            total[b] = value
            f_copy(k).start()
    for k in order:
        for j in range(n_tp - 1):
            tp_copy(k, j).wait_send()
        if k:
            f_copy(k).wait_recv()
            f_copy(k).wait_send()


def handover_kernel(sizes, tokens_hbm, gain_hbm, ids_hbm, score_hbm, gate_hbm, up_hbm, down_hbm, gate_out, up_out, down_out, mixed,
                    tokens, gain, ids, score, gate_raw, up_raw, down_raw, gate_cut, up_cut, down_cut, rows_own, line_in, meta, y_pick,
                    picked, gate_act, up_act, hidden, part, held, total, back, collect, far_out, far_in, near_w, gate_w,
                    load_sem, w_send, w_recv, g_send, g_recv, d_recv, x_send, x_recv, y_recv, k_recv, t_recv, p_recv, n_recv, c_recv, o_recv):
    n_fs = sizes["fs"]
    g, f, p = lax.axis_index("gr"), lax.axis_index("fs"), lax.axis_index("tp")
    z, y = f // 2, lax.rem(f, 2)
    low, side = lax.rem(z, 2), z // 2
    door = 1 + side
    is_door = z == door
    role = 1 - (low + side - 2 * low * side)
    depth = gate_hbm.shape[1]
    count, width = tokens.shape
    slots = back.shape[0] * 2 // n_fs
    half = width // 2
    span = half // 2
    strip = 2 * depth
    quad = n_fs // 2
    bf16, f32 = jnp.bfloat16, jnp.float32
    raws, cuts, outs = (gate_raw, up_raw, down_raw), (gate_cut, up_cut, down_cut), (gate_out, up_out, down_out)
    hbms = (gate_hbm, up_hbm, down_hbm)
    near = [(0, 1), (1, 0), (1, 1)]
    far = [(2, 0), (2, 1), (3, 0), (3, 1)]
    index = {t: i for i, t in enumerate(near + far)}
    mine = lax.rem(f, quad)
    rows_send, relay_send, y_send, t_send, k_send, p_send, n_send, c_send, e_send, o_send = [x_send.at[i] for i in range(10)]

    def at_door(act, otherwise=None):
        @pl.when(is_door)
        def _():
            act()

        if otherwise is not None:
            at_end(otherwise)

    def at_end(act):
        @pl.when(z != door)
        def _():
            act()

    def level(s):
        return (z, z + 1 - 2 * low, 2 - side, 3 - 3 * side)[s]

    def peer(t):
        return level(t[0]) * 2 + (1 - y if t[1] else y)

    def there(t):
        return index[t] if t[0] < 2 else len(near) + 2 * role + t[1]

    def cols(q):
        return pl.ds(pl.multiple_of(q * half, half), half)

    def seat(b):
        return pl.ds(pl.multiple_of(b * slots, slots), slots)

    def pair(s):
        return pl.ds(pl.multiple_of(level(s) * (2 * slots), 2 * slots), 2 * slots)

    def place(w, block):
        at = pl.ds(pl.multiple_of(block * depth, depth), depth)
        return outs[w].at[0, at, :] if w < 2 else outs[w].at[0, :, at]

    def local(block, send, recv):
        return remote(block, block, send, recv, {"tp": 1 - p})

    def w_copy(w, t):
        to = peer(t)
        return remote(cuts[w].at[to], place(w, g * n_fs + f), w_send.at[w], w_recv.at[w, there(t)], {"fs": to})

    def g_copy(w, t):
        b = g * n_fs + peer(t)
        src = cuts[w].at[f] if t == (0, 0) else place(w, b)
        return remote(src, place(w, b), g_send.at[w], g_recv.at[0] if w == 0 else d_recv.at[(w - 1) * 4 + t[0]], {"gr": 1 - g})

    def pass_on(w, *ts):
        for t in ts:
            local(place(w, g * n_fs + peer(t)), w_send.at[w], w_recv.at[w, index[t]]).wait_recv()
            g_copy(w, t).start()

    def ready(s):
        local(down_out.at[0, :, pl.ds(0, strip)], g_send.at[2], d_recv.at[4 + s]).wait_recv()

    def row_copy(s):
        if s == 1:
            return remote(rows_own.at[:, cols(p)], line_in.at[0], rows_send, x_recv.at[0], {"fs": peer((1, 0))})
        return remote(rows_own.at[:, cols(p)], line_in.at[1 + role], rows_send, x_recv.at[1 + role], {"fs": peer((2, 0))})

    def relay_copy(s):
        return remote(line_in.at[s - 1], line_in.at[s - 1], relay_send, x_recv.at[s - 1], {"fs": peer((1, 0))})

    def y_copy(s):
        return remote(y_pick.at[s], picked.at[seat(peer((s, 0))), cols(p)], y_send, y_recv.at[s], {"fs": peer((0, 1))})

    def tp_copy(t):
        block = picked.at[seat(peer(t)), cols(p)]
        return remote(block, block, t_send, t_recv.at[t[0]], {"tp": 1 - p})

    def take_y(s):
        local(picked.at[seat(peer((s, 1))), cols(p)], y_send, y_recv.at[s]).wait_recv()
        tp_copy((s, 1)).start()

    def key_copy(s):
        return remote(meta.at[f], meta.at[f], k_send, k_recv.at[s if s < 2 else 2 + role], {"fs": peer((s, 0))})

    def cut(w):
        pltpu.make_async_copy(hbms[w], raws[w], load_sem.at[w]).wait()
        if w < 2:
            scale = jnp.broadcast_to(gain[...], (128, depth)).T
            for e in range(n_fs):
                for c in range(0, raws[w].shape[2], 128):
                    cuts[w][e, :, c:c + 128] = (scale * raws[w][e, :, c:c + 128]).astype(bf16)
            outs[w][0, pl.ds(pl.multiple_of((g * n_fs + f) * depth, depth), depth), :] = cuts[w][f]
        else:
            for e in range(n_fs):
                cuts[w][e] = raws[w][e].astype(bf16)
            outs[w][0, :, pl.ds(pl.multiple_of((g * n_fs + f) * depth, depth), depth)] = cuts[w][f]

    def pick(b, expert, rows):
        wanted = (expert * slots + lax.broadcasted_iota(jnp.int32, (slots, count), 0)).astype(f32)
        hit = ((meta[b, 0:1, :] == wanted) | (meta[b, 1:2, :] == wanted)).astype(f32).astype(bf16)
        return jnp.dot(hit, rows, preferred_element_type=f32).astype(bf16)

    def shares(b):
        wanted = (side * (quad * slots) + lax.broadcasted_iota(jnp.int32, (quad * slots, count), 0)).astype(f32)
        table = jnp.where(meta[b, 0:1, :] == wanted, meta[b, 2:3, :], 0.0) + jnp.where(
            meta[b, 1:2, :] == wanted, meta[b, 3:4, :], 0.0)
        return table.T.astype(bf16)

    def take_line(s, relay):
        local(line_in.at[s - 1], rows_send, x_recv.at[s - 1]).wait_recv()
        if relay:
            relay_copy(s).start()
        b = peer((s, 0))
        local(meta.at[b], k_send, k_recv.at[s]).wait_recv()
        y_pick[s] = pick(b, peer((0, 1)), line_in[s - 1])
        picked[seat(b), cols(p)] = pick(b, f, line_in[s - 1])
        y_copy(s).start()
        tp_copy((s, 0)).start()

    def whole_gate():
        local(gate_out.at[0, pl.ds(0, n_fs * depth), :], g_send.at[0], g_recv.at[0]).wait_recv()

    def up_ready(s):
        local(up_out.at[0, pl.ds(0, strip), :], g_send.at[1], d_recv.at[s]).wait_recv()

    def up_part(s, start, size):
        k = pl.ds(pl.multiple_of(start, size), size)
        return jnp.dot(picked[pair(s), k], up_out[0, k, :], preferred_element_type=f32)

    def up_strip(s, layer):
        return up_part(s, (1 - g) * n_fs * depth + level(layer) * strip, strip)

    def up_of(s):
        up_act[pair(s), :] = up_part(s, g * n_fs * depth, n_fs * depth) + up_strip(s, 0) + up_strip(s, 1) + up_strip(s, 3)

    def gate_of(s):
        blocks = 1 if s == 0 else 2
        local(picked.at[pl.ds(0, blocks * slots), pl.ds(0, half)], t_send, t_recv.at[s]).wait_recv()
        gate_act[pair(s), :] = jnp.dot(picked[pair(s), :], gate_out[0], preferred_element_type=f32)

    barrier = pltpu.get_barrier_semaphore()
    heard = 0
    for name, size in sizes.items():
        me = lax.axis_index(name)
        for k in range(1, size):
            pl.semaphore_signal(barrier, inc=1, device_id={name: lax.rem(me + k, size)}, device_id_type=MESH)
            heard += 1
    loads = [pltpu.make_async_copy(src, dst, load_sem.at[3 + i]) for i, (src, dst) in enumerate(
        [(ids_hbm, ids), (score_hbm, score), (tokens_hbm, tokens), (gain_hbm, gain)])]
    for c in loads:
        c.start()
    for w in range(3):
        pltpu.make_async_copy(hbms[w], raws[w], load_sem.at[w]).start()
    loads[0].wait()
    loads[1].wait()
    expert = lax.broadcasted_iota(jnp.int32, (16, count), 0)
    names = ((ids[0:1, :] == expert) | (ids[1:2, :] == expert)).astype(f32).astype(bf16)
    earlier = lax.broadcasted_iota(jnp.int32, (count, count), 0) < lax.broadcasted_iota(jnp.int32, (count, count), 1)
    rank = jnp.dot(names, earlier.astype(f32).astype(bf16), preferred_element_type=f32) + (expert * slots).astype(f32)
    both = score[0:1, :] + score[1:2, :]
    table = [jnp.sum(jnp.where(ids[k:k + 1, :] == expert, rank, 0.0), axis=0, keepdims=True) for k in range(2)]
    table += [score[k:k + 1, :] / both for k in range(2)]
    for i in range(4):
        meta[f, i:i + 1, :] = table[i]
    meta[f, 4:8, :] = jnp.zeros((4, count), f32)
    loads[2].wait()
    for r in range(0, count, 32):
        x = tokens[r:r + 32, :].astype(f32)
        rows_own[r:r + 32, :] = (x * lax.rsqrt(jnp.mean(x * x, axis=-1, keepdims=True) + epsilon)).astype(bf16)
    pl.semaphore_wait(barrier, heard)
    for s in range(1, 4):
        key_copy(s).start()
    row_copy(1).start()
    row_copy(2).start()
    y_pick[0] = pick(f, peer((0, 1)), rows_own[:, cols(p)])
    loads[3].wait()
    y_copy(0).start()
    cut(0)
    for t in near:
        w_copy(0, t).start()
    g_copy(0, (0, 0)).start()
    cut(1)
    for w, ts in [(1, near), (0, far), (1, far)]:
        for t in ts:
            w_copy(w, t).start()
    g_copy(1, (0, 0)).start()
    cut(2)
    w_copy(2, (0, 1)).start()
    g_copy(2, (0, 0)).start()

    def early_down():
        w_copy(2, (1, 0)).start()
        w_copy(2, (1, 1)).start()

    at_end(early_down)
    for c in range(0, width, 512):
        picked[seat(f), c:c + 512] = pick(f, f, rows_own[:, c:c + 512])
    near_w[...] = shares(f)
    take_y(0)
    pass_on(0, (0, 1))
    pass_on(1, (0, 1))
    take_line(1, False)
    at_door(lambda: take_line(2, True))
    pass_on(0, (1, 0), (1, 1))
    at_door(lambda: take_line(3, True))
    pass_on(1, (1, 0), (1, 1))

    def gate_shares():
        for i in range(2):
            gate_w[i] = shares(peer((2 + i, 0)))

    at_door(gate_shares)
    pass_on(0, (3, 0), (3, 1))
    pass_on(0, (2, 0))
    at_end(lambda: take_line(2, False))
    at_door(lambda: pass_on(0, (2, 1)))
    take_y(1)

    def take_both():
        take_y(2)
        take_y(3)

    at_door(take_both)
    pass_on(2, (0, 1))
    pass_on(1, (3, 0), (3, 1))
    at_end(lambda: pass_on(0, (2, 1)))
    at_end(lambda: take_line(3, False))
    at_end(lambda: take_y(2))

    def far_down():
        for t in far:
            w_copy(2, t).start()

    whole_gate()
    for s in (1, 0, 2):
        gate_of(s)
    at_door(lambda: gate_of(3))
    pass_on(1, (2, 0), (2, 1))
    at_door(early_down)
    far_down()
    at_door(lambda: pass_on(2, (1, 0), (1, 1)))
    for layer in (0, 1, 3):
        up_ready(layer)
    for s in (2, 1, 0):
        up_of(s)
    at_door(lambda: up_of(3))
    up_ready(2)
    order = [2, 1, 3, 0]

    def act(s):
        gated = gate_act[pair(s), :]
        raised = up_act[pair(s), :] + up_strip(s, 2)
        hidden[pair(s), :] = (gated / (1.0 + jnp.exp(-gated)) * raised).astype(bf16)

    def here(st, base=0):
        layer = (3 * side, door, 3 - 3 * side, 2 - side)[st]
        return pl.ds(pl.multiple_of(base + layer * strip, strip), strip)

    def p_copy(st, s):
        return remote(part.at[pair(s), here(st, (1 - p) * half)], held.at[pair(s), here(st)], p_send, p_recv.at[st, s], {"tp": 1 - p})

    def n_copy(st, t):
        return remote(total.at[seat(peer(t)), here(st)], back.at[seat(mine), here(st)], n_send, n_recv.at[max(st - 1, 0)],
                      {"fs": peer(t)})

    def c_copy(st, t):
        return remote(total.at[seat(peer(t)), here(st)], collect.at[t[0] - 2, seat(mine), here(st)], c_send if t[1] else e_send,
                      c_recv.at[st, t[0] - 2], {"fs": door * 2 + (1 - y if t[1] else y)})

    def o_copy(st, i):
        return remote(far_out.at[i, :, here(st)], far_in.at[:, here(st)], o_send, o_recv.at[st], {"fs": peer((2 + i, 0))})

    def spread(st, s):
        for q in range(2):
            part[pair(s), here(st, q * half)] = jnp.dot(
                hidden[pair(s), :], down_out[0, :, here(st, q * half)], preferred_element_type=f32).astype(bf16)

    def add(st, s):
        p_copy(st, s).wait_recv()
        total[pair(s), here(st)] = (part[pair(s), here(st, p * half)].astype(f32) + held[pair(s), here(st)].astype(f32)).astype(bf16)

    def send(st, s):
        for dy in range(2):
            t = (s, dy)
            if t == (0, 0):
                back[seat(mine), here(st)] = total[seat(f), here(st)]
            elif s == 0:
                n_copy(st, t).start()
            elif dy and s > 1:
                c_copy(st, t).start()
            elif s > 1:
                def keep():
                    collect[s - 2, seat(mine), here(st)] = total[seat(peer(t)), here(st)]

                at_door(keep, lambda: c_copy(st, t).start())

    def first():
        for i in range(len(order) + 1):
            if i < len(order):
                if order[i] == 3:
                    def rest():
                        gate_of(3)
                        up_of(3)

                    at_end(rest)
                act(order[i])
            if i:
                add(0, order[i - 1])
            if i < len(order):
                spread(0, order[i])
            if i:
                send(0, order[i - 1])
            if i < len(order):
                p_copy(0, order[i]).start()
            if i == 0:
                at_end(lambda: take_y(3))
                at_end(lambda: pass_on(2, (1, 0), (1, 1)))
        give_near(0)

    later = [3, 2, 1, 0]

    def compute(st):
        for i, s in enumerate(later):
            spread(st, s)
            if i:
                p_copy(st, later[i - 1]).start()
        p_copy(st, later[-1]).start()

    def give(st):
        for i, s in enumerate(later):
            add(st, s)
            if i:
                send(st, later[i - 1])
        send(st, later[-1])

    def give_near(st):
        n_copy(st, (1, 0)).start()
        n_copy(st, (1, 1)).start()

    def merge(st):
        def act():
            for i in (1, 0):
                local(collect.at[i, pl.ds(0, (quad - 1) * slots), here(st)], c_send, c_recv.at[st, i]).wait_recv()
                far_out[i, :, here(st)] = jnp.dot(gate_w[i], collect[i, :, here(st)], preferred_element_type=f32).astype(bf16)
                o_copy(st, i).start()

        at_door(act)

    def far_wait(st):
        layer = (3 - 3 * side, 2 - side, 3 * side, door)[st]
        local(far_in.at[:, pl.ds(pl.multiple_of(layer * strip, strip), strip)], o_send, o_recv.at[st]).wait_recv()

    at_door(lambda: ready(1), lambda: ready(0))
    first()

    at_door(lambda: ready(0), lambda: ready(1))
    compute(1)
    give(1)
    at_door(lambda: give_near(1))
    pass_on(2, (3, 0), (3, 1))
    merge(0)
    pass_on(2, (2, 0), (2, 1))
    ready(3)
    compute(2)
    give(2)
    at_door(lambda: give_near(2))
    merge(1)
    ready(2)
    compute(3)
    give(3)
    give_near(3)

    def rest_near():
        give_near(1)
        give_near(2)

    at_end(rest_near)
    merge(2)
    merge(3)
    local(back.at[pl.ds(0, 3 * slots // 2), :], n_send, n_recv.at[0]).wait_recv()
    sided = pl.ds(pl.multiple_of(side * span, span), span)
    acc = jnp.dot(near_w[...], back[:, sided], preferred_element_type=f32)
    far_wait(0)
    far_wait(1)
    for st in (2, 3):
        local(back.at[pl.ds(0, 3 * slots // 4), :], n_send, n_recv.at[st - 1]).wait_recv()
        more = jnp.dot(near_w[...], back[:, here(st)], preferred_element_type=f32)
        mixed[:, here(st)] = (more + far_in[:, here(st)].astype(f32)).astype(bf16)
    far_wait(2)
    far_wait(3)
    mixed[:, sided] = (acc + far_in[:, sided].astype(f32)).astype(bf16)

    def sent(block, send):
        local(block, send, o_recv.at[0]).wait_send()

    for w in range(3):
        sent(cuts[w].at[pl.ds(0, n_fs - 1)], w_send.at[w])
        sent(cuts[w], g_send.at[w])
    sent(rows_own, rows_send)
    sent(y_pick, y_send)
    sent(picked.at[pl.ds(0, (n_fs - 1) * slots), pl.ds(0, half)], t_send)
    sent(meta.at[pl.ds(0, 3)], k_send)
    sent(held, p_send)
    sent(held.at[pl.ds(0, 3 * slots), :], n_send)
    sent(held.at[pl.ds(0, 2 * slots), :], c_send)
    at_door(lambda: sent(line_in.at[pl.ds(0, 2)], relay_send), lambda: sent(held.at[pl.ds(0, 2 * slots), :], e_send))
    at_door(lambda: sent(far_out, o_send))


def store_kernel(*refs):
    sems = refs[-1]
    pairs = list(zip(refs[:4], refs[4:8]))
    copies = [pltpu.make_async_copy(src, dst, sems.at[i]) for i, (src, dst) in enumerate(pairs)]
    for c in copies:
        c.start()
    for c in copies:
        c.wait()


def run_handover(sizes, slots, tokens, norm_gain, gate_train, up_train, down_train, expert_ids, route_score):
    n_gr, n_fs, n_tp = sizes["gr"], sizes["fs"], sizes["tp"]
    _, depth, hid = gate_train.shape
    count, width = tokens.shape
    half, quad = width // n_tp, n_fs // 2
    bf16, f32, dma = jnp.bfloat16, jnp.float32, pltpu.SemaphoreType.DMA
    vmem, hbm = pl.BlockSpec(memory_space=pltpu.VMEM), pl.BlockSpec(memory_space=pltpu.HBM)
    shapes = [(1, width, hid), (1, width, hid), (1, hid, width), (count, half)]
    made = pl.pallas_call(
        functools.partial(handover_kernel, sizes),
        out_shape=[pltpu.VMEM(shape, bf16) for shape in shapes],
        in_specs=[hbm] * 7,
        out_specs=[vmem] * 4,
        scratch_shapes=[
            pltpu.VMEM((count, width), bf16), pltpu.VMEM((1, depth), f32), pltpu.VMEM((2, count), jnp.int32), pltpu.VMEM((2, count), f32),
            pltpu.VMEM((n_fs, depth, hid), f32), pltpu.VMEM((n_fs, depth, hid), f32), pltpu.VMEM((n_fs, hid, depth), f32),
            pltpu.VMEM((n_fs, depth, hid), bf16), pltpu.VMEM((n_fs, depth, hid), bf16), pltpu.VMEM((n_fs, hid, depth), bf16),
            pltpu.VMEM((count, width), bf16), pltpu.VMEM((3, count, half), bf16), pltpu.VMEM((n_fs, 8, count), f32),
            pltpu.VMEM((4, slots, half), bf16),
            pltpu.VMEM((n_fs * slots, width), bf16), pltpu.VMEM((n_fs * slots, hid), f32), pltpu.VMEM((n_fs * slots, hid), f32), pltpu.VMEM((n_fs * slots, hid), bf16),
            pltpu.VMEM((n_fs * slots, width), bf16), pltpu.VMEM((n_fs * slots, half), bf16),
            pltpu.VMEM((n_fs * slots, half), bf16), pltpu.VMEM((quad * slots, half), bf16),
            pltpu.VMEM((2, quad * slots, half), bf16), pltpu.VMEM((2, count, half), bf16), pltpu.VMEM((count, half), bf16),
            pltpu.VMEM((count, quad * slots), bf16), pltpu.VMEM((2, count, quad * slots), bf16),
            dma((7,)), dma((3,)), dma((3, n_fs - 1)), dma((3,)), dma((1,)), dma((8,)), dma((10,)), dma((3,)), dma((4,)), dma((4,)), dma((4,)),
            dma((4, 4)), dma((3,)), dma((4, 2)), dma((4,)),
        ],
        compiler_params=pltpu.CompilerParams(collective_id=2, has_side_effects=True, vmem_limit_bytes=56 * 2**20),
        name="handover",
    )(tokens, norm_gain.reshape(1, depth), expert_ids.T, route_score.T, gate_train, up_train, down_train)
    return pl.pallas_call(
        store_kernel,
        out_shape=[jax.ShapeDtypeStruct(shape, bf16) for shape in shapes],
        in_specs=[vmem] * 4,
        out_specs=[pl.BlockSpec(memory_space=pl.ANY)] * 4,
        scratch_shapes=[dma((4,))],
        compiler_params=pltpu.CompilerParams(vmem_limit_bytes=16 * 2**20),
        name="store",
    )(*made)


def on_device(sizes, tokens, norm_gain, gate_train, up_train, down_train, expert_ids, route_score):
    n_gr, n_fs, n_tp = sizes["gr"], sizes["fs"], sizes["tp"]
    bf16 = jnp.bfloat16
    experts, depth, hid = gate_train.shape
    local = experts // n_fs
    count, width = tokens.shape
    capacity = 4 * count // experts
    direct_down = depth % 128 == 0
    if direct_down and local == 1 and capacity % 128 == 0 and (n_gr, n_fs, n_tp) == (2, 8, 2):
        return run_handover(sizes, capacity, tokens, norm_gain, gate_train, up_train, down_train, expert_ids, route_score)

    gate_cast = (norm_gain[None, :, None] * gate_train).astype(bf16)
    up_cast = (norm_gain[None, :, None] * up_train).astype(bf16)
    down_cast = down_train.astype(bf16)
    floated = tokens.astype(jnp.float32)
    normed = (floated * lax.rsqrt(jnp.mean(floated * floated, axis=-1, keepdims=True) + epsilon)).astype(bf16)

    named = expert_ids[:, :, None] == jnp.arange(experts, dtype=jnp.int32)
    names = jnp.any(named, axis=1)
    earlier = jnp.arange(count)[:, None] > jnp.arange(count)[None, :]
    rank = jnp.dot(earlier.astype(bf16), names.astype(bf16), preferred_element_type=jnp.float32).astype(jnp.int32)
    slot = expert_ids * capacity + jnp.sum(jnp.where(named, rank[:, None, :], 0), axis=2)
    keys = jnp.concatenate([slot.T, jnp.full((6, count), -1, jnp.int32)], axis=0)

    share = route_score / jnp.sum(route_score, axis=-1, keepdims=True)
    down_shape = (local, hid, n_gr * n_fs * depth) if direct_down else (n_gr * n_fs, local, hid, depth)
    dma = pltpu.SemaphoreType.DMA
    gate_ready, up_ready, down_ready, gathered, all_keys = pl.pallas_call(
        functools.partial(spread_kernel, sizes, local, direct_down),
        out_shape=(
            jax.ShapeDtypeStruct((local, n_gr * n_fs * depth, hid), bf16),
            jax.ShapeDtypeStruct((local, n_gr * n_fs * depth, hid), bf16),
            jax.ShapeDtypeStruct(down_shape, bf16),
            jax.ShapeDtypeStruct((n_fs, count, width), bf16),
            jax.ShapeDtypeStruct((n_fs, 8, count), jnp.int32),
        ),
        in_specs=[pl.BlockSpec(memory_space=pltpu.VMEM)] * 5,
        out_specs=[pl.BlockSpec(memory_space=pl.ANY)] * 5,
        scratch_shapes=[
            dma((3, n_fs)), dma((3, n_fs)), dma((3, n_fs, n_gr)), dma((3, n_fs, n_gr)),
            dma((n_fs,)), dma((n_fs,)), dma((n_fs,)), dma((n_fs,)),
            dma((n_tp, n_fs)), dma((n_tp, n_fs)), dma((n_fs,)), dma((n_fs,)), dma((5,)),
        ],
        compiler_params=pltpu.CompilerParams(collective_id=0, has_side_effects=True),
        name="spread",
    )(gate_cast, up_cast, down_cast, normed, keys)
    if not direct_down:
        down_ready = down_ready.transpose(1, 2, 0, 3).reshape(local, hid, -1)

    wanted = (lax.axis_index("fs") * local * capacity + jnp.arange(local * capacity, dtype=jnp.int32))[None, :, None]
    pick = ((all_keys[:, 0][:, None, :] == wanted) | (all_keys[:, 1][:, None, :] == wanted)).astype(bf16)
    rows = jnp.einsum("sct,std->scd", pick, gathered, preferred_element_type=jnp.float32).astype(bf16)
    rows = rows.reshape(n_fs, local, capacity, width)
    gate_act = jnp.einsum("seck,ekh->sech", rows, gate_ready, preferred_element_type=jnp.float32)
    up_act = jnp.einsum("seck,ekh->sech", rows, up_ready, preferred_element_type=jnp.float32)
    hidden = (jax.nn.silu(gate_act) * up_act).astype(bf16)
    part = jnp.einsum("sech,ehk->seck", hidden, down_ready, preferred_element_type=jnp.float32).astype(bf16)
    part = part.reshape(n_fs, local * capacity, width)
    half = width // n_tp
    returned = pl.pallas_call(
        functools.partial(return_kernel, sizes),
        out_shape=jax.ShapeDtypeStruct((n_fs, local * capacity, half), bf16),
        in_specs=[pl.BlockSpec(memory_space=pltpu.VMEM)],
        out_specs=pl.BlockSpec(memory_space=pltpu.VMEM),
        scratch_shapes=[
            pltpu.VMEM((max(n_tp - 1, 1), n_fs, local * capacity, half), bf16),
            pltpu.VMEM((n_fs, local * capacity, half), bf16),
            dma((n_tp, n_fs)), dma((n_tp, n_fs)), dma((n_fs,)), dma((n_fs,)),
        ],
        compiler_params=pltpu.CompilerParams(collective_id=1, has_side_effects=True),
        name="giveback",
    )(part)
    at = jnp.arange(experts * capacity, dtype=jnp.int32)[None, :]
    weight = jnp.where(slot[:, :1] == at, share[:, :1], 0.0) + jnp.where(slot[:, 1:] == at, share[:, 1:], 0.0)
    mixed = jnp.dot(weight.astype(bf16), returned.reshape(experts * capacity, half), preferred_element_type=jnp.float32)
    return gate_ready, up_ready, down_ready, mixed.astype(bf16)


def solution(mesh):
    return jax.shard_map(
        functools.partial(on_device, dict(mesh.shape)),
        mesh=mesh,
        in_specs=(
            P(("gr", "fs"), None),
            P(("gr", "fs")),
            P(None, ("gr", "fs"), "tp"),
            P(None, ("gr", "fs"), "tp"),
            P(None, "tp", ("gr", "fs")),
            P(("gr", "fs"), None),
            P(("gr", "fs"), None),
        ),
        out_specs=(
            P("fs", None, "tp"),
            P("fs", None, "tp"),
            P("fs", "tp", None),
            P(("gr", "fs"), "tp"),
        ),
        check_vma=False,
    )
```

```python
import functools

import jax
import jax.numpy as jnp
from jax import lax
from jax.experimental import pallas as pl
from jax.experimental.pallas import tpu as pltpu
from jax.sharding import PartitionSpec as P

epsilon = 1e-06
MESH = pl.DeviceIdType.MESH


def remote(src, dst, send_sem, recv_sem, where):
    return pltpu.make_async_remote_copy(
        src_ref=src, dst_ref=dst, send_sem=send_sem, recv_sem=recv_sem, device_id=where, device_id_type=MESH
    )


def greet(sizes):
    barrier = pltpu.get_barrier_semaphore()
    count = 0
    for name, size in sizes.items():
        me = lax.axis_index(name)
        for k in range(1, size):
            pl.semaphore_signal(barrier, inc=1, device_id={name: lax.rem(me + k, size)}, device_id_type=MESH)
            count += 1
    pl.semaphore_wait(barrier, count)


def spread_kernel(sizes, local, direct_down, gate, up, down, rows, keys, gate_out, up_out, down_out, rows_out, keys_out,
                  w_send, w_recv, g_send, g_recv, up_send, low_send, y_send, x_recv, t_send, t_recv, k_send, k_recv, own_sem):
    n_gr, n_fs, n_tp = sizes["gr"], sizes["fs"], sizes["tp"]
    g, f, p = lax.axis_index("gr"), lax.axis_index("fs"), lax.axis_index("tp")
    inner = 2 if n_fs % 2 == 0 else 1
    lines = n_fs // inner
    z, y = f // inner, lax.rem(f, inner)
    depth = gate.shape[1]
    half = rows.shape[1] // n_tp
    cols = pl.ds(pl.multiple_of(p * half, half), half)
    sources, outs = (gate, up, down), (gate_out, up_out, down_out)

    def place(w, block):
        start = pl.multiple_of(block * depth, depth)
        if w < 2:
            return outs[w].at[:, pl.ds(start, depth), :]
        return outs[w].at[:, :, pl.ds(start, depth)] if direct_down else outs[w].at[block]

    greet(sizes)

    own = [pltpu.make_async_copy(rows, rows_out.at[f], own_sem.at[0]),
           pltpu.make_async_copy(keys, keys_out.at[f], own_sem.at[1])]
    for w in range(3):
        own.append(pltpu.make_async_copy(sources[w].at[pl.ds(f * local, local)], place(w, g * n_fs + f), own_sem.at[2 + w]))

    def block_of(b):
        return rows_out.at[b, :, cols]

    def row_copy(b, first, kind, where):
        src = rows.at[:, cols] if first else block_of(b)
        return remote(src, block_of(b), {"u": up_send, "d": low_send, "y": y_send}[kind].at[b], x_recv.at[b], where)

    def tp_copy(b, j):
        return remote(block_of(b), block_of(b), t_send.at[j, b], t_recv.at[j, b], {"tp": lax.rem(p + j + 1, n_tp)})

    def go_up(b, first, act):
        @pl.when(z < lines - 1)
        def _():
            act(row_copy(b, first, "u", {"fs": lax.rem(f + inner, n_fs)}))

    def go_down(b, first, act):
        @pl.when(z > 0)
        def _():
            act(row_copy(b, first, "d", {"fs": lax.rem(f + n_fs - inner, n_fs)}))

    def go_side(b, first, act):
        if inner == 2:
            act(row_copy(b, first, "y", {"fs": f + 1 - 2 * y}))

    def start(c):
        c.start()

    def recv(c):
        c.wait_recv()

    def sent(c):
        c.wait_send()

    go_up(f, True, start)
    go_down(f, True, start)
    go_side(f, True, start)
    key_copies = []
    for k in range(1, n_fs):
        to = lax.rem(f + k, n_fs)
        c = remote(keys, keys_out.at[f], k_send.at[k], k_recv.at[k], {"fs": to})
        c.start()
        key_copies.append(c)
    for c in own:
        c.start()

    def gr_copy(w, b, k, j, first):
        src = sources[w].at[pl.ds(f * local, local)] if first else place(w, b)
        return remote(src, place(w, b), g_send.at[w, k, j], g_recv.at[w, k, j], {"gr": lax.rem(g + j + 1, n_gr)})

    for w in range(3):
        for j in range(n_gr - 1):
            gr_copy(w, g * n_fs + f, 0, j, True).start()

    for s in range(1, lines):
        @pl.when(z >= s)
        def _():
            b = f - s * inner
            row_copy(b, False, "u", {"fs": lax.rem(f + inner, n_fs)}).wait_recv()
            go_up(b, False, start)
            go_side(b, False, start)
            for j in range(n_tp - 1):
                tp_copy(b, j).start()

        @pl.when(z < lines - s)
        def _():
            b = f + s * inner
            row_copy(b, False, "d", {"fs": lax.rem(f + inner, n_fs)}).wait_recv()
            go_down(b, False, start)
            go_side(b, False, start)
            for j in range(n_tp - 1):
                tp_copy(b, j).start()

    def w_copy(w, k):
        to = lax.rem(f + k, n_fs)
        return remote(sources[w].at[pl.ds(to * local, local)], place(w, g * n_fs + f), w_send.at[w, k], w_recv.at[w, k], {"fs": to})

    for w in range(3):
        for k in range(1, n_fs):
            w_copy(w, k).start()

    if inner == 2:
        for s in range(lines):
            b = lax.rem(z + s, lines) * inner + 1 - y
            row_copy(b, False, "y", {"fs": f + 1 - 2 * y}).wait_recv()
            for j in range(n_tp - 1):
                tp_copy(b, j).start()

    for w in range(3):
        for k in range(1, n_fs):
            w_copy(w, k).wait_recv()
            b = g * n_fs + lax.rem(f + n_fs - k, n_fs)
            for j in range(n_gr - 1):
                gr_copy(w, b, k, j, False).start()

    for k in range(1, n_fs):
        b = lax.rem(f + k, n_fs)
        for j in range(n_tp - 1):
            c = tp_copy(b, j)
            c.wait_recv()
            c.wait_send()
    for c in key_copies:
        c.wait_recv()
        c.wait_send()
    for c in own:
        c.wait()
    go_up(f, True, sent)
    go_down(f, True, sent)
    go_side(f, True, sent)
    for s in range(1, lines):
        @pl.when(z >= s)
        def _():
            go_up(f - s * inner, False, sent)
            go_side(f - s * inner, False, sent)

        @pl.when(z < lines - s)
        def _():
            go_down(f + s * inner, False, sent)
            go_side(f + s * inner, False, sent)
    for w in range(3):
        for k in range(n_fs):
            if k:
                w_copy(w, k).wait_send()
            for j in range(n_gr - 1):
                c = gr_copy(w, g * n_fs + lax.rem(f + n_fs - k, n_fs), k, j, False)
                c.wait_recv()
                c.wait_send()


def return_kernel(sizes, part, out, held, total, t_send, t_recv, f_send, f_recv):
    n_fs, n_tp = sizes["fs"], sizes["tp"]
    f, p = lax.axis_index("fs"), lax.axis_index("tp")
    half = part.shape[2] // n_tp

    def cols(q):
        return pl.ds(pl.multiple_of(q * half, half), half)

    greet({"fs": n_fs, "tp": n_tp})
    order = list(range(1, n_fs)) + [0]

    def tp_copy(k, j):
        to = lax.rem(p + j + 1, n_tp)
        b = lax.rem(f + k, n_fs)
        return remote(part.at[b, :, cols(to)], held.at[j, b], t_send.at[j, k], t_recv.at[j, k], {"tp": to})

    def f_copy(k):
        b = lax.rem(f + k, n_fs)
        return remote(total.at[b], out.at[f], f_send.at[k], f_recv.at[k], {"fs": b})

    for k in order:
        for j in range(n_tp - 1):
            tp_copy(k, j).start()
    for k in order:
        b = lax.rem(f + k, n_fs)
        value = part[b, :, cols(p)].astype(jnp.float32)
        for j in range(n_tp - 1):
            tp_copy(k, j).wait_recv()
            value = value + held[j, b].astype(jnp.float32)
        value = value.astype(jnp.bfloat16)
        if k == 0:
            out[b] = value
        else:
            total[b] = value
            f_copy(k).start()
    for k in order:
        for j in range(n_tp - 1):
            tp_copy(k, j).wait_send()
        if k:
            f_copy(k).wait_recv()
            f_copy(k).wait_send()


def handover_kernel(sizes, tokens_hbm, gain_hbm, ids_hbm, score_hbm, gate_hbm, up_hbm, down_hbm, gate_out, up_out, down_out, mixed,
                    tokens, gain, ids, score, gate_raw, up_raw, down_raw, gate_cut, up_cut, down_cut, rows_own, line_in, meta, y_pick,
                    picked, gate_act, up_act, hidden, part, held, total, back, collect, far_out, far_in, near_w, gate_w,
                    load_sem, w_send, w_recv, g_send, g_recv, d_recv, x_send, x_recv, y_recv, k_recv, t_recv, p_recv, n_recv, c_recv, o_recv):
    n_fs = sizes["fs"]
    g, f, p = lax.axis_index("gr"), lax.axis_index("fs"), lax.axis_index("tp")
    z, y = f // 2, lax.rem(f, 2)
    low, side = lax.rem(z, 2), z // 2
    door = 1 + side
    is_door = z == door
    role = 1 - (low + side - 2 * low * side)
    depth = gate_hbm.shape[1]
    count, width = tokens.shape
    slots = back.shape[0] * 2 // n_fs
    half = width // 2
    span = half // 2
    strip = 2 * depth
    quad = n_fs // 2
    bf16, f32 = jnp.bfloat16, jnp.float32
    raws, cuts, outs = (gate_raw, up_raw, down_raw), (gate_cut, up_cut, down_cut), (gate_out, up_out, down_out)
    hbms = (gate_hbm, up_hbm, down_hbm)
    near = [(0, 1), (1, 0), (1, 1)]
    far = [(2, 0), (2, 1), (3, 0), (3, 1)]
    index = {t: i for i, t in enumerate(near + far)}
    mine = lax.rem(f, quad)
    rows_send, relay_send, y_send, t_send, k_send, p_send, n_send, c_send, e_send, o_send = [x_send.at[i] for i in range(10)]

    def at_door(act, otherwise=None):
        @pl.when(is_door)
        def _():
            act()

        if otherwise is not None:
            at_end(otherwise)

    def at_end(act):
        @pl.when(z != door)
        def _():
            act()

    def level(s):
        return (z, z + 1 - 2 * low, 2 - side, 3 - 3 * side)[s]

    def peer(t):
        return level(t[0]) * 2 + (1 - y if t[1] else y)

    def there(t):
        return index[t] if t[0] < 2 else len(near) + 2 * role + t[1]

    def cols(q):
        return pl.ds(pl.multiple_of(q * half, half), half)

    def seat(b):
        return pl.ds(pl.multiple_of(b * slots, slots), slots)

    def pair(s):
        return pl.ds(pl.multiple_of(level(s) * (2 * slots), 2 * slots), 2 * slots)

    def place(w, block):
        at = pl.ds(pl.multiple_of(block * depth, depth), depth)
        return outs[w].at[0, at, :] if w < 2 else outs[w].at[0, :, at]

    def local(block, send, recv):
        return remote(block, block, send, recv, {"tp": 1 - p})

    def w_copy(w, t):
        to = peer(t)
        return remote(cuts[w].at[to], place(w, g * n_fs + f), w_send.at[w], w_recv.at[w, there(t)], {"fs": to})

    def g_copy(w, t):
        b = g * n_fs + peer(t)
        src = cuts[w].at[f] if t == (0, 0) else place(w, b)
        return remote(src, place(w, b), g_send.at[w], g_recv.at[0] if w == 0 else d_recv.at[(w - 1) * 4 + t[0]], {"gr": 1 - g})

    def pass_on(w, *ts):
        for t in ts:
            local(place(w, g * n_fs + peer(t)), w_send.at[w], w_recv.at[w, index[t]]).wait_recv()
            g_copy(w, t).start()

    def ready(s):
        local(down_out.at[0, :, pl.ds(0, strip)], g_send.at[2], d_recv.at[4 + s]).wait_recv()

    def row_copy(s):
        if s == 1:
            return remote(rows_own.at[:, cols(p)], line_in.at[0], rows_send, x_recv.at[0], {"fs": peer((1, 0))})
        return remote(rows_own.at[:, cols(p)], line_in.at[1 + role], rows_send, x_recv.at[1 + role], {"fs": peer((2, 0))})

    def relay_copy(s):
        return remote(line_in.at[s - 1], line_in.at[s - 1], relay_send, x_recv.at[s - 1], {"fs": peer((1, 0))})

    def y_copy(s):
        return remote(y_pick.at[s], picked.at[seat(peer((s, 0))), cols(p)], y_send, y_recv.at[s], {"fs": peer((0, 1))})

    def tp_copy(t):
        block = picked.at[seat(peer(t)), cols(p)]
        return remote(block, block, t_send, t_recv.at[t[0]], {"tp": 1 - p})

    def take_y(s):
        local(picked.at[seat(peer((s, 1))), cols(p)], y_send, y_recv.at[s]).wait_recv()
        tp_copy((s, 1)).start()

    def key_copy(s):
        return remote(meta.at[f], meta.at[f], k_send, k_recv.at[s if s < 2 else 2 + role], {"fs": peer((s, 0))})

    def cut(w):
        pltpu.make_async_copy(hbms[w], raws[w], load_sem.at[w]).wait()
        if w < 2:
            scale = jnp.broadcast_to(gain[...], (128, depth)).T
            for e in range(n_fs):
                for c in range(0, raws[w].shape[2], 128):
                    cuts[w][e, :, c:c + 128] = (scale * raws[w][e, :, c:c + 128]).astype(bf16)
            outs[w][0, pl.ds(pl.multiple_of((g * n_fs + f) * depth, depth), depth), :] = cuts[w][f]
        else:
            for e in range(n_fs):
                cuts[w][e] = raws[w][e].astype(bf16)
            outs[w][0, :, pl.ds(pl.multiple_of((g * n_fs + f) * depth, depth), depth)] = cuts[w][f]

    def pick(b, expert, rows):
        wanted = (expert * slots + lax.broadcasted_iota(jnp.int32, (slots, count), 0)).astype(f32)
        hit = ((meta[b, 0:1, :] == wanted) | (meta[b, 1:2, :] == wanted)).astype(f32).astype(bf16)
        return jnp.dot(hit, rows, preferred_element_type=f32).astype(bf16)

    def shares(b):
        wanted = (side * (quad * slots) + lax.broadcasted_iota(jnp.int32, (quad * slots, count), 0)).astype(f32)
        table = jnp.where(meta[b, 0:1, :] == wanted, meta[b, 2:3, :], 0.0) + jnp.where(
            meta[b, 1:2, :] == wanted, meta[b, 3:4, :], 0.0)
        return table.T.astype(bf16)

    def take_line(s, relay):
        local(line_in.at[s - 1], rows_send, x_recv.at[s - 1]).wait_recv()
        if relay:
            relay_copy(s).start()
        b = peer((s, 0))
        local(meta.at[b], k_send, k_recv.at[s]).wait_recv()
        y_pick[s] = pick(b, peer((0, 1)), line_in[s - 1])
        picked[seat(b), cols(p)] = pick(b, f, line_in[s - 1])
        y_copy(s).start()
        tp_copy((s, 0)).start()

    def whole_gate():
        local(gate_out.at[0, pl.ds(0, n_fs * depth), :], g_send.at[0], g_recv.at[0]).wait_recv()

    def up_ready(s):
        local(up_out.at[0, pl.ds(0, strip), :], g_send.at[1], d_recv.at[s]).wait_recv()

    def up_part(s, start, size):
        k = pl.ds(pl.multiple_of(start, size), size)
        return jnp.dot(picked[pair(s), k], up_out[0, k, :], preferred_element_type=f32)

    def up_strip(s, layer):
        return up_part(s, (1 - g) * n_fs * depth + level(layer) * strip, strip)

    def up_of(s):
        up_act[pair(s), :] = up_part(s, g * n_fs * depth, n_fs * depth) + up_strip(s, 0) + up_strip(s, 1) + up_strip(s, 3)

    def gate_of(s):
        blocks = 1 if s == 0 else 2
        local(picked.at[pl.ds(0, blocks * slots), pl.ds(0, half)], t_send, t_recv.at[s]).wait_recv()
        gate_act[pair(s), :] = jnp.dot(picked[pair(s), :], gate_out[0], preferred_element_type=f32)

    barrier = pltpu.get_barrier_semaphore()
    heard = 0
    for name, size in sizes.items():
        me = lax.axis_index(name)
        for k in range(1, size):
            pl.semaphore_signal(barrier, inc=1, device_id={name: lax.rem(me + k, size)}, device_id_type=MESH)
            heard += 1
    loads = [pltpu.make_async_copy(src, dst, load_sem.at[3 + i]) for i, (src, dst) in enumerate(
        [(ids_hbm, ids), (score_hbm, score), (tokens_hbm, tokens), (gain_hbm, gain)])]
    for c in loads:
        c.start()
    for w in range(3):
        pltpu.make_async_copy(hbms[w], raws[w], load_sem.at[w]).start()
    loads[0].wait()
    loads[1].wait()
    expert = lax.broadcasted_iota(jnp.int32, (16, count), 0)
    names = ((ids[0:1, :] == expert) | (ids[1:2, :] == expert)).astype(f32).astype(bf16)
    earlier = lax.broadcasted_iota(jnp.int32, (count, count), 0) < lax.broadcasted_iota(jnp.int32, (count, count), 1)
    rank = jnp.dot(names, earlier.astype(f32).astype(bf16), preferred_element_type=f32) + (expert * slots).astype(f32)
    both = score[0:1, :] + score[1:2, :]
    table = [jnp.sum(jnp.where(ids[k:k + 1, :] == expert, rank, 0.0), axis=0, keepdims=True) for k in range(2)]
    table += [score[k:k + 1, :] / both for k in range(2)]
    for i in range(4):
        meta[f, i:i + 1, :] = table[i]
    meta[f, 4:8, :] = jnp.zeros((4, count), f32)
    loads[2].wait()
    for r in range(0, count, 32):
        x = tokens[r:r + 32, :].astype(f32)
        rows_own[r:r + 32, :] = (x * lax.rsqrt(jnp.mean(x * x, axis=-1, keepdims=True) + epsilon)).astype(bf16)
    pl.semaphore_wait(barrier, heard)
    for s in range(1, 4):
        key_copy(s).start()
    row_copy(1).start()
    row_copy(2).start()
    y_pick[0] = pick(f, peer((0, 1)), rows_own[:, cols(p)])
    loads[3].wait()
    y_copy(0).start()
    cut(0)
    for t in near:
        w_copy(0, t).start()
    g_copy(0, (0, 0)).start()
    cut(1)
    for w, ts in [(1, near), (0, far), (1, far)]:
        for t in ts:
            w_copy(w, t).start()
    g_copy(1, (0, 0)).start()
    cut(2)
    w_copy(2, (0, 1)).start()
    g_copy(2, (0, 0)).start()

    def early_down():
        w_copy(2, (1, 0)).start()
        w_copy(2, (1, 1)).start()

    at_end(early_down)
    for c in range(0, width, 512):
        picked[seat(f), c:c + 512] = pick(f, f, rows_own[:, c:c + 512])
    near_w[...] = shares(f)
    take_y(0)
    pass_on(0, (0, 1))
    pass_on(1, (0, 1))
    take_line(1, False)
    at_door(lambda: take_line(2, True))
    pass_on(0, (1, 0), (1, 1))
    at_door(lambda: take_line(3, True))
    pass_on(1, (1, 0), (1, 1))

    def gate_shares():
        for i in range(2):
            gate_w[i] = shares(peer((2 + i, 0)))

    at_door(gate_shares)
    pass_on(0, (3, 0), (3, 1))
    pass_on(0, (2, 0))
    at_end(lambda: take_line(2, False))
    at_door(lambda: pass_on(0, (2, 1)))
    take_y(1)

    def take_both():
        take_y(2)
        take_y(3)

    at_door(take_both)
    pass_on(2, (0, 1))
    pass_on(1, (3, 0), (3, 1))
    at_end(lambda: pass_on(0, (2, 1)))
    at_end(lambda: take_line(3, False))
    at_end(lambda: take_y(2))

    def far_down():
        for t in far:
            w_copy(2, t).start()

    whole_gate()
    for s in (1, 0, 2):
        gate_of(s)
    at_door(lambda: gate_of(3))
    pass_on(1, (2, 0), (2, 1))
    at_door(early_down)
    far_down()
    at_door(lambda: pass_on(2, (1, 0), (1, 1)))
    for layer in (0, 1, 3):
        up_ready(layer)
    for s in (2, 1, 0):
        up_of(s)
    at_door(lambda: up_of(3))
    up_ready(2)
    order = [2, 1, 3, 0]

    def act(s):
        gated = gate_act[pair(s), :]
        raised = up_act[pair(s), :] + up_strip(s, 2)
        hidden[pair(s), :] = (gated / (1.0 + jnp.exp(-gated)) * raised).astype(bf16)

    def here(st, base=0):
        layer = (3 * side, door, 3 - 3 * side, 2 - side)[st]
        return pl.ds(pl.multiple_of(base + layer * strip, strip), strip)

    def p_copy(st, s):
        return remote(part.at[pair(s), here(st, (1 - p) * half)], held.at[pair(s), here(st)], p_send, p_recv.at[st, s], {"tp": 1 - p})

    def n_copy(st, t):
        return remote(total.at[seat(peer(t)), here(st)], back.at[seat(mine), here(st)], n_send, n_recv.at[max(st - 1, 0)],
                      {"fs": peer(t)})

    def c_copy(st, t):
        return remote(total.at[seat(peer(t)), here(st)], collect.at[t[0] - 2, seat(mine), here(st)], c_send if t[1] else e_send,
                      c_recv.at[st, t[0] - 2], {"fs": door * 2 + (1 - y if t[1] else y)})

    def o_copy(st, i):
        return remote(far_out.at[i, :, here(st)], far_in.at[:, here(st)], o_send, o_recv.at[st], {"fs": peer((2 + i, 0))})

    def spread(st, s):
        for q in range(2):
            part[pair(s), here(st, q * half)] = jnp.dot(
                hidden[pair(s), :], down_out[0, :, here(st, q * half)], preferred_element_type=f32).astype(bf16)

    def add(st, s):
        p_copy(st, s).wait_recv()
        total[pair(s), here(st)] = (part[pair(s), here(st, p * half)].astype(f32) + held[pair(s), here(st)].astype(f32)).astype(bf16)

    def send(st, s):
        for dy in range(2):
            t = (s, dy)
            if t == (0, 0):
                back[seat(mine), here(st)] = total[seat(f), here(st)]
            elif s == 0:
                n_copy(st, t).start()
            elif dy and s > 1:
                c_copy(st, t).start()
            elif s > 1:
                def keep():
                    collect[s - 2, seat(mine), here(st)] = total[seat(peer(t)), here(st)]

                at_door(keep, lambda: c_copy(st, t).start())

    def first():
        for i in range(len(order) + 1):
            if i < len(order):
                if order[i] == 3:
                    def rest():
                        gate_of(3)
                        up_of(3)

                    at_end(rest)
                act(order[i])
            if i:
                add(0, order[i - 1])
            if i < len(order):
                spread(0, order[i])
            if i:
                send(0, order[i - 1])
            if i < len(order):
                p_copy(0, order[i]).start()
            if i == 0:
                at_end(lambda: take_y(3))
                at_end(lambda: pass_on(2, (1, 0), (1, 1)))
        give_near(0)

    later = [3, 2, 1, 0]

    def compute(st):
        for i, s in enumerate(later):
            spread(st, s)
            if i:
                p_copy(st, later[i - 1]).start()
        p_copy(st, later[-1]).start()

    def give(st):
        for i, s in enumerate(later):
            add(st, s)
            if i:
                send(st, later[i - 1])
        send(st, later[-1])

    def give_near(st):
        n_copy(st, (1, 0)).start()
        n_copy(st, (1, 1)).start()

    def merge(st):
        def act():
            for i in (1, 0):
                local(collect.at[i, pl.ds(0, (quad - 1) * slots), here(st)], c_send, c_recv.at[st, i]).wait_recv()
                far_out[i, :, here(st)] = jnp.dot(gate_w[i], collect[i, :, here(st)], preferred_element_type=f32).astype(bf16)
                o_copy(st, i).start()

        at_door(act)

    def far_wait(st):
        layer = (3 - 3 * side, 2 - side, 3 * side, door)[st]
        local(far_in.at[:, pl.ds(pl.multiple_of(layer * strip, strip), strip)], o_send, o_recv.at[st]).wait_recv()

    at_door(lambda: ready(1), lambda: ready(0))
    first()

    at_door(lambda: ready(0), lambda: ready(1))
    compute(1)
    give(1)
    give_near(1)
    pass_on(2, (3, 0), (3, 1))
    merge(0)
    pass_on(2, (2, 0), (2, 1))
    ready(3)
    compute(2)
    give(2)
    at_door(lambda: give_near(2))
    merge(1)
    ready(2)
    compute(3)
    give(3)
    give_near(3)

    at_end(lambda: give_near(2))
    merge(2)
    merge(3)
    local(back.at[pl.ds(0, 3 * slots // 2), :], n_send, n_recv.at[0]).wait_recv()
    sided = pl.ds(pl.multiple_of(side * span, span), span)
    acc = jnp.dot(near_w[...], back[:, sided], preferred_element_type=f32)
    far_wait(0)
    far_wait(1)
    for st in (2, 3):
        local(back.at[pl.ds(0, 3 * slots // 4), :], n_send, n_recv.at[st - 1]).wait_recv()
        more = jnp.dot(near_w[...], back[:, here(st)], preferred_element_type=f32)
        mixed[:, here(st)] = (more + far_in[:, here(st)].astype(f32)).astype(bf16)
    far_wait(2)
    far_wait(3)
    mixed[:, sided] = (acc + far_in[:, sided].astype(f32)).astype(bf16)

    def sent(block, send):
        local(block, send, o_recv.at[0]).wait_send()

    for w in range(3):
        sent(cuts[w].at[pl.ds(0, n_fs - 1)], w_send.at[w])
        sent(cuts[w], g_send.at[w])
    sent(rows_own, rows_send)
    sent(y_pick, y_send)
    sent(picked.at[pl.ds(0, (n_fs - 1) * slots), pl.ds(0, half)], t_send)
    sent(meta.at[pl.ds(0, 3)], k_send)
    sent(held, p_send)
    sent(held.at[pl.ds(0, 3 * slots), :], n_send)
    sent(held.at[pl.ds(0, 2 * slots), :], c_send)
    at_door(lambda: sent(line_in.at[pl.ds(0, 2)], relay_send), lambda: sent(held.at[pl.ds(0, 2 * slots), :], e_send))
    at_door(lambda: sent(far_out, o_send))


def store_kernel(*refs):
    sems = refs[-1]
    pairs = list(zip(refs[:4], refs[4:8]))
    copies = [pltpu.make_async_copy(src, dst, sems.at[i]) for i, (src, dst) in enumerate(pairs)]
    for c in copies:
        c.start()
    for c in copies:
        c.wait()


def run_handover(sizes, slots, tokens, norm_gain, gate_train, up_train, down_train, expert_ids, route_score):
    n_gr, n_fs, n_tp = sizes["gr"], sizes["fs"], sizes["tp"]
    _, depth, hid = gate_train.shape
    count, width = tokens.shape
    half, quad = width // n_tp, n_fs // 2
    bf16, f32, dma = jnp.bfloat16, jnp.float32, pltpu.SemaphoreType.DMA
    vmem, hbm = pl.BlockSpec(memory_space=pltpu.VMEM), pl.BlockSpec(memory_space=pltpu.HBM)
    shapes = [(1, width, hid), (1, width, hid), (1, hid, width), (count, half)]
    made = pl.pallas_call(
        functools.partial(handover_kernel, sizes),
        out_shape=[pltpu.VMEM(shape, bf16) for shape in shapes],
        in_specs=[hbm] * 7,
        out_specs=[vmem] * 4,
        scratch_shapes=[
            pltpu.VMEM((count, width), bf16), pltpu.VMEM((1, depth), f32), pltpu.VMEM((2, count), jnp.int32), pltpu.VMEM((2, count), f32),
            pltpu.VMEM((n_fs, depth, hid), f32), pltpu.VMEM((n_fs, depth, hid), f32), pltpu.VMEM((n_fs, hid, depth), f32),
            pltpu.VMEM((n_fs, depth, hid), bf16), pltpu.VMEM((n_fs, depth, hid), bf16), pltpu.VMEM((n_fs, hid, depth), bf16),
            pltpu.VMEM((count, width), bf16), pltpu.VMEM((3, count, half), bf16), pltpu.VMEM((n_fs, 8, count), f32),
            pltpu.VMEM((4, slots, half), bf16),
            pltpu.VMEM((n_fs * slots, width), bf16), pltpu.VMEM((n_fs * slots, hid), f32), pltpu.VMEM((n_fs * slots, hid), f32), pltpu.VMEM((n_fs * slots, hid), bf16),
            pltpu.VMEM((n_fs * slots, width), bf16), pltpu.VMEM((n_fs * slots, half), bf16),
            pltpu.VMEM((n_fs * slots, half), bf16), pltpu.VMEM((quad * slots, half), bf16),
            pltpu.VMEM((2, quad * slots, half), bf16), pltpu.VMEM((2, count, half), bf16), pltpu.VMEM((count, half), bf16),
            pltpu.VMEM((count, quad * slots), bf16), pltpu.VMEM((2, count, quad * slots), bf16),
            dma((7,)), dma((3,)), dma((3, n_fs - 1)), dma((3,)), dma((1,)), dma((8,)), dma((10,)), dma((3,)), dma((4,)), dma((4,)), dma((4,)),
            dma((4, 4)), dma((3,)), dma((4, 2)), dma((4,)),
        ],
        compiler_params=pltpu.CompilerParams(collective_id=2, has_side_effects=True, vmem_limit_bytes=56 * 2**20),
        name="handover",
    )(tokens, norm_gain.reshape(1, depth), expert_ids.T, route_score.T, gate_train, up_train, down_train)
    return pl.pallas_call(
        store_kernel,
        out_shape=[jax.ShapeDtypeStruct(shape, bf16) for shape in shapes],
        in_specs=[vmem] * 4,
        out_specs=[pl.BlockSpec(memory_space=pl.ANY)] * 4,
        scratch_shapes=[dma((4,))],
        compiler_params=pltpu.CompilerParams(vmem_limit_bytes=16 * 2**20),
        name="store",
    )(*made)


def on_device(sizes, tokens, norm_gain, gate_train, up_train, down_train, expert_ids, route_score):
    n_gr, n_fs, n_tp = sizes["gr"], sizes["fs"], sizes["tp"]
    bf16 = jnp.bfloat16
    experts, depth, hid = gate_train.shape
    local = experts // n_fs
    count, width = tokens.shape
    capacity = 4 * count // experts
    direct_down = depth % 128 == 0
    if direct_down and local == 1 and capacity % 128 == 0 and (n_gr, n_fs, n_tp) == (2, 8, 2):
        return run_handover(sizes, capacity, tokens, norm_gain, gate_train, up_train, down_train, expert_ids, route_score)

    gate_cast = (norm_gain[None, :, None] * gate_train).astype(bf16)
    up_cast = (norm_gain[None, :, None] * up_train).astype(bf16)
    down_cast = down_train.astype(bf16)
    floated = tokens.astype(jnp.float32)
    normed = (floated * lax.rsqrt(jnp.mean(floated * floated, axis=-1, keepdims=True) + epsilon)).astype(bf16)

    named = expert_ids[:, :, None] == jnp.arange(experts, dtype=jnp.int32)
    names = jnp.any(named, axis=1)
    earlier = jnp.arange(count)[:, None] > jnp.arange(count)[None, :]
    rank = jnp.dot(earlier.astype(bf16), names.astype(bf16), preferred_element_type=jnp.float32).astype(jnp.int32)
    slot = expert_ids * capacity + jnp.sum(jnp.where(named, rank[:, None, :], 0), axis=2)
    keys = jnp.concatenate([slot.T, jnp.full((6, count), -1, jnp.int32)], axis=0)

    share = route_score / jnp.sum(route_score, axis=-1, keepdims=True)
    down_shape = (local, hid, n_gr * n_fs * depth) if direct_down else (n_gr * n_fs, local, hid, depth)
    dma = pltpu.SemaphoreType.DMA
    gate_ready, up_ready, down_ready, gathered, all_keys = pl.pallas_call(
        functools.partial(spread_kernel, sizes, local, direct_down),
        out_shape=(
            jax.ShapeDtypeStruct((local, n_gr * n_fs * depth, hid), bf16),
            jax.ShapeDtypeStruct((local, n_gr * n_fs * depth, hid), bf16),
            jax.ShapeDtypeStruct(down_shape, bf16),
            jax.ShapeDtypeStruct((n_fs, count, width), bf16),
            jax.ShapeDtypeStruct((n_fs, 8, count), jnp.int32),
        ),
        in_specs=[pl.BlockSpec(memory_space=pltpu.VMEM)] * 5,
        out_specs=[pl.BlockSpec(memory_space=pl.ANY)] * 5,
        scratch_shapes=[
            dma((3, n_fs)), dma((3, n_fs)), dma((3, n_fs, n_gr)), dma((3, n_fs, n_gr)),
            dma((n_fs,)), dma((n_fs,)), dma((n_fs,)), dma((n_fs,)),
            dma((n_tp, n_fs)), dma((n_tp, n_fs)), dma((n_fs,)), dma((n_fs,)), dma((5,)),
        ],
        compiler_params=pltpu.CompilerParams(collective_id=0, has_side_effects=True),
        name="spread",
    )(gate_cast, up_cast, down_cast, normed, keys)
    if not direct_down:
        down_ready = down_ready.transpose(1, 2, 0, 3).reshape(local, hid, -1)

    wanted = (lax.axis_index("fs") * local * capacity + jnp.arange(local * capacity, dtype=jnp.int32))[None, :, None]
    pick = ((all_keys[:, 0][:, None, :] == wanted) | (all_keys[:, 1][:, None, :] == wanted)).astype(bf16)
    rows = jnp.einsum("sct,std->scd", pick, gathered, preferred_element_type=jnp.float32).astype(bf16)
    rows = rows.reshape(n_fs, local, capacity, width)
    gate_act = jnp.einsum("seck,ekh->sech", rows, gate_ready, preferred_element_type=jnp.float32)
    up_act = jnp.einsum("seck,ekh->sech", rows, up_ready, preferred_element_type=jnp.float32)
    hidden = (jax.nn.silu(gate_act) * up_act).astype(bf16)
    part = jnp.einsum("sech,ehk->seck", hidden, down_ready, preferred_element_type=jnp.float32).astype(bf16)
    part = part.reshape(n_fs, local * capacity, width)
    half = width // n_tp
    returned = pl.pallas_call(
        functools.partial(return_kernel, sizes),
        out_shape=jax.ShapeDtypeStruct((n_fs, local * capacity, half), bf16),
        in_specs=[pl.BlockSpec(memory_space=pltpu.VMEM)],
        out_specs=pl.BlockSpec(memory_space=pltpu.VMEM),
        scratch_shapes=[
            pltpu.VMEM((max(n_tp - 1, 1), n_fs, local * capacity, half), bf16),
            pltpu.VMEM((n_fs, local * capacity, half), bf16),
            dma((n_tp, n_fs)), dma((n_tp, n_fs)), dma((n_fs,)), dma((n_fs,)),
        ],
        compiler_params=pltpu.CompilerParams(collective_id=1, has_side_effects=True),
        name="giveback",
    )(part)
    at = jnp.arange(experts * capacity, dtype=jnp.int32)[None, :]
    weight = jnp.where(slot[:, :1] == at, share[:, :1], 0.0) + jnp.where(slot[:, 1:] == at, share[:, 1:], 0.0)
    mixed = jnp.dot(weight.astype(bf16), returned.reshape(experts * capacity, half), preferred_element_type=jnp.float32)
    return gate_ready, up_ready, down_ready, mixed.astype(bf16)


def solution(mesh):
    return jax.shard_map(
        functools.partial(on_device, dict(mesh.shape)),
        mesh=mesh,
        in_specs=(
            P(("gr", "fs"), None),
            P(("gr", "fs")),
            P(None, ("gr", "fs"), "tp"),
            P(None, ("gr", "fs"), "tp"),
            P(None, "tp", ("gr", "fs")),
            P(("gr", "fs"), None),
            P(("gr", "fs"), None),
        ),
        out_specs=(
            P("fs", None, "tp"),
            P("fs", None, "tp"),
            P("fs", "tp", None),
            P(("gr", "fs"), "tp"),
        ),
        check_vma=False,
    )
```
